32 devices in a mesh: sp: 8 (over z, x), dp: 4 (over y, core).
Axes of the slice: x: 2, y: 2, z: 4, core: 2. Of those that a mesh axis runs over, the one named last changes fastest.
Arguments:
- layer_activity: bfloat16 [4, 1024, 2048], P('dp', 'sp'), may hold values from -6 to 6
- writer_matrix: bfloat16 [2048, 256], P('dp'), may hold values from -0.125 to 0.125
- reader_matrix: bfloat16 [2048, 256], P('dp'), may hold values from -0.125 to 0.125
- source_unfiltered: bfloat16 [4, 1024, 2048], P('dp', 'sp'), may hold values from -6 to 6
- switch_raw_signal: bfloat16 [4, 1024, 2048], P('dp', 'sp'), may hold values from -6 to 6
- saved_result: bfloat16 [4, 1024, 2048], P('dp', 'sp'), may hold values from -6 to 6
- final_adjoint: bfloat16 [4, 1024, 2048], P('dp', 'sp'), may hold values from -6 to 6
- delta_raw: bfloat16 [4, 1024, 32], P('dp', 'sp'), may hold values from -4 to 4
- extra_logdrop: float32 [4, 1024, 32], P('dp', None, 'sp'), may hold values from 0 to 2.1
- source_filter_coefs: float32 [5, 2048], P(None, 'sp'), may hold values from -2.5 to 2.5
- writer_filter_coefs: float32 [5, 256], replicated, may hold values from -2.5 to 2.5
- reader_filter_coefs: float32 [5, 256], replicated, may hold values from -2.5 to 2.5
- delta_offset: float32 [32], P('sp'), may hold values from -7.5 to -6
- fading_exponents: float32 [32], P('sp'), may hold values from -6 to 3.4
- direct_factor: float32 [32], P('sp'), may hold values from 0.1 to 1.9
- rescale_factor: float32 [2048], replicated, may hold values from 0.1 to 1.9
Outputs:
- d_hidden: bfloat16 [4, 1024, 2048], P('dp', 'sp')
- d_x_raw: bfloat16 [4, 1024, 2048], P('dp', 'sp')
- d_gate: bfloat16 [4, 1024, 2048], P('dp', 'sp')
- d_dt_raw: bfloat16 [4, 1024, 32], P('dp', 'sp')
- d_w_b: float32 [2048, 256], P('dp')
- d_w_c: float32 [2048, 256], P('dp')
The draws below stay inside these ranges and needn't reach their ends.
All inputs are finite; a program needn't handle non-finite values.
Results may differ from the reference program's by a relative error of at most 0.012.
Values may be sent and summed in bfloat16 or wider, within the bound.
A program may use at most 128 MiB of HBM per device.

```python
import jax
import jax.numpy as jnp
from jax import lax

D = 2048
HEADS = 32
HEAD_DIM = 64
STATE = 128
GROUPS = 2
NORM_GROUPS = 8
CONV_K = 5
BLOCK = 128
TOK_DEV = 128
INNER = 2048
TOKEN_TOTAL = 1024
BATCH_TOTAL = 4


def draw_delta_raw(key, part):
    key_base, key_shift = jax.random.split(key)
    baseline = jnp.clip(0.7 * jax.random.normal(key_base, (BATCH_TOTAL, TOKEN_TOTAL, HEADS), jnp.float32), -2.8, 2.8)
    blocks = TOKEN_TOTAL // TOK_DEV
    shifts = jax.random.uniform(key_shift, (BATCH_TOTAL, blocks, 1, 1), jnp.float32, -1.0, 1.0)
    shifts = jnp.broadcast_to(shifts, (BATCH_TOTAL, blocks, TOK_DEV, 1)).reshape(BATCH_TOTAL, TOKEN_TOTAL, 1)
    return (baseline + shifts).astype(jnp.bfloat16)


def draw_extra_logdrop(key, part):
    key_where, key_size = jax.random.split(key)
    places = jax.random.randint(key_where, (3, BATCH_TOTAL, 1, HEADS), 0, TOKEN_TOTAL)
    amounts = jax.random.uniform(key_size, (3, BATCH_TOTAL, 1, HEADS), jnp.float32, 0.22, 0.69)
    positions = jnp.arange(TOKEN_TOTAL, dtype=jnp.int32)[None, None, :, None]
    return jnp.sum(jnp.where(positions == places, amounts, 0.0), axis=0)


def draw_fading_exponents(key, part):
    key_pick, key_fast, key_slow = jax.random.split(key, 3)
    fraction = 0.5
    picked = jax.random.uniform(key_pick, (HEADS,), jnp.float32) < fraction
    fast_rate = jax.random.uniform(key_fast, (HEADS,), jnp.float32, 2.3, 3.0)
    slow_rate = jnp.log(jax.random.uniform(key_slow, (HEADS,), jnp.float32, 0.2, 0.8) / (TOKEN_TOTAL * 0.0018))
    return jnp.where(picked, fast_rate, slow_rate)


def strengthened(result, key, source, target, blocks, factor):
    owner, partner = [(jnp.arange(result.shape[position]) // (result.shape[position] // blocks)).reshape([-1 if axis == position else 1 for axis in range(result.ndim)]) for position in (source, target)]
    chosen = jax.random.permutation(key, blocks)[partner]
    strong = (owner == chosen) | (owner == (partner + blocks // 2) % blocks)
    return jnp.where(strong, factor * result, result)


def level_of(stream_key, extent, cuts, smallest, high):
    factor_of = 1.0
    for axis_at, shards_of in cuts:
        heights = jax.random.uniform(jax.random.fold_in(jax.random.fold_in(stream_key, 6), axis_at), (shards_of,), jnp.float32, smallest / len(cuts), high / len(cuts))
        factor_of = factor_of * jnp.repeat(jnp.exp(heights), extent[axis_at] // shards_of).reshape((-1,) + (1,) * (len(extent) - 1 - axis_at))
    return factor_of


def gaussian(key, extent, spread, most, pieces=(), held_as=jnp.bfloat16):
    values = jax.random.normal(key, extent, jnp.float32) * spread
    if len(pieces) > 0:
        values = level_of(key, extent, pieces, -0.22, 0.18) * values
    return jnp.clip(values, min=-most, max=most).astype(held_as)


def bell_draw_with(rng, dims, scale, bound, shards, heavy, kind=jnp.bfloat16):
    entries = scale * jax.random.normal(rng, dims, jnp.float32)
    if shards:
        entries = entries * level_of(rng, dims, shards, -0.22, 0.18)
    return jnp.clip(strengthened(entries, jax.random.fold_in(rng, 3), *heavy), -bound, bound).astype(kind)


def setup_inputs(seed: int = 0) -> dict:
    seeds = jax.random.split(jax.random.key(seed), 17)
    return {
        "layer_activity": bell_draw_with(seeds[0], (BATCH_TOTAL, TOKEN_TOTAL, D), 1.0, 6.0, ((0, 4), (1, 8)), (1, 2, 8, 2.0)),
        "writer_matrix": gaussian(seeds[1], (D, GROUPS * STATE), D ** -0.5, 0.125, ((0, 4),)),
        "reader_matrix": gaussian(seeds[2], (D, GROUPS * STATE), D ** -0.5, 0.125, ((0, 4),)),
        "source_unfiltered": gaussian(seeds[3], (BATCH_TOTAL, TOKEN_TOTAL, INNER), 1.0, 6.0, ((0, 4), (1, 8))),
        "switch_raw_signal": gaussian(seeds[4], (BATCH_TOTAL, TOKEN_TOTAL, INNER), 1.0, 6.0, ((0, 4), (1, 8))),
        "saved_result": gaussian(seeds[5], (BATCH_TOTAL, TOKEN_TOTAL, INNER), 1.0, 6.0, ((0, 4), (1, 8))),
        "final_adjoint": gaussian(seeds[6], (BATCH_TOTAL, TOKEN_TOTAL, INNER), 1.0, 6.0, ((0, 4), (1, 8))),
        "delta_raw": draw_delta_raw(jax.random.fold_in(seeds[16], 71), 0),
        "extra_logdrop": draw_extra_logdrop(jax.random.fold_in(seeds[16], 71), 0),
        "source_filter_coefs": gaussian(seeds[9], (CONV_K, INNER), CONV_K ** -0.5, 2.5, ((1, 8),), jnp.float32),
        "writer_filter_coefs": gaussian(seeds[10], (CONV_K, GROUPS * STATE), CONV_K ** -0.5, 2.5, (), jnp.float32),
        "reader_filter_coefs": gaussian(seeds[11], (CONV_K, GROUPS * STATE), CONV_K ** -0.5, 2.5, (), jnp.float32),
        "delta_offset": jnp.clip(-7.5 + 1.5 * jax.random.uniform(seeds[12], (HEADS,), jnp.float32) ** level_of(seeds[12], (HEADS,), ((0, 8),), -0.2, 0.2), -7.5, -6.0),
        "fading_exponents": draw_fading_exponents(jax.random.fold_in(seeds[16], 71), 0),
        "direct_factor": jnp.clip(1.0 + 0.18 * jax.random.normal(seeds[14], (HEADS,), jnp.float32), 0.1, 1.9),
        "rescale_factor": jnp.clip(1.0 + 0.18 * jax.random.normal(seeds[15], (INNER,), jnp.float32), 0.1, 1.9),
    }


EPSILON = 1e-06
highest = lax.Precision.HIGHEST

def centred_conv(values, tap_weights):
    sample_window = values.shape[0]
    reach_side = (tap_weights.shape[0] - 1) // 2
    padded = jnp.pad(values, ((reach_side, reach_side), (0, 0)))
    summed = jnp.zeros_like(values)
    for offset in range(tap_weights.shape[0]):
        summed = summed + tap_weights[offset][None, :] * padded[offset:offset + sample_window]
    return summed

def one_channel_scan(source_unfiltered, writer_unfiltered, reader_unfiltered, delta_raw, extra_logdrop, source_filter_coefs, writer_filter_coefs, reader_filter_coefs, delta_offset, fading_exponents, direct_factor):
    inputs = jax.nn.silu(centred_conv(source_unfiltered, source_filter_coefs))
    keys_b = jax.nn.silu(centred_conv(writer_unfiltered, writer_filter_coefs))
    reads_c = jax.nn.silu(centred_conv(reader_unfiltered, reader_filter_coefs))
    smooth_delta = jax.nn.softplus(delta_raw + delta_offset)
    channel_fading = smooth_delta * jnp.exp(fading_exponents) + extra_logdrop
    cumulative = jnp.cumsum(channel_fading)
    sample_window = source_unfiltered.shape[0]
    blocks = sample_window // BLOCK
    driven = (inputs * smooth_delta[:, None]).reshape(blocks, BLOCK, -1)
    keyed = keys_b.reshape(blocks, BLOCK, -1)
    reading = reads_c.reshape(blocks, BLOCK, -1)
    levels = cumulative.reshape(blocks, BLOCK)
    within = jnp.exp(-jnp.abs(levels[:, :, None] - levels[:, None, :]))
    scores = jnp.einsum('ktn,ksn->kts', reading, keyed, precision=highest) * within
    output = jnp.einsum('kts,ksp->ktp', scores, driven, precision=highest)
    block_ends = levels[:, -1]
    block_starts = levels[:, 0]
    block_order = jnp.arange(blocks, dtype=jnp.int32)
    prev_end = jnp.concatenate([cumulative[:1], block_ends[:-1]])
    next_start = jnp.concatenate([block_starts[1:], cumulative[-1:]])
    weight_fwd = jnp.exp(levels - block_ends[:, None])
    state_fwd = jnp.einsum('ksn,ksp->knp', keyed * weight_fwd[:, :, None], driven, precision=highest)
    mask_fwd = (block_order[None, :] < block_order[:, None]).astype(cumulative.dtype)
    link_fwd = jnp.exp(-jnp.abs(prev_end[:, None] - block_ends[None, :])) * mask_fwd
    carry_fwd = jnp.einsum('kj,jnp->knp', link_fwd, state_fwd, precision=highest)
    read_fwd = reading * jnp.exp(prev_end[:, None] - levels)[:, :, None]
    weight_bwd = jnp.exp(block_starts[:, None] - levels)
    state_bwd = jnp.einsum('ksn,ksp->knp', keyed * weight_bwd[:, :, None], driven, precision=highest)
    mask_bwd = (block_order[None, :] > block_order[:, None]).astype(cumulative.dtype)
    link_bwd = jnp.exp(-jnp.abs(next_start[:, None] - block_starts[None, :])) * mask_bwd
    carry_bwd = jnp.einsum('kj,jnp->knp', link_bwd, state_bwd, precision=highest)
    read_bwd = reading * jnp.exp(levels - next_start[:, None])[:, :, None]
    output = output + jnp.einsum('ktn,knp->ktp', read_fwd, carry_fwd, precision=highest)
    output = output + jnp.einsum('ktn,knp->ktp', read_bwd, carry_bwd, precision=highest)
    return output.reshape(sample_window, -1) + direct_factor * inputs

def channelwise_derivs(source_unfiltered, writer_unfiltered, reader_unfiltered, delta_raw, extra_logdrop, source_filter_coefs, writer_filter_coefs, reader_filter_coefs, delta_offset, fading_exponents, direct_factor, result_adjoint):

    def forward(source_filtered, writer_filtered, reader_filtered, delta_argument):
        return one_channel_scan(source_filtered, writer_filtered, reader_filtered, delta_argument, extra_logdrop, source_filter_coefs, writer_filter_coefs, reader_filter_coefs, delta_offset, fading_exponents, direct_factor)
    primal, pullback = jax.vjp(forward, source_unfiltered.astype(jnp.float32), writer_unfiltered.astype(jnp.float32), reader_unfiltered.astype(jnp.float32), delta_raw.astype(jnp.float32))
    source_derivative, writer_derivative, reader_derivative, delta_derivative = pullback(result_adjoint.astype(jnp.float32))
    return (source_derivative.astype(jnp.bfloat16), writer_derivative.astype(jnp.bfloat16), reader_derivative.astype(jnp.bfloat16), delta_derivative.astype(jnp.bfloat16))

def gated_norm(values, gating, rescale_factor):
    mixed = values * jax.nn.silu(gating)
    grouped = mixed.reshape(mixed.shape[0], NORM_GROUPS, -1)
    scaled = grouped * lax.rsqrt(lax.optimization_barrier(jnp.mean(grouped * grouped, axis=-1, keepdims=True)) + EPSILON)
    return scaled.reshape(mixed.shape) * rescale_factor

def norm_backward(saved_result, switch_raw_signal, final_adjoint, rescale_factor):
    primal, pullback = jax.vjp(lambda values, gating: gated_norm(values, gating, rescale_factor), saved_result.astype(jnp.float32), switch_raw_signal.astype(jnp.float32))
    d_values, d_gates = pullback(final_adjoint.astype(jnp.float32))
    return (d_values.astype(jnp.bfloat16), d_gates.astype(jnp.bfloat16))

def reference(layer_activity, writer_matrix, reader_matrix, source_unfiltered, switch_raw_signal, saved_result, final_adjoint, delta_raw, extra_logdrop, source_filter_coefs, writer_filter_coefs, reader_filter_coefs, delta_offset, fading_exponents, direct_factor, rescale_factor):
    latent_dimension = GROUPS * STATE
    per_group = HEADS // GROUPS
    group_of = jnp.arange(HEADS, dtype=jnp.int32) // per_group
    token_rows = layer_activity.reshape(BATCH_TOTAL * TOKEN_TOTAL, D)
    writer_linear = jnp.dot(token_rows, writer_matrix, preferred_element_type=jnp.float32).astype(jnp.bfloat16)
    reader_linear = jnp.dot(token_rows, reader_matrix, preferred_element_type=jnp.float32).astype(jnp.bfloat16)
    source_filter_fn = jnp.transpose(source_filter_coefs.reshape(CONV_K, HEADS, HEAD_DIM), (1, 0, 2))
    writer_filter_fn = jnp.transpose(writer_filter_coefs.reshape(CONV_K, GROUPS, STATE)[:, group_of], (1, 0, 2))
    reader_filter_fn = jnp.transpose(reader_filter_coefs.reshape(CONV_K, GROUPS, STATE)[:, group_of], (1, 0, 2))

    def one_sample_pass(collected_parts):
        sample_source, sample_writer, sample_reader, sample_delta, sample_logdrop_lines, sample_result, sample_switch, sample_final = collected_parts
        result_adjoint, d_gate = norm_backward(sample_result, sample_switch, sample_final, rescale_factor)
        channelwise_source = jnp.transpose(sample_source.reshape(TOKEN_TOTAL, HEADS, HEAD_DIM), (1, 0, 2))
        channelwise_writer = jnp.transpose(sample_writer.reshape(TOKEN_TOTAL, GROUPS, STATE)[:, group_of], (1, 0, 2))
        channelwise_reader = jnp.transpose(sample_reader.reshape(TOKEN_TOTAL, GROUPS, STATE)[:, group_of], (1, 0, 2))
        channelwise_adjoint = jnp.transpose(result_adjoint.reshape(TOKEN_TOTAL, HEADS, HEAD_DIM), (1, 0, 2))
        source_derivative, writer_derivative, reader_derivative, delta_derivative = lax.map(lambda collected_items: channelwise_derivs(*collected_items), (channelwise_source, channelwise_writer, channelwise_reader, sample_delta.T, sample_logdrop_lines.T, source_filter_fn, writer_filter_fn, reader_filter_fn, delta_offset, fading_exponents, direct_factor, channelwise_adjoint))
        summed_b = lax.optimization_barrier(jnp.sum(writer_derivative.astype(jnp.float32).reshape(GROUPS, per_group, TOKEN_TOTAL, STATE), axis=1))
        summed_c = lax.optimization_barrier(jnp.sum(reader_derivative.astype(jnp.float32).reshape(GROUPS, per_group, TOKEN_TOTAL, STATE), axis=1))
        summed_b = jnp.transpose(summed_b, (1, 0, 2)).reshape(TOKEN_TOTAL, latent_dimension).astype(jnp.bfloat16)
        summed_c = jnp.transpose(summed_c, (1, 0, 2)).reshape(TOKEN_TOTAL, latent_dimension).astype(jnp.bfloat16)
        return (jnp.transpose(source_derivative, (1, 0, 2)).reshape(TOKEN_TOTAL, INNER), summed_b, summed_c, delta_derivative.T, d_gate)
    whole_batch_source, whole_batch_writer, whole_batch_reader, whole_batch_delta, whole_batch_switch = lax.map(one_sample_pass, (source_unfiltered, writer_linear.reshape(BATCH_TOTAL, TOKEN_TOTAL, latent_dimension), reader_linear.reshape(BATCH_TOTAL, TOKEN_TOTAL, latent_dimension), delta_raw, extra_logdrop, saved_result, switch_raw_signal, final_adjoint))
    grad_rows_b = whole_batch_writer.reshape(BATCH_TOTAL * TOKEN_TOTAL, latent_dimension)
    grad_rows_c = whole_batch_reader.reshape(BATCH_TOTAL * TOKEN_TOTAL, latent_dimension)
    d_hidden = (jnp.dot(grad_rows_b, writer_matrix.T, preferred_element_type=jnp.float32) + jnp.dot(grad_rows_c, reader_matrix.T, preferred_element_type=jnp.float32)).astype(jnp.bfloat16)
    d_w_b = jnp.dot(token_rows.T, grad_rows_b, preferred_element_type=jnp.float32)
    d_w_c = jnp.dot(token_rows.T, grad_rows_c, preferred_element_type=jnp.float32)
    return (d_hidden.reshape(BATCH_TOTAL, TOKEN_TOTAL, D), whole_batch_source, whole_batch_switch, whole_batch_delta, d_w_b, d_w_c)
```

```python
import functools

import jax
import jax.numpy as jnp
from jax import lax
from jax.experimental import pallas as pl
from jax.experimental.pallas import tpu as pltpu
from jax.sharding import PartitionSpec as P

HEADS = 32
HEAD_DIM = 64
STATE = 128
GROUPS = 2
NORM_GROUPS = 8
CONV_K = 5
LANES = 128
HALO = 16
SKEW = 2
EPSILON = 1e-06
LOG2E = 1.4426950408889634
highest = lax.Precision.HIGHEST
f32 = jnp.float32
bf16 = jnp.bfloat16
NT = (((1,), (1,)), ((), ()))
TN = (((0,), (0,)), ((), ()))


def sigmoid(v):
    return 1.0 / (1.0 + jnp.exp(-v))


def softplus(v):
    e = jnp.exp(-jnp.abs(v))
    z = e / (2.0 + e)
    z2 = z * z
    series = jnp.full_like(z, 1.0 / 17.0)
    for odd in (15, 13, 11, 9, 7, 5, 3, 1):
        series = series * z2 + 1.0 / odd
    return jnp.maximum(v, 0.0) + 2.0 * z * series


def mm(a, b):
    return jnp.dot(a, b, preferred_element_type=f32)


def mm_nt(a, b):
    return lax.dot_general(a, b, NT, preferred_element_type=f32)


def mm_tn(a, b):
    return lax.dot_general(a, b, TN, preferred_element_type=f32)


def split_mm(a, b):
    hi = a.astype(bf16)
    lo = (a - hi.astype(f32)).astype(bf16)
    return mm(hi, b) + mm(lo, b)


def window_conv(rows, taps, count, flip):
    total = None
    for k in range(CONV_K):
        shift = HALO - CONV_K // 2 + k
        tap = taps[CONV_K - 1 - k if flip else k][None, :]
        term = tap * pltpu.roll(rows, rows.shape[0] - shift, axis=0)[:count]
        total = term if total is None else total + term
    return total


def greet(axes):
    barrier = pltpu.get_barrier_semaphore()
    count = 0
    for axis in axes:
        size = lax.axis_size(axis)
        me = lax.axis_index(axis)
        for o in range(1, size):
            pl.semaphore_signal(
                barrier,
                inc=1,
                device_id={axis: lax.rem(me + o, size)},
                device_id_type=pl.DeviceIdType.MESH,
            )
            count += 1
    pl.semaphore_wait(barrier, count)


def slot_table(sp, dp, cores, pairs):
    ny = dp // cores
    chunks = sp // GROUPS
    counts = (
        ("w_y", 2 * ny),
        ("w_core", 2),
        ("w_fwd", 2 * ny),
        ("la", dp),
        ("x", 1),
        ("x_left", GROUPS),
        ("x_right", GROUPS),
        ("dt", 1),
        ("drop", chunks),
        ("tap", sp),
        ("dy", NORM_GROUPS),
        ("bc", 1),
        ("bc_left", GROUPS),
        ("bc_right", GROUPS),
        ("right", pairs),
        ("left", pairs),
        ("gx", pairs),
        ("gx_left", GROUPS),
        ("gx_right", GROUPS),
        ("gbc", 1),
        ("gbc_left", GROUPS),
        ("gbc_right", GROUPS),
        ("ddt", 1),
        ("g_y", ny),
        ("g_core", 1),
        ("g_fwd", ny),
        ("w1", 2),
        ("w2", 2 * chunks),
        ("w3", 2 * chunks),
        ("w4", 2),
    )
    table = {}
    at = 0
    for name, count in counts:
        table[name] = at
        at += count
    return table, at


def mega_kernel(
    heads,
    cores,
    la_ref,
    wb_ref,
    wc_ref,
    x_ref,
    gates_ref,
    values_ref,
    adjoint_ref,
    dt_ref,
    drop_ref,
    tapx_ref,
    tapb_ref,
    tapc_ref,
    scale_ref,
    offset_ref,
    fade_ref,
    skip_ref,
    dgate_ref,
    dx_ref,
    ddt_ref,
    dh_ref,
    tall,
    wball,
    wcall,
    cols,
    xin,
    dyin,
    dysend,
    dtin,
    dropsend,
    dropin,
    drow,
    tapsend,
    tapin,
    tapall,
    bcsend,
    bcin,
    u_ref,
    sux_ref,
    dts_ref,
    ef_ref,
    eb_ref,
    tdec,
    vb_ref,
    vef_ref,
    veb_ref,
    dyef_ref,
    dyeb_ref,
    kn,
    rn,
    kt,
    rt,
    sbc_ref,
    score_ref,
    sign_ref,
    gesum,
    lcolb,
    lrow,
    sigrow,
    faderow,
    dv_ref,
    sr_ref,
    sl_ref,
    rin,
    lin,
    rout,
    lout,
    dksum,
    drsum,
    dlev,
    sdt,
    cross,
    colrow,
    dpx,
    gx,
    dpbc,
    gbc,
    ddtsend,
    gsend,
    gall,
    wsend,
    wown,
    w1in,
    s1send,
    w2in,
    s3send,
    ss,
    rs,
):
    dp = lax.axis_size("dp")
    sp = lax.axis_size("sp")
    me_dp = lax.axis_index("dp")
    me_sp = lax.axis_index("sp")
    ny = dp // cores
    chunks = sp // GROUPS
    y = me_dp // cores
    core = lax.rem(me_dp, cores)
    c = me_sp // GROUPS
    m = lax.rem(me_sp, GROUPS)
    p = GROUPS - 1 - m
    partner = c * GROUPS + p
    other_core = y * cores + (cores - 1 - core)
    tokens, inner = x_ref.shape
    gw = inner // GROUPS
    gh = HEADS // GROUPS
    ch = tokens * GROUPS
    pairs = gw // LANES
    cw = wb_ref.shape[0]
    latent = wb_ref.shape[1]
    xc = heads * HEAD_DIM
    nsrc = sp // GROUPS
    rows = cw // sp
    first = c == 0
    last = c == chunks - 1
    table, _ = slot_table(sp, dp, cores, pairs)
    sent = []

    def copy(src, dst, name, index, axis, peer, into=None):
        at = table[name]
        return pltpu.make_async_remote_copy(
            src_ref=src,
            dst_ref=dst,
            send_sem=ss.at[at + index],
            recv_sem=rs.at[at + (index if into is None else into)],
            device_id={axis: peer},
            device_id_type=pl.DeviceIdType.MESH,
        )

    def go(item, cond=None):
        if cond is None:
            item.start()
        else:

            @pl.when(cond)
            def _():
                item.start()

        sent.append((item, cond))
        return item

    def arrive(item, cond=None):
        if cond is None:
            item.wait_recv()
        else:

            @pl.when(cond)
            def _():
                item.wait_recv()

    def lanes(index, width):
        return pl.ds(pl.multiple_of(index * width, LANES), width)

    def near(step):
        return lax.rem(me_sp + step + 2 * sp, sp)

    mine = pl.ds(pl.multiple_of(HALO + m * tokens, HALO), tokens)
    mine0 = pl.ds(pl.multiple_of(m * tokens, HALO), tokens)
    body = slice(HALO, HALO + ch)
    left_rows = slice(0, HALO)
    right_rows = slice(HALO + ch, 2 * HALO + ch)
    to_right = jnp.logical_and(m == GROUPS - 1, jnp.logical_not(last))
    to_left = jnp.logical_and(m == 0, jnp.logical_not(first))

    greet(("dp", "sp"))

    w_y = []
    for o in range(1, ny):
        peer = lax.rem(y + o, ny) * cores + core
        w_y.append(
            (
                go(copy(wb_ref, wball.at[me_dp], "w_y", 2 * o, "dp", peer)),
                go(copy(wc_ref, wcall.at[me_dp], "w_y", 2 * o + 1, "dp", peer)),
            )
        )
    w_core = []
    if cores > 1:
        w_core = [
            go(copy(wb_ref, wball.at[me_dp], "w_core", 0, "dp", other_core)),
            go(copy(wc_ref, wcall.at[me_dp], "w_core", 1, "dp", other_core)),
        ]
    x_copy = go(copy(x_ref.at[:, lanes(p, gw)], xin.at[mine, :], "x", 0, "sp", partner))
    dt_copy = go(
        copy(
            dt_ref.at[pl.ds(pl.multiple_of(p * gh, gh), gh), :],
            dtin.at[:, lanes(m, tokens)],
            "dt",
            0,
            "sp",
            partner,
        )
    )

    def send_halo(name, source, target):
        for g in range(GROUPS):
            go(
                copy(
                    source(g, slice(tokens - HALO, tokens)),
                    target.at[left_rows, :],
                    name + "_left",
                    g,
                    "sp",
                    near(1 + g),
                    into=0,
                ),
                to_right,
            )
            go(
                copy(
                    source(g, slice(0, HALO)),
                    target.at[right_rows, :],
                    name + "_right",
                    g,
                    "sp",
                    near(g - GROUPS),
                    into=0,
                ),
                to_left,
            )

    def await_halo(name, target):
        arrive(
            copy(target.at[left_rows, :], target.at[left_rows, :], name + "_left", 0, "sp", partner),
            jnp.logical_not(first),
        )
        arrive(
            copy(target.at[right_rows, :], target.at[right_rows, :], name + "_right", 0, "sp", partner),
            jnp.logical_not(last),
        )

        @pl.when(first)
        def _():
            target[left_rows, :] = jnp.zeros((HALO, target.shape[1]), bf16)

        @pl.when(last)
        def _():
            target[right_rows, :] = jnp.zeros((HALO, target.shape[1]), bf16)

    send_halo("x", lambda g, r: x_ref.at[r, g * gw : (g + 1) * gw], xin)

    rows_h = dropsend.shape[1]
    head_row = lax.broadcasted_iota(jnp.int32, (rows_h, LANES), 0)
    offsets = jnp.zeros((rows_h, LANES), f32)
    fades = jnp.zeros((rows_h, LANES), f32)
    for h in range(heads):
        offsets = jnp.where(head_row == h, offset_ref[h], offsets)
        fades = jnp.where(head_row == h, fade_ref[h], fades)
    dropsend[...] = jnp.zeros_like(dropsend)
    for k in range(chunks):
        dropsend[k, :heads, :ch] = drop_ref[:, k * ch : (k + 1) * ch]
        dropsend[k, :, ch : ch + LANES] = offsets
        dropsend[k, :, ch + LANES :] = fades
    owner = (me_sp * heads) // gh
    place = me_sp - owner * nsrc
    for o in range(chunks):
        k = lax.rem(c + o, chunks)
        go(
            copy(
                dropsend.at[k],
                dropin.at[place],
                "drop",
                o,
                "sp",
                k * GROUPS + owner if o else partner,
                into=place,
            ),
            None if o else owner != m,
        )

    @pl.when(owner == m)
    def _():
        dropin[place] = dropsend[c]

    xw = tapsend.shape[1]
    tap_lane = lax.broadcasted_iota(jnp.int32, (1, xw), 1) // HEAD_DIM
    skips = jnp.zeros((1, xw), f32)
    for h in range(heads):
        skips = jnp.where(tap_lane == h, skip_ref[h], skips)
    tapsend[...] = jnp.zeros_like(tapsend)
    tapsend[:CONV_K, :xc] = tapx_ref[...]
    tapsend[CONV_K : CONV_K + 1, :] = skips
    tap_copies = []
    for o in range(1, sp):
        tap_copies.append(go(copy(tapsend, tapin.at[me_sp], "tap", o, "sp", lax.rem(me_sp + o, sp))))
    tapin[me_sp] = tapsend[...]
    la_copies = []
    for o in range(1, dp):
        peer = lax.rem(me_dp + o, dp)
        la_copies.append(
            go(copy(la_ref.at[:, lanes(peer, cw)], cols.at[me_dp], "la", o, "dp", peer))
        )
    cols[me_dp] = la_ref[:, lanes(me_dp, cw)]
    xin[mine, :] = x_ref[:, lanes(m, gw)]
    dtin[:, lanes(m, tokens)] = dt_ref[pl.ds(pl.multiple_of(m * gh, gh), gh), :]

    width = inner // NORM_GROUPS
    per_half = NORM_GROUPS // GROUPS
    dy_copies = []
    for half in range(GROUPS):
        who = p if half == 0 else m
        for i in range(per_half):
            span = lanes(who * per_half + i, width)
            values = values_ref[:, span].astype(f32)
            gates = gates_ref[:, span].astype(f32)
            sig = sigmoid(gates)
            act = gates * sig
            g = values * act
            dn = adjoint_ref[:, span].astype(f32) * scale_ref[:, span]
            inv = lax.rsqrt(jnp.sum(g * g, axis=1, keepdims=True) * (1.0 / width) + EPSILON)
            along = jnp.sum(dn * g, axis=1, keepdims=True) * (1.0 / width)
            dg = inv * dn - g * (inv * inv * inv * along)
            dgate_ref[:, span] = (dg * values * (sig + act * (1.0 - sig))).astype(bf16)
            dy = (dg * act).astype(bf16)
            at = slice(i * width, (i + 1) * width)
            if half == 0:
                dysend[:, at] = dy
                dy_copies.append(
                    go(copy(dysend.at[:, at], dyin.at[mine0, at], "dy", i, "sp", partner))
                )
            else:
                dyin[mine0, at] = dy

    arrive(dt_copy)
    for i in range(nsrc):
        arrive(
            copy(dropsend.at[0], dropin.at[i], "drop", i, "sp", partner), m * nsrc + i != me_sp
        )
        drow[i * heads : (i + 1) * heads, :] = dropin[i, :heads, :]
    twice = lambda v: jnp.concatenate([v] * (ch // LANES), axis=1)
    fade = jnp.exp(drow[:, ch + LANES :])
    a = dtin[...].astype(f32) + twice(drow[:, ch : ch + LANES])
    dt = softplus(a)
    sigrow[...] = sigmoid(a)
    faderow[...] = fade
    rate = dt * twice(fade) + drow[:, :ch]
    row_i = lax.broadcasted_iota(jnp.int32, (ch, ch), 0)
    col_i = lax.broadcasted_iota(jnp.int32, (ch, ch), 1)
    upper = (row_i <= col_i).astype(f32)
    level = jnp.dot(rate, upper, precision=highest, preferred_element_type=f32) * LOG2E
    lrow[...] = level
    fill = jnp.zeros((LANES - gh, ch), f32)
    lcol = jnp.concatenate([level, fill], axis=0).T
    dtcol = jnp.concatenate([dt, fill], axis=0).T
    low_lane = lax.broadcasted_iota(jnp.int32, (ch, LANES), 1) < HEAD_DIM
    for j in range(pairs):
        pair = []
        for h in (2 * j, 2 * j + 1):
            wide = jnp.broadcast_to(lcol[:, h : h + 1], (ch, LANES))
            lcolb[h] = wide
            pair.append(wide)
        spread = jnp.where(low_lane, pair[0], pair[1])
        end = spread[ch - 1 : ch, :]
        ef_ref[j] = jnp.exp2(-spread)
        eb_ref[j] = jnp.exp2(spread - end)
        tdec[j] = jnp.broadcast_to(jnp.exp2(-end), (8, LANES))
        dts_ref[j] = jnp.where(low_lane, dtcol[:, 2 * j : 2 * j + 1], dtcol[:, 2 * j + 1 : 2 * j + 2])

    for item in tap_copies:
        arrive(item)
    if xc % LANES == 0:
        for i in range(sp):
            tapall[:, i * xc : (i + 1) * xc] = tapin[i]
    else:
        per = LANES // xc
        for i in range(inner // LANES):
            tapall[:, i * LANES : (i + 1) * LANES] = jnp.concatenate(
                [tapin[i * per + q][:, :xc] for q in range(per)], axis=1
            )
    arrive(x_copy)
    await_halo("x", xin)

    @pl.loop(0, pairs)
    def _(j):
        taps = tapall[:, lanes(m * pairs + j, LANES)]
        pre = window_conv(xin[:, lanes(j, LANES)].astype(f32), taps, ch, False)
        sig = sigmoid(pre)
        u = pre * sig
        u_ref[j] = u
        sux_ref[j] = sig + u * (1.0 - sig)
        v = u * dts_ref[j]
        vb_ref[j] = v.astype(bf16)
        vef_ref[j] = (v * ef_ref[j]).astype(bf16)
        veb_ref[j] = (v * eb_ref[j]).astype(bf16)

    wball[me_dp] = wb_ref[...]
    wcall[me_dp] = wc_ref[...]

    def project(total, index):
        part = la_ref[:, lanes(index, cw)]
        tb, tc = mm(part, wball[index]), mm(part, wcall[index])
        return (tb, tc) if total is None else (total[0] + tb, total[1] + tc)

    total = project(None, me_dp)
    for item in w_core:
        arrive(item)
    if cores > 1:
        total = project(total, other_core)
    w_fwd = []
    for o in range(1, ny):
        src = lax.rem(y - o + ny, ny) * cores + core
        for q in range(2):
            arrive(w_y[o - 1][q])
            if cores > 1:
                full = (wball, wcall)[q].at[src]
                w_fwd.append(go(copy(full, full, "w_fwd", 2 * o + q, "dp", other_core)))
        total = project(total, src)
    for o in range(1, ny):
        if cores > 1:
            arrive(w_fwd[2 * o - 2])
            arrive(w_fwd[2 * o - 1])
            total = project(total, lax.rem(y - o + ny, ny) * cores + cores - 1 - core)
    proj_b, proj_c = total[0].astype(bf16), total[1].astype(bf16)
    for g in range(GROUPS):
        bcsend[g, :, :STATE] = proj_b[:, g * STATE : (g + 1) * STATE]
        bcsend[g, :, STATE:] = proj_c[:, g * STATE : (g + 1) * STATE]
    bc_copy = go(copy(bcsend.at[p], bcin.at[mine, :], "bc", 0, "sp", partner))
    send_halo("bc", lambda g, r: bcsend.at[g, r, :], bcin)
    bcin[mine, :] = bcsend[m]

    for item in dy_copies:
        arrive(item)

    @pl.loop(0, pairs)
    def _(j):
        dy = dyin[:, lanes(j, LANES)].astype(f32)
        dyef_ref[j] = (dy * ef_ref[j]).astype(bf16)
        dyeb_ref[j] = (dy * eb_ref[j]).astype(bf16)

    arrive(bc_copy)
    await_halo("bc", bcin)
    for q in range(2):
        taps = (tapb_ref, tapc_ref)[q][:, lanes(m, STATE)]
        at = slice(q * STATE, (q + 1) * STATE)
        pre = window_conv(bcin[:, at].astype(f32), taps, ch, False)
        sig = sigmoid(pre)
        kr = pre * sig
        sbc_ref[:, at] = sig + kr * (1.0 - sig)
        (kn, rn)[q][...] = kr.astype(bf16)
        (kt, rt)[q][...] = kr.T.astype(bf16)
    score = mm_nt(kn[...], rn[...])
    score_ref[...] = score
    sign_ref[...] = score * jnp.clip(col_i - row_i, -1, 1).astype(f32)

    gesum[...] = jnp.zeros_like(gesum)
    dksum[...] = jnp.zeros_like(dksum)
    drsum[...] = jnp.zeros_like(drsum)
    dlev[...] = jnp.zeros_like(dlev)
    sdt[...] = jnp.zeros_like(sdt)
    cross[...] = jnp.zeros_like(cross)

    @pl.when(first)
    def _():
        rin[...] = jnp.zeros_like(rin)

    @pl.when(last)
    def _():
        lin[...] = jnp.zeros_like(lin)

    lane_low = lax.broadcasted_iota(jnp.int32, (1, LANES), 1) < HEAD_DIM
    masks = (lane_low.astype(bf16), 1.0 - lane_low.astype(bf16))
    pick_lane = lax.broadcasted_iota(jnp.int32, (LANES, LANES), 1)
    pick_half = lax.broadcasted_iota(jnp.int32, (LANES, LANES), 0) // HEAD_DIM
    block = min(ch, LANES)

    def intra(j):
        dyj = dyin[:, lanes(j, LANES)]
        for a in range(2):
            h = 2 * j + a
            lr = lrow[pl.ds(h, 1), :]
            dym = dyj * masks[a]
            onehot = (pick_lane == h).astype(bf16)
            below = None
            for b in range(ch // block):
                at = slice(b * block, (b + 1) * block)
                gap = twice(lcolb[h, at]) - lr
                decay = jnp.exp2(-jnp.abs(gap))
                ge = mm_nt(vb_ref[j, at] * masks[a], dyj) * decay
                gesum[at, :] += ge
                part = mm((score_ref[at, :] * decay).astype(bf16), dym)
                if a == 0:
                    dv_ref[j, at] = part
                else:
                    dv_ref[j, at] += part
                q = sign_ref[at, :] * ge
                down = jnp.sum(q, axis=0, keepdims=True)
                below = down if below is None else below + down
                part = q[:, :LANES]
                for piece in range(1, ch // LANES):
                    part = part + q[:, piece * LANES : (piece + 1) * LANES]
                dlev[at, :] += split_mm(part, onehot)
            colrow[pl.ds(h, 1), :] = below

    def gx_copy(j):
        return copy(
            dpx.at[pl.ds(pl.multiple_of(p * (tokens - HALO), HALO), tokens + HALO), lanes(j, LANES)],
            gx.at[
                m, pl.ds(pl.multiple_of(HALO - HALO * p, HALO), tokens + HALO), lanes(j, LANES)
            ],
            "gx",
            j,
            "sp",
            partner,
        )

    keep_src = pl.ds(pl.multiple_of(m * (tokens - HALO), HALO), tokens + HALO)
    keep_dst = pl.ds(pl.multiple_of(HALO - HALO * m, HALO), tokens + HALO)

    def consume(j):
        k, r = kn[...], rn[...]
        ra, rb, la, lb = rin[j, 0], rin[j, 1], lin[j, 0], lin[j, 1]
        ef, eb = ef_ref[j], eb_ref[j]
        u = u_ref[j]
        at = lanes(j, LANES)
        dy = dyin[:, at].astype(f32)
        v = vb_ref[j].astype(f32)
        skip = tapall[CONV_K : CONV_K + 1, lanes(m * pairs + j, LANES)]
        onehot = (pick_lane == 2 * j + pick_half).astype(bf16)
        dl, dr = ef * mm(k, rb), eb * mm(k, lb)
        ml, mr = ef * mm(r, ra), eb * mm(r, la)
        dv = dv_ref[j] + dl + dr
        dpx[:, at] = ((dv * dts_ref[j] + skip * dy) * sux_ref[j]).astype(bf16)
        gx_copy(j).start()
        gx[m, keep_dst, at] = dpx[keep_src, at]
        dksum[...] += mm_nt(vef_ref[j], rb) + mm_nt(veb_ref[j], lb)
        drsum[...] += mm_nt(dyef_ref[j], ra) + mm_nt(dyeb_ref[j], la)
        dlev[...] += split_mm(dy * (mr - ml) + v * (dr - dl), onehot)
        sdt[...] += split_mm(u * dv, onehot)
        over = lb.astype(f32) * rout[j, 0].astype(f32) + la.astype(f32) * rout[j, 1].astype(f32)
        over = jnp.broadcast_to(jnp.sum(over, axis=0, keepdims=True), (8, LANES))
        cross[...] += split_mm(over, onehot)

    def chain(name, j, into_ref, own_ref, out_ref, head, tail, step):
        item = copy(out_ref.at[j], into_ref.at[j], name, j, "sp", near(step))

        @pl.when(jnp.logical_not(head))
        def _():
            item.wait_recv()

        decay = tdec[j][0:1, :]
        for q in range(2):
            out_ref[j, q] = (own_ref[j, q] + decay * into_ref[j, q].astype(f32)).astype(bf16)

        @pl.when(jnp.logical_not(tail))
        def _():
            item.start()

    delay = SKEW * (chunks - 1)

    @pl.loop(0, pairs + delay)
    def _(tick):
        @pl.when(tick < pairs)
        def _():
            sr_ref[tick, 0] = mm(kt[...], veb_ref[tick])
            sr_ref[tick, 1] = mm(rt[...], dyeb_ref[tick])
            sl_ref[tick, 0] = mm(kt[...], vef_ref[tick])
            sl_ref[tick, 1] = mm(rt[...], dyef_ref[tick])

        jr = tick - SKEW * c

        @pl.when(jnp.logical_and(jr >= 0, jr < pairs))
        def _():
            chain("right", jr, rin, sr_ref, rout, first, last, GROUPS)

        jl = tick - SKEW * (chunks - 1 - c)

        @pl.when(jnp.logical_and(jl >= 0, jl < pairs))
        def _():
            chain("left", jl, lin, sl_ref, lout, last, first, -GROUPS)

        @pl.when(tick < pairs)
        def _():
            intra(tick)

        @pl.when(tick == pairs - 1)
        def _():
            ge = gesum[...].astype(bf16)
            dksum[...] += mm(ge, rn[...])
            drsum[...] += mm_tn(ge, kn[...])

        @pl.when(tick >= delay)
        def _():
            consume(tick - delay)

    sbc = sbc_ref[...]
    dpbc[:, :STATE] = (dksum[...] * sbc[:, :STATE]).astype(bf16)
    dpbc[:, STATE:] = (drsum[...] * sbc[:, STATE:]).astype(bf16)
    gbc_copy = go(
        copy(
            dpbc.at[pl.ds(pl.multiple_of(p * (tokens - HALO), HALO), tokens + HALO), :],
            gbc.at[m, pl.ds(pl.multiple_of(HALO - HALO * p, HALO), tokens + HALO), :],
            "gbc",
            0,
            "sp",
            partner,
        )
    )

    def send_edges(name, source, target):
        go(
            copy(
                source.at[ch - HALO :, :],
                target.at[m, :HALO, :],
                name + "_left",
                0,
                "sp",
                lax.rem((c + 1) * GROUPS, sp),
                into=m,
            ),
            jnp.logical_not(last),
        )
        go(
            copy(
                source.at[:HALO, :],
                target.at[m, HALO + tokens :, :],
                name + "_right",
                0,
                "sp",
                lax.rem(c * GROUPS - 1 + sp, sp),
                into=m,
            ),
            jnp.logical_not(first),
        )

    def await_edges(name, target):
        lead, trail = m == 0, m == GROUPS - 1
        for g in range(GROUPS):
            slot = target.at[g, :HALO, :]
            arrive(
                copy(slot, slot, name + "_left", g, "sp", partner),
                jnp.logical_and(lead, jnp.logical_not(first)),
            )
            slot = target.at[g, HALO + tokens :, :]
            arrive(
                copy(slot, slot, name + "_right", g, "sp", partner),
                jnp.logical_and(trail, jnp.logical_not(last)),
            )

        @pl.when(jnp.logical_and(lead, first))
        def _():
            target[:, :HALO, :] = jnp.zeros((GROUPS, HALO, target.shape[2]), bf16)

        @pl.when(jnp.logical_and(trail, last))
        def _():
            target[:, HALO + tokens :, :] = jnp.zeros((GROUPS, HALO, target.shape[2]), bf16)

    send_edges("gbc", dpbc, gbc)
    send_edges("gx", dpx, gx)
    gbc[m, keep_dst, :] = dpbc[keep_src, :]

    fill = jnp.zeros((LANES - gh, ch), f32)
    down = jnp.concatenate([colrow[...], fill], axis=0).T
    drate = jnp.dot(upper, dlev[...] - down, precision=highest, preferred_element_type=f32)
    drate = (drate - cross[0:1, :]).T[:gh]
    ddt = ((drate * twice(faderow[...]) + sdt[...].T[:gh]) * sigrow[...]).astype(bf16)
    for g in range(GROUPS):
        ddtsend[g] = ddt[:, g * tokens : (g + 1) * tokens]
    group_rows = pl.ds(pl.multiple_of(m * gh, gh), gh)
    ddt_copy = go(copy(ddtsend.at[p], ddt_ref.at[group_rows, :], "ddt", 0, "sp", partner))
    ddt_ref[group_rows, :] = ddtsend[m]

    arrive(gbc_copy)
    await_edges("gbc", gbc)
    for g in range(GROUPS):
        for q in range(2):
            at = slice(g * STATE, (g + 1) * STATE)
            taps = (tapb_ref, tapc_ref)[q][:, at]
            part = gbc[g, :, q * STATE : (q + 1) * STATE].astype(f32)
            to = q * latent + g * STATE
            gsend[:, to : to + STATE] = window_conv(part, taps, tokens, True).astype(bf16)

    g_y = []
    for o in range(1, ny):
        peer = lax.rem(y + o, ny) * cores + core
        g_y.append(go(copy(gsend, gall.at[me_dp], "g_y", o, "dp", peer)))
    g_core = None
    if cores > 1:
        g_core = go(copy(gsend, gall.at[me_dp], "g_core", 0, "dp", other_core))
    gall[me_dp] = gsend[...]
    gb, gc = gsend[:, :latent], gsend[:, latent:]
    for i in range(dp):
        dh_ref[:, i * cw : (i + 1) * cw] = (mm_nt(gb, wball[i]) + mm_nt(gc, wcall[i])).astype(bf16)
    for item in la_copies:
        arrive(item)
    g_fwd = []
    for o in range(1, ny):
        src = lax.rem(y - o + ny, ny) * cores + core
        arrive(g_y[o - 1])
        if cores > 1:
            g_fwd.append(go(copy(gall.at[src], gall.at[src], "g_fwd", o, "dp", other_core)))
    if cores > 1:
        arrive(g_core)
    for item in g_fwd:
        arrive(item)

    w1 = []
    for q in range(2):
        total = None
        for i in range(dp):
            term = mm_tn(cols[i], gall[i, :, q * latent : (q + 1) * latent])
            total = term if total is None else total + term
        total = total.reshape(GROUPS, chunks, rows, latent)
        wsend[q] = total.astype(bf16)
        w1.append(go(copy(wsend.at[q, p], w1in.at[q], "w1", q, "sp", partner)))

    def input_gradient(g):
        @pl.loop(0, pairs)
        def _(j):
            taps = tapall[:, lanes(g * pairs + j, LANES)]
            part = gx[g, :, lanes(j, LANES)].astype(f32)
            dx_ref[:, lanes(g * pairs + j, LANES)] = window_conv(part, taps, tokens, True).astype(
                bf16
            )

    @pl.loop(0, pairs)
    def _(j):
        gx_copy(j).wait_recv()

    await_edges("gx", gx)
    w2 = []
    for q in range(2):
        arrive(w1[q])
        part = wsend[q, m].astype(f32) + w1in[q].astype(f32)
        s1send[q] = part.astype(bf16)
        for o in range(1, chunks):
            k = lax.rem(c + o, chunks)
            w2.append(
                go(
                    copy(
                        s1send.at[q, k],
                        w2in.at[q, c],
                        "w2",
                        q * chunks + o,
                        "sp",
                        k * GROUPS + m,
                    )
                )
            )
        wown[q] = s1send[q, c].astype(f32)
    input_gradient(0)
    w3 = []
    for q in range(2):
        share = wown[q]
        for o in range(1, chunks):
            arrive(w2[q * (chunks - 1) + o - 1])
            share = share + w2in[q, lax.rem(c - o + chunks, chunks)].astype(f32)
        s3send[q] = share.astype(bf16)
        tall[q, m, c] = s3send[q]
        for o in range(1, chunks):
            k = lax.rem(c + o, chunks)
            w3.append(
                go(
                    copy(
                        s3send.at[q],
                        tall.at[q, m, c],
                        "w3",
                        q * chunks + o,
                        "sp",
                        k * GROUPS + m,
                    )
                )
            )
    input_gradient(1)
    w4 = []
    for q in range(2):
        for o in range(1, chunks):
            arrive(w3[q * (chunks - 1) + o - 1])
        w4.append(go(copy(tall.at[q, m], tall.at[q, m], "w4", q, "sp", partner)))
    arrive(ddt_copy)
    for item in w4:
        arrive(item)

    @pl.loop(0, pairs)
    def _(j):
        gx_copy(j).wait_send()

        @pl.when(jnp.logical_not(last))
        def _():
            copy(rout.at[j], rin.at[j], "right", j, "sp", near(GROUPS)).wait_send()

        @pl.when(jnp.logical_not(first))
        def _():
            copy(lout.at[j], lin.at[j], "left", j, "sp", near(-GROUPS)).wait_send()

    for item, cond in sent:
        if cond is None:
            item.wait_send()
        else:

            @pl.when(cond)
            def _():
                item.wait_send()


def out_kernel(dgate, dx, dh, tall, dgate_out, dx_out, dh_out, dwb_out, dwc_out):
    dgate_out[...] = dgate[...]
    dx_out[...] = dx[...]
    dh_out[...] = dh[...]
    dwb_out[...] = tall[0].astype(f32).reshape(dwb_out.shape)
    dwc_out[...] = tall[1].astype(f32).reshape(dwc_out.shape)


def local(
    layer_activity,
    writer_matrix,
    reader_matrix,
    source_unfiltered,
    switch_raw_signal,
    saved_result,
    final_adjoint,
    delta_raw,
    extra_logdrop,
    source_filter_coefs,
    writer_filter_coefs,
    reader_filter_coefs,
    delta_offset,
    fading_exponents,
    direct_factor,
    rescale_factor,
):
    tokens, width_in = layer_activity.shape[1:]
    inner = source_unfiltered.shape[2]
    dp = lax.axis_size("dp")
    sp = lax.axis_size("sp")
    cores = 2 if dp % 2 == 0 else 1
    heads = delta_offset.shape[0]
    cw, latent = writer_matrix.shape
    xc = heads * HEAD_DIM
    xw = -(-xc // LANES) * LANES
    rows_h = -(-heads // 8) * 8
    chunks = sp // GROUPS
    ch = tokens * GROUPS
    gw = inner // GROUPS
    gh = HEADS // GROUPS
    pairs = gw // LANES
    rows = cw // sp
    window = tokens * sp
    _, slots = slot_table(sp, dp, cores, pairs)

    vmem = pl.BlockSpec(memory_space=pltpu.VMEM)
    smem = pl.BlockSpec(memory_space=pltpu.SMEM)
    scratch = [
        ((dp, cw, latent), bf16),
        ((dp, cw, latent), bf16),
        ((dp, tokens, cw), bf16),
        ((ch + 2 * HALO, gw), bf16),
        ((ch, gw), bf16),
        ((tokens, gw), bf16),
        ((gh, ch), bf16),
        ((chunks, rows_h, ch + 2 * LANES), f32),
        ((chunks, rows_h, ch + 2 * LANES), f32),
        ((gh, ch + 2 * LANES), f32),
        ((8, xw), f32),
        ((sp, 8, xw), f32),
        ((8, inner), f32),
        ((GROUPS, tokens, 2 * STATE), bf16),
        ((ch + 2 * HALO, 2 * STATE), bf16),
        ((pairs, ch, LANES), f32),
        ((pairs, ch, LANES), f32),
        ((pairs, ch, LANES), f32),
        ((pairs, ch, LANES), f32),
        ((pairs, ch, LANES), f32),
        ((pairs, 8, LANES), f32),
        ((pairs, ch, LANES), bf16),
        ((pairs, ch, LANES), bf16),
        ((pairs, ch, LANES), bf16),
        ((pairs, ch, LANES), bf16),
        ((pairs, ch, LANES), bf16),
        ((ch, STATE), bf16),
        ((ch, STATE), bf16),
        ((STATE, ch), bf16),
        ((STATE, ch), bf16),
        ((ch, 2 * STATE), f32),
        ((ch, ch), f32),
        ((ch, ch), f32),
        ((ch, ch), f32),
        ((gh, ch, LANES), f32),
        ((gh, ch), f32),
        ((gh, ch), f32),
        ((gh, LANES), f32),
        ((pairs, ch, LANES), f32),
        ((pairs, 2, STATE, LANES), f32),
        ((pairs, 2, STATE, LANES), f32),
        ((pairs, 2, STATE, LANES), bf16),
        ((pairs, 2, STATE, LANES), bf16),
        ((pairs, 2, STATE, LANES), bf16),
        ((pairs, 2, STATE, LANES), bf16),
        ((ch, STATE), f32),
        ((ch, STATE), f32),
        ((ch, LANES), f32),
        ((ch, LANES), f32),
        ((8, LANES), f32),
        ((gh, ch), f32),
        ((ch, gw), bf16),
        ((GROUPS, tokens + 2 * HALO, gw), bf16),
        ((ch, 2 * STATE), bf16),
        ((GROUPS, tokens + 2 * HALO, 2 * STATE), bf16),
        ((GROUPS, gh, tokens), bf16),
        ((tokens, 2 * latent), bf16),
        ((dp, tokens, 2 * latent), bf16),
        ((2, GROUPS, chunks, rows, latent), bf16),
        ((2, rows, latent), f32),
        ((2, chunks, rows, latent), bf16),
        ((2, chunks, rows, latent), bf16),
        ((2, chunks, rows, latent), bf16),
        ((2, rows, latent), bf16),
    ]
    dgate, dx, ddt, dh, tall = pl.pallas_call(
        functools.partial(mega_kernel, heads, cores),
        in_specs=[vmem] * 13 + [smem] * 3,
        out_specs=[vmem] * 5,
        out_shape=[
            jax.ShapeDtypeStruct((tokens, inner), bf16),
            jax.ShapeDtypeStruct((tokens, inner), bf16),
            jax.ShapeDtypeStruct((HEADS, tokens), bf16),
            jax.ShapeDtypeStruct((tokens, width_in), bf16),
            jax.ShapeDtypeStruct((2, GROUPS, chunks, rows, latent), bf16),
        ],
        scratch_shapes=[pltpu.VMEM(shape, kind) for shape, kind in scratch]
        + [pltpu.SemaphoreType.DMA((slots,)), pltpu.SemaphoreType.DMA((slots,))],
        compiler_params=pltpu.CompilerParams(
            collective_id=0, has_side_effects=True, vmem_limit_bytes=60 * 1024 * 1024
        ),
        name="mega",
    )(
        layer_activity.reshape(tokens, width_in),
        writer_matrix,
        reader_matrix,
        source_unfiltered.reshape(tokens, inner),
        switch_raw_signal.reshape(tokens, inner),
        saved_result.reshape(tokens, inner),
        final_adjoint.reshape(tokens, inner),
        delta_raw.reshape(tokens, HEADS).T,
        extra_logdrop.reshape(window, heads).T,
        source_filter_coefs,
        writer_filter_coefs,
        reader_filter_coefs,
        rescale_factor.reshape(1, inner),
        delta_offset,
        fading_exponents,
        direct_factor,
    )
    d_gate, d_x, d_hidden, d_w_b, d_w_c = pl.pallas_call(
        out_kernel,
        in_specs=[vmem] * 4,
        out_specs=[vmem] * 5,
        out_shape=[
            jax.ShapeDtypeStruct((tokens, inner), bf16),
            jax.ShapeDtypeStruct((tokens, inner), bf16),
            jax.ShapeDtypeStruct((tokens, width_in), bf16),
            jax.ShapeDtypeStruct((cw, latent), f32),
            jax.ShapeDtypeStruct((cw, latent), f32),
        ],
        name="outputs",
    )(dgate, dx, dh, tall)
    return (
        d_hidden.reshape(1, tokens, width_in),
        d_x.reshape(1, tokens, inner),
        d_gate.reshape(1, tokens, inner),
        ddt.T.reshape(1, tokens, HEADS),
        d_w_b,
        d_w_c,
    )


def solution(mesh):
    in_specs = (
        P("dp", "sp", None),
        P("dp", None),
        P("dp", None),
        P("dp", "sp", None),
        P("dp", "sp", None),
        P("dp", "sp", None),
        P("dp", "sp", None),
        P("dp", "sp", None),
        P("dp", None, "sp"),
        P(None, "sp"),
        P(),
        P(),
        P("sp"),
        P("sp"),
        P("sp"),
        P(),
    )
    out_specs = (
        P("dp", "sp", None),
        P("dp", "sp", None),
        P("dp", "sp", None),
        P("dp", "sp", None),
        P("dp", None),
        P("dp", None),
    )
    return jax.shard_map(local, mesh=mesh, in_specs=in_specs, out_specs=out_specs, check_vma=False)
```

```python
import functools

import jax
import jax.numpy as jnp
from jax import lax
from jax.experimental import pallas as pl
from jax.experimental.pallas import tpu as pltpu
from jax.sharding import PartitionSpec as P

HEADS = 32
HEAD_DIM = 64
STATE = 128
GROUPS = 2
NORM_GROUPS = 8
CONV_K = 5
LANES = 128
HALO = 16
SKEW = 2
EPSILON = 1e-06
LOG2E = 1.4426950408889634
highest = lax.Precision.HIGHEST
f32 = jnp.float32
bf16 = jnp.bfloat16
NT = (((1,), (1,)), ((), ()))
TN = (((0,), (0,)), ((), ()))


def sigmoid(v):
    return 1.0 / (1.0 + jnp.exp(-v))


def softplus(v):
    e = jnp.exp(-jnp.abs(v))
    z = e / (2.0 + e)
    z2 = z * z
    series = jnp.full_like(z, 1.0 / 17.0)
    for odd in (15, 13, 11, 9, 7, 5, 3, 1):
        series = series * z2 + 1.0 / odd
    return jnp.maximum(v, 0.0) + 2.0 * z * series


def mm(a, b):
    return jnp.dot(a, b, preferred_element_type=f32)


def mm_nt(a, b):
    return lax.dot_general(a, b, NT, preferred_element_type=f32)


def mm_tn(a, b):
    return lax.dot_general(a, b, TN, preferred_element_type=f32)


def split_mm(a, b):
    hi = a.astype(bf16)
    lo = (a - hi.astype(f32)).astype(bf16)
    return mm(hi, b) + mm(lo, b)


def window_conv(rows, taps, count, flip):
    total = None
    for k in range(CONV_K):
        shift = HALO - CONV_K // 2 + k
        tap = taps[CONV_K - 1 - k if flip else k][None, :]
        term = tap * pltpu.roll(rows, rows.shape[0] - shift, axis=0)[:count]
        total = term if total is None else total + term
    return total


def greet(axes):
    barrier = pltpu.get_barrier_semaphore()
    count = 0
    for axis in axes:
        size = lax.axis_size(axis)
        me = lax.axis_index(axis)
        for o in range(1, size):
            pl.semaphore_signal(
                barrier,
                inc=1,
                device_id={axis: lax.rem(me + o, size)},
                device_id_type=pl.DeviceIdType.MESH,
            )
            count += 1
    pl.semaphore_wait(barrier, count)


class Phases:
    def __init__(self):
        self.scope = None

    def __call__(self, name):
        self.end()
        self.scope = jax.named_scope(name)
        self.scope.__enter__()

    def end(self):
        if self.scope is not None:
            self.scope.__exit__(None, None, None)
            self.scope = None


def slot_table(sp, dp, cores, pairs):
    ny = dp // cores
    chunks = sp // GROUPS
    counts = (
        ("w_y", 2 * ny),
        ("w_core", 2),
        ("w_fwd", 2 * ny),
        ("la", dp),
        ("x", 1),
        ("x_left", GROUPS),
        ("x_right", GROUPS),
        ("dt", 1),
        ("drop", chunks),
        ("tap", sp),
        ("dy", NORM_GROUPS),
        ("bc", 1),
        ("bc_left", GROUPS),
        ("bc_right", GROUPS),
        ("right", 2 * pairs),
        ("left", 2 * pairs),
        ("gx", pairs),
        ("gx_left", GROUPS),
        ("gx_right", GROUPS),
        ("gbc", 1),
        ("gbc_left", GROUPS),
        ("gbc_right", GROUPS),
        ("ddt", 1),
        ("g_y", 2 * ny),
        ("g_core", 2),
        ("g_fwd", 2 * ny),
        ("w1", 2),
        ("w2", 2 * chunks),
        ("w3", 2 * chunks),
        ("w4", 2),
    )
    table = {}
    at = 0
    for name, count in counts:
        table[name] = at
        at += count
    return table, at


def mega_kernel(
    heads,
    cores,
    la_hbm,
    wb_hbm,
    wc_hbm,
    x_hbm,
    gates_hbm,
    values_hbm,
    adjoint_hbm,
    dt_ref,
    drop_ref,
    tapx_ref,
    tapb_ref,
    tapc_ref,
    scale_ref,
    offset_ref,
    fade_ref,
    skip_ref,
    dgate_ref,
    dx_ref,
    ddt_ref,
    dh_ref,
    tall,
    la_ref,
    wb_ref,
    wc_ref,
    x_ref,
    gates_ref,
    values_ref,
    adjoint_ref,
    wball,
    wcall,
    cols,
    xin,
    dyin,
    dysend,
    dtin,
    dropsend,
    dropin,
    drow,
    tapsend,
    tapin,
    tapall,
    bcsend,
    bcin,
    u_ref,
    sux_ref,
    dts_ref,
    ef_ref,
    eb_ref,
    tdec,
    vb_ref,
    vef_ref,
    veb_ref,
    dyef_ref,
    dyeb_ref,
    kn,
    rn,
    kt,
    rt,
    sbc_ref,
    score_ref,
    sign_ref,
    gesum,
    lcolb,
    lrow,
    sigrow,
    faderow,
    dv_ref,
    sr_ref,
    sl_ref,
    rin,
    lin,
    rout,
    lout,
    dksum,
    drsum,
    dlev,
    sdt,
    cross,
    colrow,
    dpx,
    gx,
    dpbc,
    gbc,
    ddtsend,
    gsend,
    gall,
    wsend,
    wown,
    w1in,
    s1send,
    w2in,
    s3send,
    ss,
    rs,
    ls,
):
    dp = lax.axis_size("dp")
    sp = lax.axis_size("sp")
    me_dp = lax.axis_index("dp")
    me_sp = lax.axis_index("sp")
    ny = dp // cores
    chunks = sp // GROUPS
    y = me_dp // cores
    core = lax.rem(me_dp, cores)
    c = me_sp // GROUPS
    m = lax.rem(me_sp, GROUPS)
    p = GROUPS - 1 - m
    partner = c * GROUPS + p
    other_core = y * cores + (cores - 1 - core)
    tokens, inner = x_ref.shape
    gw = inner // GROUPS
    gh = HEADS // GROUPS
    ch = tokens * GROUPS
    pairs = gw // LANES
    cw = wb_ref.shape[0]
    latent = wb_ref.shape[1]
    xc = heads * HEAD_DIM
    nsrc = sp // GROUPS
    rows = cw // sp
    first = c == 0
    last = c == chunks - 1
    table, _ = slot_table(sp, dp, cores, pairs)
    sent = []

    def copy(src, dst, name, index, axis, peer, into=None):
        at = table[name]
        return pltpu.make_async_remote_copy(
            src_ref=src,
            dst_ref=dst,
            send_sem=ss.at[at + index],
            recv_sem=rs.at[at + (index if into is None else into)],
            device_id={axis: peer},
            device_id_type=pl.DeviceIdType.MESH,
        )

    def go(item, cond=None):
        if cond is None:
            item.start()
        else:

            @pl.when(cond)
            def _():
                item.start()

        sent.append((item, cond))
        return item

    def arrive(item, cond=None):
        if cond is None:
            item.wait_recv()
        else:

            @pl.when(cond)
            def _():
                item.wait_recv()

    def lanes(index, width):
        return pl.ds(pl.multiple_of(index * width, LANES), width)

    def near(step):
        return lax.rem(me_sp + step + 2 * sp, sp)

    mine = pl.ds(pl.multiple_of(HALO + m * tokens, HALO), tokens)
    mine0 = pl.ds(pl.multiple_of(m * tokens, HALO), tokens)
    body = slice(HALO, HALO + ch)
    left_rows = slice(0, HALO)
    right_rows = slice(HALO + ch, 2 * HALO + ch)
    to_right = jnp.logical_and(m == GROUPS - 1, jnp.logical_not(last))
    to_left = jnp.logical_and(m == 0, jnp.logical_not(first))

    phase = Phases()
    phase("greet")
    loads = {}
    for at, (source, target) in enumerate(
        (
            (wb_hbm, wb_ref),
            (wc_hbm, wc_ref),
            (x_hbm, x_ref),
            (values_hbm, values_ref),
            (gates_hbm, gates_ref),
            (adjoint_hbm, adjoint_ref),
            (la_hbm, la_ref),
        )
    ):
        loads[at] = pltpu.make_async_copy(source, target, ls.at[at])
        loads[at].start()
    greet(("dp", "sp"))
    loads[0].wait()
    loads[1].wait()

    phase("send_first")
    w_y = []
    for o in range(1, ny):
        peer = lax.rem(y + o, ny) * cores + core
        w_y.append(
            (
                go(copy(wb_ref, wball.at[me_dp], "w_y", 2 * o, "dp", peer)),
                go(copy(wc_ref, wcall.at[me_dp], "w_y", 2 * o + 1, "dp", peer)),
            )
        )
    w_core = []
    if cores > 1:
        w_core = [
            go(copy(wb_ref, wball.at[me_dp], "w_core", 0, "dp", other_core)),
            go(copy(wc_ref, wcall.at[me_dp], "w_core", 1, "dp", other_core)),
        ]
    loads[2].wait()
    x_copy = go(copy(x_ref.at[:, lanes(p, gw)], xin.at[mine, :], "x", 0, "sp", partner))
    dt_copy = go(
        copy(
            dt_ref.at[pl.ds(pl.multiple_of(p * gh, gh), gh), :],
            dtin.at[:, lanes(m, tokens)],
            "dt",
            0,
            "sp",
            partner,
        )
    )

    def send_halo(name, source, target):
        for g in range(GROUPS):
            go(
                copy(
                    source(g, slice(tokens - HALO, tokens)),
                    target.at[left_rows, :],
                    name + "_left",
                    g,
                    "sp",
                    near(1 + g),
                    into=0,
                ),
                to_right,
            )
            go(
                copy(
                    source(g, slice(0, HALO)),
                    target.at[right_rows, :],
                    name + "_right",
                    g,
                    "sp",
                    near(g - GROUPS),
                    into=0,
                ),
                to_left,
            )

    def await_halo(name, target):
        arrive(
            copy(target.at[left_rows, :], target.at[left_rows, :], name + "_left", 0, "sp", partner),
            jnp.logical_not(first),
        )
        arrive(
            copy(target.at[right_rows, :], target.at[right_rows, :], name + "_right", 0, "sp", partner),
            jnp.logical_not(last),
        )

        @pl.when(first)
        def _():
            target[left_rows, :] = jnp.zeros((HALO, target.shape[1]), bf16)

        @pl.when(last)
        def _():
            target[right_rows, :] = jnp.zeros((HALO, target.shape[1]), bf16)

    send_halo("x", lambda g, r: x_ref.at[r, g * gw : (g + 1) * gw], xin)

    phase("params")
    rows_h = dropsend.shape[1]
    head_row = lax.broadcasted_iota(jnp.int32, (rows_h, LANES), 0)
    offsets = jnp.zeros((rows_h, LANES), f32)
    fades = jnp.zeros((rows_h, LANES), f32)
    for h in range(heads):
        offsets = jnp.where(head_row == h, offset_ref[h], offsets)
        fades = jnp.where(head_row == h, fade_ref[h], fades)
    dropsend[...] = jnp.zeros_like(dropsend)
    for k in range(chunks):
        dropsend[k, :heads, :ch] = drop_ref[:, k * ch : (k + 1) * ch]
        dropsend[k, :, ch : ch + LANES] = offsets
        dropsend[k, :, ch + LANES :] = fades
    owner = (me_sp * heads) // gh
    place = me_sp - owner * nsrc
    for o in range(chunks):
        k = lax.rem(c + o, chunks)
        go(
            copy(
                dropsend.at[k],
                dropin.at[place],
                "drop",
                o,
                "sp",
                k * GROUPS + owner if o else partner,
                into=place,
            ),
            None if o else owner != m,
        )

    @pl.when(owner == m)
    def _():
        dropin[place] = dropsend[c]

    xw = tapsend.shape[1]
    tap_lane = lax.broadcasted_iota(jnp.int32, (1, xw), 1) // HEAD_DIM
    skips = jnp.zeros((1, xw), f32)
    for h in range(heads):
        skips = jnp.where(tap_lane == h, skip_ref[h], skips)
    tapsend[...] = jnp.zeros_like(tapsend)
    tapsend[:CONV_K, :xc] = tapx_ref[...]
    tapsend[CONV_K : CONV_K + 1, :] = skips
    tap_copies = []
    for o in range(1, sp):
        tap_copies.append(go(copy(tapsend, tapin.at[me_sp], "tap", o, "sp", lax.rem(me_sp + o, sp))))
    tapin[me_sp] = tapsend[...]
    loads[6].wait()
    la_copies = []
    for o in range(1, dp):
        peer = lax.rem(me_dp + o, dp)
        la_copies.append(
            go(copy(la_ref.at[:, lanes(peer, cw)], cols.at[me_dp], "la", o, "dp", peer))
        )
    cols[me_dp] = la_ref[:, lanes(me_dp, cw)]
    xin[mine, :] = x_ref[:, lanes(m, gw)]
    dtin[:, lanes(m, tokens)] = dt_ref[pl.ds(pl.multiple_of(m * gh, gh), gh), :]

    phase("norm")
    width = inner // NORM_GROUPS
    per_half = NORM_GROUPS // GROUPS
    dy_copies = []
    for at in (3, 4, 5):
        loads[at].wait()
    for half in range(GROUPS):
        who = p if half == 0 else m
        for i in range(per_half):
            span = lanes(who * per_half + i, width)
            values = values_ref[:, span].astype(f32)
            gates = gates_ref[:, span].astype(f32)
            sig = sigmoid(gates)
            act = gates * sig
            g = values * act
            dn = adjoint_ref[:, span].astype(f32) * scale_ref[:, span]
            inv = lax.rsqrt(jnp.sum(g * g, axis=1, keepdims=True) * (1.0 / width) + EPSILON)
            along = jnp.sum(dn * g, axis=1, keepdims=True) * (1.0 / width)
            dg = inv * dn - g * (inv * inv * inv * along)
            dgate_ref[:, span] = (dg * values * (sig + act * (1.0 - sig))).astype(bf16)
            dy = (dg * act).astype(bf16)
            at = slice(i * width, (i + 1) * width)
            if half == 0:
                dysend[:, at] = dy
                dy_copies.append(
                    go(copy(dysend.at[:, at], dyin.at[mine0, at], "dy", i, "sp", partner))
                )
            else:
                dyin[mine0, at] = dy

    phase("levels")
    arrive(dt_copy)
    for i in range(nsrc):
        arrive(
            copy(dropsend.at[0], dropin.at[i], "drop", i, "sp", partner), m * nsrc + i != me_sp
        )
        drow[i * heads : (i + 1) * heads, :] = dropin[i, :heads, :]
    twice = lambda v: jnp.concatenate([v] * (ch // LANES), axis=1)
    fade = jnp.exp(drow[:, ch + LANES :])
    a = dtin[...].astype(f32) + twice(drow[:, ch : ch + LANES])
    dt = softplus(a)
    sigrow[...] = sigmoid(a)
    faderow[...] = fade
    rate = dt * twice(fade) + drow[:, :ch]
    row_i = lax.broadcasted_iota(jnp.int32, (ch, ch), 0)
    col_i = lax.broadcasted_iota(jnp.int32, (ch, ch), 1)
    upper = (row_i <= col_i).astype(f32)
    level = jnp.dot(rate, upper, precision=highest, preferred_element_type=f32) * LOG2E
    lrow[...] = level
    fill = jnp.zeros((LANES - gh, ch), f32)
    lcol = jnp.concatenate([level, fill], axis=0).T
    dtcol = jnp.concatenate([dt, fill], axis=0).T
    low_lane = lax.broadcasted_iota(jnp.int32, (ch, LANES), 1) < HEAD_DIM
    for j in range(pairs):
        pair = []
        for h in (2 * j, 2 * j + 1):
            wide = jnp.broadcast_to(lcol[:, h : h + 1], (ch, LANES))
            lcolb[h] = wide
            pair.append(wide)
        spread = jnp.where(low_lane, pair[0], pair[1])
        end = spread[ch - 1 : ch, :]
        ef_ref[j] = jnp.exp2(-spread)
        eb_ref[j] = jnp.exp2(spread - end)
        tdec[j] = jnp.broadcast_to(jnp.exp2(-end), (8, LANES))
        dts_ref[j] = jnp.where(low_lane, dtcol[:, 2 * j : 2 * j + 1], dtcol[:, 2 * j + 1 : 2 * j + 2])

    phase("wait_x")
    for item in tap_copies:
        arrive(item)
    if xc % LANES == 0:
        for i in range(sp):
            tapall[:, i * xc : (i + 1) * xc] = tapin[i]
    else:
        per = LANES // xc
        for i in range(inner // LANES):
            tapall[:, i * LANES : (i + 1) * LANES] = jnp.concatenate(
                [tapin[i * per + q][:, :xc] for q in range(per)], axis=1
            )
    arrive(x_copy)
    await_halo("x", xin)

    phase("prep_x")
    @pl.loop(0, pairs)
    def _(j):
        taps = tapall[:, lanes(m * pairs + j, LANES)]
        pre = window_conv(xin[:, lanes(j, LANES)].astype(f32), taps, ch, False)
        sig = sigmoid(pre)
        u = pre * sig
        u_ref[j] = u
        sux_ref[j] = sig + u * (1.0 - sig)
        v = u * dts_ref[j]
        vb_ref[j] = v.astype(bf16)
        vef_ref[j] = (v * ef_ref[j]).astype(bf16)
        veb_ref[j] = (v * eb_ref[j]).astype(bf16)

    phase("project")
    wball[me_dp] = wb_ref[...]
    wcall[me_dp] = wc_ref[...]

    def project(total, index):
        part = la_ref[:, lanes(index, cw)]
        tb, tc = mm(part, wball[index]), mm(part, wcall[index])
        return (tb, tc) if total is None else (total[0] + tb, total[1] + tc)

    total = project(None, me_dp)
    for item in w_core:
        arrive(item)
    if cores > 1:
        total = project(total, other_core)
    w_fwd = []
    for o in range(1, ny):
        src = lax.rem(y - o + ny, ny) * cores + core
        for q in range(2):
            arrive(w_y[o - 1][q])
            if cores > 1:
                full = (wball, wcall)[q].at[src]
                w_fwd.append(go(copy(full, full, "w_fwd", 2 * o + q, "dp", other_core)))
        total = project(total, src)
    for o in range(1, ny):
        if cores > 1:
            arrive(w_fwd[2 * o - 2])
            arrive(w_fwd[2 * o - 1])
            total = project(total, lax.rem(y - o + ny, ny) * cores + cores - 1 - core)
    proj_b, proj_c = total[0].astype(bf16), total[1].astype(bf16)
    for g in range(GROUPS):
        bcsend[g, :, :STATE] = proj_b[:, g * STATE : (g + 1) * STATE]
        bcsend[g, :, STATE:] = proj_c[:, g * STATE : (g + 1) * STATE]
    bc_copy = go(copy(bcsend.at[p], bcin.at[mine, :], "bc", 0, "sp", partner))
    send_halo("bc", lambda g, r: bcsend.at[g, r, :], bcin)
    bcin[mine, :] = bcsend[m]

    phase("wait_dy")
    for item in dy_copies:
        arrive(item)

    @pl.loop(0, pairs)
    def _(j):
        dy = dyin[:, lanes(j, LANES)].astype(f32)
        dyef_ref[j] = (dy * ef_ref[j]).astype(bf16)
        dyeb_ref[j] = (dy * eb_ref[j]).astype(bf16)

    phase("wait_bc")
    arrive(bc_copy)
    await_halo("bc", bcin)
    phase("conv_bc")
    for q in range(2):
        taps = (tapb_ref, tapc_ref)[q][:, lanes(m, STATE)]
        at = slice(q * STATE, (q + 1) * STATE)
        pre = window_conv(bcin[:, at].astype(f32), taps, ch, False)
        sig = sigmoid(pre)
        kr = pre * sig
        sbc_ref[:, at] = sig + kr * (1.0 - sig)
        (kn, rn)[q][...] = kr.astype(bf16)
        (kt, rt)[q][...] = kr.T.astype(bf16)
    score = mm_nt(kn[...], rn[...])
    score_ref[...] = score
    sign_ref[...] = score * jnp.clip(col_i - row_i, -1, 1).astype(f32)

    gesum[...] = jnp.zeros_like(gesum)
    dksum[...] = jnp.zeros_like(dksum)
    drsum[...] = jnp.zeros_like(drsum)
    dlev[...] = jnp.zeros_like(dlev)
    sdt[...] = jnp.zeros_like(sdt)
    cross[...] = jnp.zeros_like(cross)

    @pl.when(first)
    def _():
        rin[...] = jnp.zeros_like(rin)

    @pl.when(last)
    def _():
        lin[...] = jnp.zeros_like(lin)

    lane_low = lax.broadcasted_iota(jnp.int32, (1, LANES), 1) < HEAD_DIM
    masks = (lane_low.astype(bf16), 1.0 - lane_low.astype(bf16))
    pick_lane = lax.broadcasted_iota(jnp.int32, (LANES, LANES), 1)
    pick_half = lax.broadcasted_iota(jnp.int32, (LANES, LANES), 0) // HEAD_DIM
    block = min(ch, LANES)

    def intra(j):
        dyj = dyin[:, lanes(j, LANES)]
        for a in range(2):
            h = 2 * j + a
            lr = lrow[pl.ds(h, 1), :]
            dym = dyj * masks[a]
            onehot = (pick_lane == h).astype(bf16)
            below = None
            for b in range(ch // block):
                at = slice(b * block, (b + 1) * block)
                gap = twice(lcolb[h, at]) - lr
                decay = jnp.exp2(-jnp.abs(gap))
                ge = mm_nt(vb_ref[j, at] * masks[a], dyj) * decay
                gesum[at, :] += ge
                part = mm((score_ref[at, :] * decay).astype(bf16), dym)
                if a == 0:
                    dv_ref[j, at] = part
                else:
                    dv_ref[j, at] += part
                q = sign_ref[at, :] * ge
                down = jnp.sum(q, axis=0, keepdims=True)
                below = down if below is None else below + down
                part = q[:, :LANES]
                for piece in range(1, ch // LANES):
                    part = part + q[:, piece * LANES : (piece + 1) * LANES]
                dlev[at, :] += split_mm(part, onehot)
            colrow[pl.ds(h, 1), :] = below

    def gx_copy(j):
        return copy(
            dpx.at[pl.ds(pl.multiple_of(p * (tokens - HALO), HALO), tokens + HALO), lanes(j, LANES)],
            gx.at[
                m, pl.ds(pl.multiple_of(HALO - HALO * p, HALO), tokens + HALO), lanes(j, LANES)
            ],
            "gx",
            j,
            "sp",
            partner,
        )

    keep_src = pl.ds(pl.multiple_of(m * (tokens - HALO), HALO), tokens + HALO)
    keep_dst = pl.ds(pl.multiple_of(HALO - HALO * m, HALO), tokens + HALO)

    def consume(j):
        k, r = kn[...], rn[...]
        ra, rb, la, lb = rin[j, 0], rin[j, 1], lin[j, 0], lin[j, 1]
        ef, eb = ef_ref[j], eb_ref[j]
        u = u_ref[j]
        at = lanes(j, LANES)
        dy = dyin[:, at].astype(f32)
        v = vb_ref[j].astype(f32)
        skip = tapall[CONV_K : CONV_K + 1, lanes(m * pairs + j, LANES)]
        onehot = (pick_lane == 2 * j + pick_half).astype(bf16)
        dl, dr = ef * mm(k, rb), eb * mm(k, lb)
        ml, mr = ef * mm(r, ra), eb * mm(r, la)
        dv = dv_ref[j] + dl + dr
        dpx[:, at] = ((dv * dts_ref[j] + skip * dy) * sux_ref[j]).astype(bf16)

        @pl.when(j < pairs - 1)
        def _():
            gx_copy(j).start()

        gx[m, keep_dst, at] = dpx[keep_src, at]
        dksum[...] += mm_nt(vef_ref[j], rb) + mm_nt(veb_ref[j], lb)
        drsum[...] += mm_nt(dyef_ref[j], ra) + mm_nt(dyeb_ref[j], la)
        dlev[...] += split_mm(dy * (mr - ml) + v * (dr - dl), onehot)
        sdt[...] += split_mm(u * dv, onehot)
        over = lb.astype(f32) * rout[j, 0].astype(f32) + la.astype(f32) * rout[j, 1].astype(f32)
        over = jnp.broadcast_to(jnp.sum(over, axis=0, keepdims=True), (8, LANES))
        cross[...] += split_mm(over, onehot)

    def chain_copy(name, j, q, into_ref, out_ref, step):
        return copy(out_ref.at[j, q], into_ref.at[j, q], name, 2 * j + q, "sp", near(step))

    def chain(name, j, into_ref, own_ref, out_ref, head, tail, step):
        decay = tdec[j][0:1, :]
        for q in range(2):
            item = chain_copy(name, j, q, into_ref, out_ref, step)

            @pl.when(jnp.logical_not(head))
            def _():
                item.wait_recv()

            out_ref[j, q] = (own_ref[j, q] + decay * into_ref[j, q].astype(f32)).astype(bf16)

            @pl.when(jnp.logical_not(tail))
            def _():
                item.start()

    delay = SKEW * (chunks - 1)

    phase("ticks")
    @pl.loop(0, pairs + delay)
    def _(tick):
        @pl.when(tick < pairs)
        def _():
            sr_ref[tick, 0] = mm(kt[...], veb_ref[tick])
            sr_ref[tick, 1] = mm(rt[...], dyeb_ref[tick])
            sl_ref[tick, 0] = mm(kt[...], vef_ref[tick])
            sl_ref[tick, 1] = mm(rt[...], dyef_ref[tick])

        jr = tick - SKEW * c

        @pl.when(jnp.logical_and(jr >= 0, jr < pairs))
        def _():
            with jax.named_scope("chain_r"):
                chain("right", jr, rin, sr_ref, rout, first, last, GROUPS)

        jl = tick - SKEW * (chunks - 1 - c)

        @pl.when(jnp.logical_and(jl >= 0, jl < pairs))
        def _():
            with jax.named_scope("chain_l"):
                chain("left", jl, lin, sl_ref, lout, last, first, -GROUPS)

        @pl.when(tick < pairs)
        def _():
            with jax.named_scope("intra"):
                intra(tick)

        @pl.when(tick == pairs - 1)
        def _():
            ge = gesum[...].astype(bf16)
            dksum[...] += mm(ge, rn[...])
            drsum[...] += mm_tn(ge, kn[...])

        @pl.when(tick >= delay)
        def _():
            with jax.named_scope("consume"):
                consume(tick - delay)

    phase("send_dbc")
    sbc = sbc_ref[...]
    dpbc[:, :STATE] = (dksum[...] * sbc[:, :STATE]).astype(bf16)
    dpbc[:, STATE:] = (drsum[...] * sbc[:, STATE:]).astype(bf16)
    gbc_copy = go(
        copy(
            dpbc.at[pl.ds(pl.multiple_of(p * (tokens - HALO), HALO), tokens + HALO), :],
            gbc.at[m, pl.ds(pl.multiple_of(HALO - HALO * p, HALO), tokens + HALO), :],
            "gbc",
            0,
            "sp",
            partner,
        )
    )

    def send_edges(name, source, target):
        go(
            copy(
                source.at[ch - HALO :, :],
                target.at[m, :HALO, :],
                name + "_left",
                0,
                "sp",
                lax.rem((c + 1) * GROUPS, sp),
                into=m,
            ),
            jnp.logical_not(last),
        )
        go(
            copy(
                source.at[:HALO, :],
                target.at[m, HALO + tokens :, :],
                name + "_right",
                0,
                "sp",
                lax.rem(c * GROUPS - 1 + sp, sp),
                into=m,
            ),
            jnp.logical_not(first),
        )

    def await_edges(name, target):
        lead, trail = m == 0, m == GROUPS - 1
        for g in range(GROUPS):
            slot = target.at[g, :HALO, :]
            arrive(
                copy(slot, slot, name + "_left", g, "sp", partner),
                jnp.logical_and(lead, jnp.logical_not(first)),
            )
            slot = target.at[g, HALO + tokens :, :]
            arrive(
                copy(slot, slot, name + "_right", g, "sp", partner),
                jnp.logical_and(trail, jnp.logical_not(last)),
            )

        @pl.when(jnp.logical_and(lead, first))
        def _():
            target[:, :HALO, :] = jnp.zeros((GROUPS, HALO, target.shape[2]), bf16)

        @pl.when(jnp.logical_and(trail, last))
        def _():
            target[:, HALO + tokens :, :] = jnp.zeros((GROUPS, HALO, target.shape[2]), bf16)

    send_edges("gbc", dpbc, gbc)
    gx_copy(pairs - 1).start()
    send_edges("gx", dpx, gx)
    gbc[m, keep_dst, :] = dpbc[keep_src, :]

    phase("ddt")
    fill = jnp.zeros((LANES - gh, ch), f32)
    down = jnp.concatenate([colrow[...], fill], axis=0).T
    drate = jnp.dot(upper, dlev[...] - down, precision=highest, preferred_element_type=f32)
    drate = (drate - cross[0:1, :]).T[:gh]
    ddt = ((drate * twice(faderow[...]) + sdt[...].T[:gh]) * sigrow[...]).astype(bf16)
    for g in range(GROUPS):
        ddtsend[g] = ddt[:, g * tokens : (g + 1) * tokens]
    group_rows = pl.ds(pl.multiple_of(m * gh, gh), gh)
    ddt_copy = go(copy(ddtsend.at[p], ddt_ref.at[group_rows, :], "ddt", 0, "sp", partner))
    ddt_ref[group_rows, :] = ddtsend[m]

    phase("wait_gbc")
    arrive(gbc_copy)
    await_edges("gbc", gbc)
    phase("conv_g")
    for g in range(GROUPS):
        for q in range(2):
            at = slice(g * STATE, (g + 1) * STATE)
            taps = (tapb_ref, tapc_ref)[q][:, at]
            part = gbc[g, :, q * STATE : (q + 1) * STATE].astype(f32)
            to = q * latent + g * STATE
            gsend[:, to : to + STATE] = window_conv(part, taps, tokens, True).astype(bf16)

    phase("d_hidden")
    halves = [slice(q * latent, (q + 1) * latent) for q in range(2)]

    def g_copy(source, block, name, index, q, peer):
        return go(
            copy(
                source.at[:, halves[q]],
                gall.at[block, :, halves[q]],
                name,
                2 * index + q,
                "dp",
                peer,
            )
        )

    g_y = {}
    g_core = {}
    for q in range(2):
        for o in range(1, ny):
            peer = lax.rem(y + o, ny) * cores + core
            g_y[o, q] = g_copy(gsend, me_dp, "g_y", o, q, peer)
        if cores > 1:
            g_core[q] = g_copy(gsend, me_dp, "g_core", 0, q, other_core)
    gall[me_dp] = gsend[...]
    gb, gc = gsend[:, :latent], gsend[:, latent:]
    for i in range(dp):
        dh_ref[:, i * cw : (i + 1) * cw] = (mm_nt(gb, wball[i]) + mm_nt(gc, wcall[i])).astype(bf16)
    phase("wait_g")
    for item in la_copies:
        arrive(item)
    w1 = []
    g_fwd = {}

    def forward_g(q):
        for o in range(1, ny):
            src = lax.rem(y - o + ny, ny) * cores + core
            arrive(g_y[o, q])
            if cores > 1:
                g_fwd[o, q] = g_copy(gall.at[src], src, "g_fwd", o, q, other_core)

    forward_g(0)
    for q in range(2):
        if cores > 1:
            arrive(g_core[q])
            for o in range(1, ny):
                arrive(g_fwd[o, q])
        if q == 0:
            forward_g(1)
        phase("dw")
        total = None
        for i in range(dp):
            term = mm_tn(cols[i], gall[i, :, halves[q]])
            total = term if total is None else total + term
        total = total.reshape(GROUPS, chunks, rows, latent)
        wsend[q] = total.astype(bf16)
        w1.append(go(copy(wsend.at[q, p], w1in.at[q], "w1", q, "sp", partner)))

    def input_gradient(g):
        @pl.loop(0, pairs)
        def _(j):
            taps = tapall[:, lanes(g * pairs + j, LANES)]
            part = gx[g, :, lanes(j, LANES)].astype(f32)
            dx_ref[:, lanes(g * pairs + j, LANES)] = window_conv(part, taps, tokens, True).astype(
                bf16
            )

    phase("wait_gx")
    @pl.loop(0, pairs)
    def _(j):
        gx_copy(j).wait_recv()

    await_edges("gx", gx)
    phase("w2")
    w2 = []
    for q in range(2):
        arrive(w1[q])
        part = wsend[q, m].astype(f32) + w1in[q].astype(f32)
        s1send[q] = part.astype(bf16)
        for o in range(1, chunks):
            k = lax.rem(c + o, chunks)
            w2.append(
                go(
                    copy(
                        s1send.at[q, k],
                        w2in.at[q, c],
                        "w2",
                        q * chunks + o,
                        "sp",
                        k * GROUPS + m,
                    )
                )
            )
        wown[q] = s1send[q, c].astype(f32)
    phase("dx0")
    input_gradient(0)
    phase("w3")
    w3 = []
    for q in range(2):
        share = wown[q]
        for o in range(1, chunks):
            arrive(w2[q * (chunks - 1) + o - 1])
            share = share + w2in[q, lax.rem(c - o + chunks, chunks)].astype(f32)
        s3send[q] = share.astype(bf16)
        tall[q, m, c] = s3send[q]
        for o in range(1, chunks):
            k = lax.rem(c + o, chunks)
            w3.append(
                go(
                    copy(
                        s3send.at[q],
                        tall.at[q, m, c],
                        "w3",
                        q * chunks + o,
                        "sp",
                        k * GROUPS + m,
                    )
                )
            )
    phase("dx1")
    input_gradient(1)
    phase("w4")
    w4 = []
    for q in range(2):
        for o in range(1, chunks):
            arrive(w3[q * (chunks - 1) + o - 1])
        w4.append(go(copy(tall.at[q, m], tall.at[q, m], "w4", q, "sp", partner)))
    phase("last")
    arrive(ddt_copy)
    for item in w4:
        arrive(item)

    @pl.loop(0, pairs)
    def _(j):
        gx_copy(j).wait_send()

        @pl.when(jnp.logical_not(last))
        def _():
            for q in range(2):
                chain_copy("right", j, q, rin, rout, GROUPS).wait_send()

        @pl.when(jnp.logical_not(first))
        def _():
            for q in range(2):
                chain_copy("left", j, q, lin, lout, -GROUPS).wait_send()

    for item, cond in sent:
        if cond is None:
            item.wait_send()
        else:

            @pl.when(cond)
            def _():
                item.wait_send()

    phase.end()


def out_kernel(dgate, dx, dh, ddt, tall, dgate_out, dx_out, dh_out, ddt_out, dwb_out, dwc_out):
    ddt_out[...] = ddt[...]
    dgate_out[...] = dgate[...]
    dx_out[...] = dx[...]
    dh_out[...] = dh[...]
    dwb_out[...] = tall[0].astype(f32).reshape(dwb_out.shape)
    dwc_out[...] = tall[1].astype(f32).reshape(dwc_out.shape)


def local(
    layer_activity,
    writer_matrix,
    reader_matrix,
    source_unfiltered,
    switch_raw_signal,
    saved_result,
    final_adjoint,
    delta_raw,
    extra_logdrop,
    source_filter_coefs,
    writer_filter_coefs,
    reader_filter_coefs,
    delta_offset,
    fading_exponents,
    direct_factor,
    rescale_factor,
):
    tokens, width_in = layer_activity.shape[1:]
    inner = source_unfiltered.shape[2]
    dp = lax.axis_size("dp")
    sp = lax.axis_size("sp")
    cores = 2 if dp % 2 == 0 else 1
    heads = delta_offset.shape[0]
    cw, latent = writer_matrix.shape
    xc = heads * HEAD_DIM
    xw = -(-xc // LANES) * LANES
    rows_h = -(-heads // 8) * 8
    chunks = sp // GROUPS
    ch = tokens * GROUPS
    gw = inner // GROUPS
    gh = HEADS // GROUPS
    pairs = gw // LANES
    rows = cw // sp
    window = tokens * sp
    _, slots = slot_table(sp, dp, cores, pairs)

    vmem = pl.BlockSpec(memory_space=pltpu.VMEM)
    hbm = pl.BlockSpec(memory_space=pltpu.HBM)
    smem = pl.BlockSpec(memory_space=pltpu.SMEM)
    scratch = [
        ((tokens, width_in), bf16),
        ((cw, latent), bf16),
        ((cw, latent), bf16),
        ((tokens, inner), bf16),
        ((tokens, inner), bf16),
        ((tokens, inner), bf16),
        ((tokens, inner), bf16),
        ((dp, cw, latent), bf16),
        ((dp, cw, latent), bf16),
        ((dp, tokens, cw), bf16),
        ((ch + 2 * HALO, gw), bf16),
        ((ch, gw), bf16),
        ((tokens, gw), bf16),
        ((gh, ch), bf16),
        ((chunks, rows_h, ch + 2 * LANES), f32),
        ((chunks, rows_h, ch + 2 * LANES), f32),
        ((gh, ch + 2 * LANES), f32),
        ((8, xw), f32),
        ((sp, 8, xw), f32),
        ((8, inner), f32),
        ((GROUPS, tokens, 2 * STATE), bf16),
        ((ch + 2 * HALO, 2 * STATE), bf16),
        ((pairs, ch, LANES), f32),
        ((pairs, ch, LANES), f32),
        ((pairs, ch, LANES), f32),
        ((pairs, ch, LANES), f32),
        ((pairs, ch, LANES), f32),
        ((pairs, 8, LANES), f32),
        ((pairs, ch, LANES), bf16),
        ((pairs, ch, LANES), bf16),
        ((pairs, ch, LANES), bf16),
        ((pairs, ch, LANES), bf16),
        ((pairs, ch, LANES), bf16),
        ((ch, STATE), bf16),
        ((ch, STATE), bf16),
        ((STATE, ch), bf16),
        ((STATE, ch), bf16),
        ((ch, 2 * STATE), f32),
        ((ch, ch), f32),
        ((ch, ch), f32),
        ((ch, ch), f32),
        ((gh, ch, LANES), f32),
        ((gh, ch), f32),
        ((gh, ch), f32),
        ((gh, LANES), f32),
        ((pairs, ch, LANES), f32),
        ((pairs, 2, STATE, LANES), f32),
        ((pairs, 2, STATE, LANES), f32),
        ((pairs, 2, STATE, LANES), bf16),
        ((pairs, 2, STATE, LANES), bf16),
        ((pairs, 2, STATE, LANES), bf16),
        ((pairs, 2, STATE, LANES), bf16),
        ((ch, STATE), f32),
        ((ch, STATE), f32),
        ((ch, LANES), f32),
        ((ch, LANES), f32),
        ((8, LANES), f32),
        ((gh, ch), f32),
        ((ch, gw), bf16),
        ((GROUPS, tokens + 2 * HALO, gw), bf16),
        ((ch, 2 * STATE), bf16),
        ((GROUPS, tokens + 2 * HALO, 2 * STATE), bf16),
        ((GROUPS, gh, tokens), bf16),
        ((tokens, 2 * latent), bf16),
        ((dp, tokens, 2 * latent), bf16),
        ((2, GROUPS, chunks, rows, latent), bf16),
        ((2, rows, latent), f32),
        ((2, chunks, rows, latent), bf16),
        ((2, chunks, rows, latent), bf16),
        ((2, chunks, rows, latent), bf16),
        ((2, rows, latent), bf16),
    ]
    dgate, dx, ddt, dh, tall = pl.pallas_call(
        functools.partial(mega_kernel, heads, cores),
        in_specs=[hbm] * 7 + [vmem] * 6 + [smem] * 3,
        out_specs=[vmem] * 5,
        out_shape=[
            pltpu.VMEM((tokens, inner), bf16),
            pltpu.VMEM((tokens, inner), bf16),
            pltpu.VMEM((HEADS, tokens), bf16),
            pltpu.VMEM((tokens, width_in), bf16),
            pltpu.VMEM((2, GROUPS, chunks, rows, latent), bf16),
        ],
        scratch_shapes=[pltpu.VMEM(shape, kind) for shape, kind in scratch]
        + [pltpu.SemaphoreType.DMA((slots,)), pltpu.SemaphoreType.DMA((slots,))]
        + [pltpu.SemaphoreType.DMA((7,))],
        compiler_params=pltpu.CompilerParams(
            collective_id=0, has_side_effects=True, vmem_limit_bytes=60 * 1024 * 1024
        ),
        name="mega",
    )(
        layer_activity.reshape(tokens, width_in),
        writer_matrix,
        reader_matrix,
        source_unfiltered.reshape(tokens, inner),
        switch_raw_signal.reshape(tokens, inner),
        saved_result.reshape(tokens, inner),
        final_adjoint.reshape(tokens, inner),
        delta_raw.reshape(tokens, HEADS).T,
        extra_logdrop.reshape(window, heads).T,
        source_filter_coefs,
        writer_filter_coefs,
        reader_filter_coefs,
        rescale_factor.reshape(1, inner),
        delta_offset,
        fading_exponents,
        direct_factor,
    )
    d_gate, d_x, d_hidden, d_dt, d_w_b, d_w_c = pl.pallas_call(
        out_kernel,
        in_specs=[vmem] * 5,
        out_specs=[vmem] * 6,
        out_shape=[
            jax.ShapeDtypeStruct((tokens, inner), bf16),
            jax.ShapeDtypeStruct((tokens, inner), bf16),
            jax.ShapeDtypeStruct((tokens, width_in), bf16),
            jax.ShapeDtypeStruct((HEADS, tokens), bf16),
            jax.ShapeDtypeStruct((cw, latent), f32),
            jax.ShapeDtypeStruct((cw, latent), f32),
        ],
        name="outputs",
    )(*[pltpu.with_memory_space_constraint(v, pltpu.VMEM) for v in (dgate, dx, dh, ddt, tall)])
    return (
        d_hidden.reshape(1, tokens, width_in),
        d_x.reshape(1, tokens, inner),
        d_gate.reshape(1, tokens, inner),
        d_dt.T.reshape(1, tokens, HEADS),
        d_w_b,
        d_w_c,
    )


def solution(mesh):
    in_specs = (
        P("dp", "sp", None),
        P("dp", None),
        P("dp", None),
        P("dp", "sp", None),
        P("dp", "sp", None),
        P("dp", "sp", None),
        P("dp", "sp", None),
        P("dp", "sp", None),
        P("dp", None, "sp"),
        P(None, "sp"),
        P(),
        P(),
        P("sp"),
        P("sp"),
        P("sp"),
        P(),
    )
    out_specs = (
        P("dp", "sp", None),
        P("dp", "sp", None),
        P("dp", "sp", None),
        P("dp", "sp", None),
        P("dp", None),
        P("dp", None),
    )
    return jax.shard_map(local, mesh=mesh, in_specs=in_specs, out_specs=out_specs, check_vma=False)
```

```python
import functools

import jax
import jax.numpy as jnp
from jax import lax
from jax.experimental import pallas as pl
from jax.experimental.pallas import tpu as pltpu
from jax.sharding import PartitionSpec as P

HEADS = 32
HEAD_DIM = 64
STATE = 128
GROUPS = 2
NORM_GROUPS = 8
CONV_K = 5
LANES = 128
HALO = 16
SKEW = 2
EPSILON = 1e-06
LOG2E = 1.4426950408889634
highest = lax.Precision.HIGHEST
f32 = jnp.float32
bf16 = jnp.bfloat16
NT = (((1,), (1,)), ((), ()))
TN = (((0,), (0,)), ((), ()))


def sigmoid(v):
    return 1.0 / (1.0 + jnp.exp(-v))


def softplus(v):
    e = jnp.exp(-jnp.abs(v))
    z = e / (2.0 + e)
    z2 = z * z
    series = jnp.full_like(z, 1.0 / 17.0)
    for odd in (15, 13, 11, 9, 7, 5, 3, 1):
        series = series * z2 + 1.0 / odd
    return jnp.maximum(v, 0.0) + 2.0 * z * series


def mm(a, b):
    return jnp.dot(a, b, preferred_element_type=f32)


def mm_nt(a, b):
    return lax.dot_general(a, b, NT, preferred_element_type=f32)


def mm_tn(a, b):
    return lax.dot_general(a, b, TN, preferred_element_type=f32)


def split_mm(a, b):
    hi = a.astype(bf16)
    lo = (a - hi.astype(f32)).astype(bf16)
    return mm(hi, b) + mm(lo, b)


def window_conv(rows, taps, count, flip):
    total = None
    for k in range(CONV_K):
        shift = HALO - CONV_K // 2 + k
        tap = taps[CONV_K - 1 - k if flip else k][None, :]
        term = tap * pltpu.roll(rows, rows.shape[0] - shift, axis=0)[:count]
        total = term if total is None else total + term
    return total


def greet(axes):
    barrier = pltpu.get_barrier_semaphore()
    count = 0
    for axis in axes:
        size = lax.axis_size(axis)
        me = lax.axis_index(axis)
        for o in range(1, size):
            pl.semaphore_signal(
                barrier,
                inc=1,
                device_id={axis: lax.rem(me + o, size)},
                device_id_type=pl.DeviceIdType.MESH,
            )
            count += 1
    pl.semaphore_wait(barrier, count)


class Phases:
    def __init__(self):
        self.scope = None

    def __call__(self, name):
        self.end()
        self.scope = jax.named_scope(name)
        self.scope.__enter__()

    def end(self):
        if self.scope is not None:
            self.scope.__exit__(None, None, None)
            self.scope = None


def slot_table(sp, dp, cores, pairs):
    ny = dp // cores
    chunks = sp // GROUPS
    counts = (
        ("w_y", 2 * ny),
        ("w_core", 2),
        ("w_fwd", 2 * ny),
        ("la_y", 2 * ny),
        ("la", ny),
        ("p_y", 2 * ny),
        ("x", 1),
        ("x_left", GROUPS),
        ("x_right", GROUPS),
        ("dt", 1),
        ("drop", chunks),
        ("tap", sp),
        ("dy", NORM_GROUPS),
        ("bc", 1),
        ("bc_left", GROUPS),
        ("bc_right", GROUPS),
        ("right", 2 * pairs),
        ("left", 2 * pairs),
        ("gx", pairs),
        ("gx_left", GROUPS),
        ("gx_right", GROUPS),
        ("db_left", 1),
        ("db_right", 1),
        ("gx_g", 1),
        ("cols", 1),
        ("ddt", 1),
        ("g_y", 2 * ny),
        ("g_core", 2),
        ("g_fwd", 2 * ny),
        ("w2", 2 * chunks),
        ("w3", 2 * chunks),
        ("w4", 2 * chunks),
    )
    table = {}
    at = 0
    for name, count in counts:
        table[name] = at
        at += count
    return table, at


def mega_kernel(
    heads,
    cores,
    la_hbm,
    wb_hbm,
    wc_hbm,
    x_hbm,
    gates_hbm,
    values_hbm,
    adjoint_hbm,
    dt_ref,
    drop_ref,
    tapx_ref,
    tapb_ref,
    tapc_ref,
    scale_ref,
    offset_ref,
    fade_ref,
    skip_ref,
    dgate_ref,
    dx_ref,
    ddt_ref,
    dh_ref,
    tall,
    la_ref,
    wb_ref,
    wc_ref,
    x_ref,
    gates_ref,
    values_ref,
    adjoint_ref,
    wball,
    wcall,
    cols,
    lain,
    psend,
    pin,
    psum,
    xin,
    dyin,
    dysend,
    dtin,
    dropsend,
    dropin,
    drow,
    tapsend,
    tapin,
    tapall,
    bcsend,
    bcin,
    u_ref,
    sux_ref,
    dts_ref,
    ef_ref,
    eb_ref,
    tdec,
    vb_ref,
    vef_ref,
    veb_ref,
    dyef_ref,
    dyeb_ref,
    kn,
    rn,
    kt,
    rt,
    sbc_ref,
    score_ref,
    sign_ref,
    gesum,
    lcolb,
    lrow,
    sigrow,
    faderow,
    dv_ref,
    sr_ref,
    sl_ref,
    rin,
    lin,
    rout,
    lout,
    dksum,
    drsum,
    dlev,
    sdt,
    cross,
    colrow,
    dpx,
    gx,
    dbin,
    ddtsend,
    gsend,
    ghid,
    gall,
    wsend,
    wown,
    w2in,
    s3send,
    ss,
    rs,
    ls,
):
    dp = lax.axis_size("dp")
    sp = lax.axis_size("sp")
    me_dp = lax.axis_index("dp")
    me_sp = lax.axis_index("sp")
    ny = dp // cores
    chunks = sp // GROUPS
    y = me_dp // cores
    core = lax.rem(me_dp, cores)
    c = me_sp // GROUPS
    m = lax.rem(me_sp, GROUPS)
    p = GROUPS - 1 - m
    partner = c * GROUPS + p
    other_core = y * cores + (cores - 1 - core)
    tokens, inner = x_ref.shape
    gw = inner // GROUPS
    gh = HEADS // GROUPS
    ch = tokens * GROUPS
    pairs = gw // LANES
    cw = wb_ref.shape[0]
    latent = wb_ref.shape[1]
    xc = heads * HEAD_DIM
    nsrc = sp // GROUPS
    rows = cw // chunks
    first = c == 0
    last = c == chunks - 1
    table, _ = slot_table(sp, dp, cores, pairs)
    sent = []

    def copy(src, dst, name, index, axis, peer, into=None):
        at = table[name]
        return pltpu.make_async_remote_copy(
            src_ref=src,
            dst_ref=dst,
            send_sem=ss.at[at + index],
            recv_sem=rs.at[at + (index if into is None else into)],
            device_id={axis: peer},
            device_id_type=pl.DeviceIdType.MESH,
        )

    def go(item, cond=None):
        if cond is None:
            item.start()
        else:

            @pl.when(cond)
            def _():
                item.start()

        sent.append((item, cond))
        return item

    def arrive(item, cond=None):
        if cond is None:
            item.wait_recv()
        else:

            @pl.when(cond)
            def _():
                item.wait_recv()

    def lanes(index, width):
        return pl.ds(pl.multiple_of(index * width, LANES), width)

    def near(step):
        return lax.rem(me_sp + step + 2 * sp, sp)

    mine = pl.ds(pl.multiple_of(HALO + m * tokens, HALO), tokens)
    mine0 = pl.ds(pl.multiple_of(m * tokens, HALO), tokens)
    body = slice(HALO, HALO + ch)
    left_rows = slice(0, HALO)
    right_rows = slice(HALO + ch, 2 * HALO + ch)
    to_right = jnp.logical_and(m == GROUPS - 1, jnp.logical_not(last))
    to_left = jnp.logical_and(m == 0, jnp.logical_not(first))

    phase = Phases()
    phase("greet")
    loads = {}
    for at, (source, target) in enumerate(
        (
            (wb_hbm, wb_ref),
            (wc_hbm, wc_ref),
            (x_hbm, x_ref),
            (values_hbm, values_ref),
            (gates_hbm, gates_ref),
            (adjoint_hbm, adjoint_ref),
            (la_hbm, la_ref),
        )
    ):
        loads[at] = pltpu.make_async_copy(source, target, ls.at[at])
    for at in (6, 2, 0, 1, 3, 4, 5):
        loads[at].start()
    greet(("dp", "sp"))
    loads[6].wait()

    phase("send_first")
    cwy = cores * cw
    part_rows = tokens // 2
    parts = [slice(t * part_rows, (t + 1) * part_rows) for t in range(2)]
    la_y = {}
    for t in range(2):
        for o in range(1, ny):
            there = lax.rem(y + o, ny)
            la_y[o, t] = go(
                copy(
                    la_ref.at[parts[t], lanes(there, cwy)],
                    lain.at[y, parts[t], :],
                    "la_y",
                    2 * o + t,
                    "dp",
                    there * cores + core,
                )
            )
    loads[2].wait()
    x_copy = go(copy(x_ref.at[:, lanes(p, gw)], xin.at[mine, :], "x", 0, "sp", partner))
    loads[0].wait()
    loads[1].wait()
    w_core = []
    if cores > 1:
        w_core = [
            go(copy(wb_ref, wball.at[me_dp], "w_core", 0, "dp", other_core)),
            go(copy(wc_ref, wcall.at[me_dp], "w_core", 1, "dp", other_core)),
        ]
    dt_copy = go(
        copy(
            dt_ref.at[pl.ds(pl.multiple_of(p * gh, gh), gh), :],
            dtin.at[:, lanes(m, tokens)],
            "dt",
            0,
            "sp",
            partner,
        )
    )

    def send_halo(name, source, target):
        for g in range(GROUPS):
            go(
                copy(
                    source(g, slice(tokens - HALO, tokens)),
                    target.at[left_rows, :],
                    name + "_left",
                    g,
                    "sp",
                    near(1 + g),
                    into=0,
                ),
                to_right,
            )
            go(
                copy(
                    source(g, slice(0, HALO)),
                    target.at[right_rows, :],
                    name + "_right",
                    g,
                    "sp",
                    near(g - GROUPS),
                    into=0,
                ),
                to_left,
            )

    def await_halo(name, target):
        arrive(
            copy(target.at[left_rows, :], target.at[left_rows, :], name + "_left", 0, "sp", partner),
            jnp.logical_not(first),
        )
        arrive(
            copy(target.at[right_rows, :], target.at[right_rows, :], name + "_right", 0, "sp", partner),
            jnp.logical_not(last),
        )

        @pl.when(first)
        def _():
            target[left_rows, :] = jnp.zeros((HALO, target.shape[1]), bf16)

        @pl.when(last)
        def _():
            target[right_rows, :] = jnp.zeros((HALO, target.shape[1]), bf16)

    send_halo("x", lambda g, r: x_ref.at[r, g * gw : (g + 1) * gw], xin)

    phase("params")
    rows_h = dropsend.shape[1]
    head_row = lax.broadcasted_iota(jnp.int32, (rows_h, LANES), 0)
    offsets = jnp.zeros((rows_h, LANES), f32)
    fades = jnp.zeros((rows_h, LANES), f32)
    for h in range(heads):
        offsets = jnp.where(head_row == h, offset_ref[h], offsets)
        fades = jnp.where(head_row == h, fade_ref[h], fades)
    dropsend[...] = jnp.zeros_like(dropsend)
    for k in range(chunks):
        dropsend[k, :heads, :ch] = drop_ref[:, k * ch : (k + 1) * ch]
        dropsend[k, :, ch : ch + LANES] = offsets
        dropsend[k, :, ch + LANES :] = fades
    owner = (me_sp * heads) // gh
    place = me_sp - owner * nsrc
    for o in range(chunks):
        k = lax.rem(c + o, chunks)
        go(
            copy(
                dropsend.at[k],
                dropin.at[place],
                "drop",
                o,
                "sp",
                k * GROUPS + owner if o else partner,
                into=place,
            ),
            None if o else owner != m,
        )

    @pl.when(owner == m)
    def _():
        dropin[place] = dropsend[c]

    xw = tapsend.shape[1]
    tap_lane = lax.broadcasted_iota(jnp.int32, (1, xw), 1) // HEAD_DIM
    skips = jnp.zeros((1, xw), f32)
    for h in range(heads):
        skips = jnp.where(tap_lane == h, skip_ref[h], skips)
    tapsend[...] = jnp.zeros_like(tapsend)
    tapsend[:CONV_K, :xc] = tapx_ref[...]
    tapsend[CONV_K : CONV_K + 1, :] = skips
    tap_copies = []
    for o in range(1, sp):
        tap_copies.append(go(copy(tapsend, tapin.at[me_sp], "tap", o, "sp", lax.rem(me_sp + o, sp))))
    tapin[me_sp] = tapsend[...]
    la_copies = []
    if cores > 1:
        la_copies.append(
            go(copy(la_ref.at[:, lanes(other_core, cw)], cols.at[m, me_dp], "la", 0, "dp", other_core))
        )
    cols[m, me_dp] = la_ref[:, lanes(me_dp, cw)]
    wball[me_dp] = wb_ref[...]
    wcall[me_dp] = wc_ref[...]
    xin[mine, :] = x_ref[:, lanes(m, gw)]
    dtin[:, lanes(m, tokens)] = dt_ref[pl.ds(pl.multiple_of(m * gh, gh), gh), :]

    phase("norm")
    width = inner // NORM_GROUPS
    per_half = NORM_GROUPS // GROUPS
    early = per_half // 2
    dy_copies = []
    for at in (3, 4, 5):
        loads[at].wait()
    for half in range(GROUPS):
        who = p if half == 0 else m
        for i in range(per_half):
            span = lanes(who * per_half + i, width)
            values = values_ref[:, span].astype(f32)
            gates = gates_ref[:, span].astype(f32)
            sig = sigmoid(gates)
            act = gates * sig
            g = values * act
            dn = adjoint_ref[:, span].astype(f32) * scale_ref[:, span]
            inv = lax.rsqrt(jnp.sum(g * g, axis=1, keepdims=True) * (1.0 / width) + EPSILON)
            along = jnp.sum(dn * g, axis=1, keepdims=True) * (1.0 / width)
            dg = inv * dn - g * (inv * inv * inv * along)
            dgate_ref[:, span] = (dg * values * (sig + act * (1.0 - sig))).astype(bf16)
            dy = (dg * act).astype(bf16)
            at = slice(i * width, (i + 1) * width)
            if half == 0:
                dysend[:, at] = dy
                dy_copies.append(copy(dysend.at[:, at], dyin.at[mine0, at], "dy", i, "sp", partner))
                if i < early:
                    go(dy_copies[i])
            else:
                dyin[mine0, at] = dy

    phase("partial")
    for item in w_core:
        arrive(item)
    p_y = {}
    for t in range(2):
        for o in range(1, ny):
            there = lax.rem(y - o + ny, ny)
            arrive(la_y[o, t])
            tb = tc = None
            for k in range(cores):
                part = lain[there, parts[t], k * cw : (k + 1) * cw]
                one, two = mm(part, wball[y * cores + k]), mm(part, wcall[y * cores + k])
                tb, tc = (one, two) if tb is None else (tb + one, tc + two)
            psend[there, parts[t], :latent] = tb.astype(bf16)
            psend[there, parts[t], latent:] = tc.astype(bf16)
            p_y[o, t] = go(
                copy(
                    psend.at[there, parts[t], :],
                    pin.at[y, parts[t], :],
                    "p_y",
                    2 * o + t,
                    "dp",
                    there * cores + core,
                )
            )
    w_y = []
    for o in range(1, ny):
        peer = lax.rem(y + o, ny) * cores + core
        w_y.append(
            (
                go(copy(wb_ref, wball.at[me_dp], "w_y", 2 * o, "dp", peer)),
                go(copy(wc_ref, wcall.at[me_dp], "w_y", 2 * o + 1, "dp", peer)),
            )
        )
    for o in range(1, ny):
        there = lax.rem(y - o + ny, ny)
        block = there * cores + core
        cols[m, block] = lain[there, :, lanes(core, cw)]
        if cores > 1:
            la_copies.append(
                go(
                    copy(
                        lain.at[there, :, lanes(cores - 1 - core, cw)],
                        cols.at[m, block],
                        "la",
                        o,
                        "dp",
                        other_core,
                    )
                )
            )
    total_b = total_c = None
    for k in range(cores):
        part = la_ref[:, lanes(y * cores + k, cw)]
        one, two = mm(part, wball[y * cores + k]), mm(part, wcall[y * cores + k])
        total_b, total_c = (one, two) if k == 0 else (total_b + one, total_c + two)
    psum[:, :latent] = total_b
    psum[:, latent:] = total_c
    phase("levels")
    arrive(dt_copy)
    for i in range(nsrc):
        arrive(
            copy(dropsend.at[0], dropin.at[i], "drop", i, "sp", partner), m * nsrc + i != me_sp
        )
        drow[i * heads : (i + 1) * heads, :] = dropin[i, :heads, :]
    twice = lambda v: jnp.concatenate([v] * (ch // LANES), axis=1)
    fade = jnp.exp(drow[:, ch + LANES :])
    a = dtin[...].astype(f32) + twice(drow[:, ch : ch + LANES])
    dt = softplus(a)
    sigrow[...] = sigmoid(a)
    faderow[...] = fade
    rate = dt * twice(fade) + drow[:, :ch]
    row_i = lax.broadcasted_iota(jnp.int32, (ch, ch), 0)
    col_i = lax.broadcasted_iota(jnp.int32, (ch, ch), 1)
    upper = (row_i <= col_i).astype(f32)
    level = jnp.dot(rate, upper, precision=highest, preferred_element_type=f32) * LOG2E
    lrow[...] = level
    fill = jnp.zeros((LANES - gh, ch), f32)
    lcol = jnp.concatenate([level, fill], axis=0).T
    dtcol = jnp.concatenate([dt, fill], axis=0).T
    low_lane = lax.broadcasted_iota(jnp.int32, (ch, LANES), 1) < HEAD_DIM
    for j in range(pairs):
        pair = []
        for h in (2 * j, 2 * j + 1):
            wide = jnp.broadcast_to(lcol[:, h : h + 1], (ch, LANES))
            lcolb[h] = wide
            pair.append(wide)
        spread = jnp.where(low_lane, pair[0], pair[1])
        end = spread[ch - 1 : ch, :]
        ef_ref[j] = jnp.exp2(-spread)
        eb_ref[j] = jnp.exp2(spread - end)
        tdec[j] = jnp.broadcast_to(jnp.exp2(-end), (8, LANES))
        dts_ref[j] = jnp.where(low_lane, dtcol[:, 2 * j : 2 * j + 1], dtcol[:, 2 * j + 1 : 2 * j + 2])

    phase("project")
    total = psum[...]
    for o in range(1, ny):
        for t in range(2):
            arrive(p_y[o, t])
        total = total + pin[lax.rem(y - o + ny, ny)].astype(f32)
    total = total.astype(bf16)
    proj_b, proj_c = total[:, :latent], total[:, latent:]
    for g in range(GROUPS):
        bcsend[g, :, :STATE] = proj_b[:, g * STATE : (g + 1) * STATE]
        bcsend[g, :, STATE:] = proj_c[:, g * STATE : (g + 1) * STATE]
    bc_copy = go(copy(bcsend.at[p], bcin.at[mine, :], "bc", 0, "sp", partner))
    send_halo("bc", lambda g, r: bcsend.at[g, r, :], bcin)
    bcin[mine, :] = bcsend[m]
    for item in dy_copies[early:]:
        go(item)

    phase("wait_x")
    for item in tap_copies:
        arrive(item)
    if xc % LANES == 0:
        for i in range(sp):
            tapall[:, i * xc : (i + 1) * xc] = tapin[i]
    else:
        per = LANES // xc
        for i in range(inner // LANES):
            tapall[:, i * LANES : (i + 1) * LANES] = jnp.concatenate(
                [tapin[i * per + q][:, :xc] for q in range(per)], axis=1
            )
    arrive(x_copy)
    await_halo("x", xin)

    phase("prep_x")
    @pl.loop(0, pairs)
    def _(j):
        taps = tapall[:, lanes(m * pairs + j, LANES)]
        pre = window_conv(xin[:, lanes(j, LANES)].astype(f32), taps, ch, False)
        sig = sigmoid(pre)
        u = pre * sig
        u_ref[j] = u
        sux_ref[j] = sig + u * (1.0 - sig)
        v = u * dts_ref[j]
        vb_ref[j] = v.astype(bf16)
        vef_ref[j] = (v * ef_ref[j]).astype(bf16)
        veb_ref[j] = (v * eb_ref[j]).astype(bf16)

    phase("wait_bc")
    arrive(bc_copy)
    await_halo("bc", bcin)
    phase("conv_bc")
    for q in range(2):
        taps = (tapb_ref, tapc_ref)[q][:, lanes(m, STATE)]
        at = slice(q * STATE, (q + 1) * STATE)
        pre = window_conv(bcin[:, at].astype(f32), taps, ch, False)
        sig = sigmoid(pre)
        kr = pre * sig
        sbc_ref[:, at] = sig + kr * (1.0 - sig)
        (kn, rn)[q][...] = kr.astype(bf16)
        (kt, rt)[q][...] = kr.T.astype(bf16)
    score = mm_nt(kn[...], rn[...])
    score_ref[...] = score
    sign_ref[...] = score * jnp.clip(col_i - row_i, -1, 1).astype(f32)

    gesum[...] = jnp.zeros_like(gesum)
    dksum[...] = jnp.zeros_like(dksum)
    drsum[...] = jnp.zeros_like(drsum)
    dlev[...] = jnp.zeros_like(dlev)
    sdt[...] = jnp.zeros_like(sdt)
    cross[...] = jnp.zeros_like(cross)

    @pl.when(first)
    def _():
        rin[...] = jnp.zeros_like(rin)

    @pl.when(last)
    def _():
        lin[...] = jnp.zeros_like(lin)

    lane_low = lax.broadcasted_iota(jnp.int32, (1, LANES), 1) < HEAD_DIM
    masks = (lane_low.astype(bf16), 1.0 - lane_low.astype(bf16))
    pick_lane = lax.broadcasted_iota(jnp.int32, (LANES, LANES), 1)
    pick_half = lax.broadcasted_iota(jnp.int32, (LANES, LANES), 0) // HEAD_DIM
    block = min(ch, LANES)

    def intra(j):
        dyj = dyin[:, lanes(j, LANES)]
        for a in range(2):
            h = 2 * j + a
            lr = lrow[pl.ds(h, 1), :]
            dym = dyj * masks[a]
            onehot = (pick_lane == h).astype(bf16)
            below = None
            for b in range(ch // block):
                at = slice(b * block, (b + 1) * block)
                gap = twice(lcolb[h, at]) - lr
                decay = jnp.exp2(-jnp.abs(gap))
                ge = mm_nt(vb_ref[j, at] * masks[a], dyj) * decay
                gesum[at, :] += ge
                part = mm((score_ref[at, :] * decay).astype(bf16), dym)
                if a == 0:
                    dv_ref[j, at] = part
                else:
                    dv_ref[j, at] += part
                q = sign_ref[at, :] * ge
                down = jnp.sum(q, axis=0, keepdims=True)
                below = down if below is None else below + down
                part = q[:, :LANES]
                for piece in range(1, ch // LANES):
                    part = part + q[:, piece * LANES : (piece + 1) * LANES]
                dlev[at, :] += split_mm(part, onehot)
            colrow[pl.ds(h, 1), :] = below

    def gx_copy(j):
        return copy(
            dpx.at[pl.ds(pl.multiple_of(p * (tokens - HALO), HALO), tokens + HALO), lanes(j, LANES)],
            gx.at[
                m, pl.ds(pl.multiple_of(HALO - HALO * p, HALO), tokens + HALO), lanes(j, LANES)
            ],
            "gx",
            j,
            "sp",
            partner,
        )

    keep_src = pl.ds(pl.multiple_of(m * (tokens - HALO), HALO), tokens + HALO)
    keep_dst = pl.ds(pl.multiple_of(HALO - HALO * m, HALO), tokens + HALO)

    def consume(j):
        k, r = kn[...], rn[...]
        ra, rb, la, lb = rin[j, 0], rin[j, 1], lin[j, 0], lin[j, 1]
        ef, eb = ef_ref[j], eb_ref[j]
        u = u_ref[j]
        at = lanes(j, LANES)
        dy = dyin[:, at].astype(f32)
        v = vb_ref[j].astype(f32)
        skip = tapall[CONV_K : CONV_K + 1, lanes(m * pairs + j, LANES)]
        onehot = (pick_lane == 2 * j + pick_half).astype(bf16)
        dl, dr = ef * mm(k, rb), eb * mm(k, lb)
        ml, mr = ef * mm(r, ra), eb * mm(r, la)
        dv = dv_ref[j] + dl + dr
        dpx[:, at] = ((dv * dts_ref[j] + skip * dy) * sux_ref[j]).astype(bf16)

        @pl.when(j < pairs - 1)
        def _():
            gx_copy(j).start()

        gx[m, keep_dst, at] = dpx[keep_src, at]
        dksum[...] += mm_nt(vef_ref[j], rb) + mm_nt(veb_ref[j], lb)
        drsum[...] += mm_nt(dyef_ref[j], ra) + mm_nt(dyeb_ref[j], la)
        dlev[...] += split_mm(dy * (mr - ml) + v * (dr - dl), onehot)
        sdt[...] += split_mm(u * dv, onehot)
        over = lb.astype(f32) * rout[j, 0].astype(f32) + la.astype(f32) * rout[j, 1].astype(f32)
        over = jnp.broadcast_to(jnp.sum(over, axis=0, keepdims=True), (8, LANES))
        cross[...] += split_mm(over, onehot)

    def chain_copy(name, j, q, into_ref, out_ref, step):
        return copy(out_ref.at[j, q], into_ref.at[j, q], name, 2 * j + q, "sp", near(step))

    def chain(name, j, into_ref, own_ref, out_ref, head, tail, step):
        decay = tdec[j][0:1, :]
        for q in range(2):
            item = chain_copy(name, j, q, into_ref, out_ref, step)

            @pl.when(jnp.logical_not(head))
            def _():
                item.wait_recv()

            out_ref[j, q] = (own_ref[j, q] + decay * into_ref[j, q].astype(f32)).astype(bf16)

            @pl.when(jnp.logical_not(tail))
            def _():
                item.start()

    delay = SKEW * (chunks - 1)

    for item in la_copies:
        arrive(item)
    cols_copy = go(copy(cols.at[m], cols.at[m], "cols", 0, "sp", partner))
    phase("ticks")
    @pl.loop(0, pairs + delay)
    def _(tick):
        per = width // LANES

        @pl.when(jnp.logical_and(tick < pairs, lax.rem(tick, per) == 0))
        def _():
            piece = lanes(tick // per, width)
            arrive(copy(dysend.at[:, piece], dyin.at[mine0, piece], "dy", tick // per, "sp", partner))

        @pl.when(tick < pairs)
        def _():
            dy = dyin[:, lanes(tick, LANES)].astype(f32)
            dyef_ref[tick] = (dy * ef_ref[tick]).astype(bf16)
            dyeb_ref[tick] = (dy * eb_ref[tick]).astype(bf16)
            sr_ref[tick, 0] = mm(kt[...], veb_ref[tick])
            sr_ref[tick, 1] = mm(rt[...], dyeb_ref[tick])
            sl_ref[tick, 0] = mm(kt[...], vef_ref[tick])
            sl_ref[tick, 1] = mm(rt[...], dyef_ref[tick])

        jr = tick - SKEW * c

        @pl.when(jnp.logical_and(jr >= 0, jr < pairs))
        def _():
            with jax.named_scope("chain_r"):
                chain("right", jr, rin, sr_ref, rout, first, last, GROUPS)

        jl = tick - SKEW * (chunks - 1 - c)

        @pl.when(jnp.logical_and(jl >= 0, jl < pairs))
        def _():
            with jax.named_scope("chain_l"):
                chain("left", jl, lin, sl_ref, lout, last, first, -GROUPS)

        @pl.when(tick < pairs)
        def _():
            with jax.named_scope("intra"):
                intra(tick)

        @pl.when(tick == pairs - 1)
        def _():
            ge = gesum[...].astype(bf16)
            dksum[...] += mm(ge, rn[...])
            drsum[...] += mm_tn(ge, kn[...])

        @pl.when(tick >= delay)
        def _():
            with jax.named_scope("consume"):
                consume(tick - delay)

    phase("send_dbc")
    sbc = sbc_ref[...]
    dbin[body, :STATE] = (dksum[...] * sbc[:, :STATE]).astype(bf16)
    dbin[body, STATE:] = (drsum[...] * sbc[:, STATE:]).astype(bf16)
    go(
        copy(
            dbin.at[ch : HALO + ch, :], dbin.at[left_rows, :], "db_left", 0, "sp", near(GROUPS)
        ),
        jnp.logical_not(last),
    )
    go(
        copy(
            dbin.at[HALO : 2 * HALO, :], dbin.at[right_rows, :], "db_right", 0, "sp", near(-GROUPS)
        ),
        jnp.logical_not(first),
    )

    def send_edges(name, source, target):
        go(
            copy(
                source.at[ch - HALO :, :],
                target.at[m, :HALO, :],
                name + "_left",
                0,
                "sp",
                lax.rem((c + 1) * GROUPS, sp),
                into=m,
            ),
            jnp.logical_not(last),
        )
        go(
            copy(
                source.at[:HALO, :],
                target.at[m, HALO + tokens :, :],
                name + "_right",
                0,
                "sp",
                lax.rem(c * GROUPS - 1 + sp, sp),
                into=m,
            ),
            jnp.logical_not(first),
        )

    def await_edges(name, target):
        lead, trail = m == 0, m == GROUPS - 1
        for g in range(GROUPS):
            slot = target.at[g, :HALO, :]
            arrive(
                copy(slot, slot, name + "_left", g, "sp", partner),
                jnp.logical_and(lead, jnp.logical_not(first)),
            )
            slot = target.at[g, HALO + tokens :, :]
            arrive(
                copy(slot, slot, name + "_right", g, "sp", partner),
                jnp.logical_and(trail, jnp.logical_not(last)),
            )

        @pl.when(jnp.logical_and(lead, first))
        def _():
            target[:, :HALO, :] = jnp.zeros((GROUPS, HALO, target.shape[2]), bf16)

        @pl.when(jnp.logical_and(trail, last))
        def _():
            target[:, HALO + tokens :, :] = jnp.zeros((GROUPS, HALO, target.shape[2]), bf16)

    gx_copy(pairs - 1).start()
    send_edges("gx", dpx, gx)

    phase("ddt")
    w_fwd = []
    for o in range(1, ny):
        src = lax.rem(y - o + ny, ny) * cores + core
        for q in range(2):
            arrive(w_y[o - 1][q])
            if cores > 1:
                full = (wball, wcall)[q].at[src]
                w_fwd.append(go(copy(full, full, "w_fwd", 2 * o + q, "dp", other_core)))

    fill = jnp.zeros((LANES - gh, ch), f32)
    down = jnp.concatenate([colrow[...], fill], axis=0).T
    drate = jnp.dot(upper, dlev[...] - down, precision=highest, preferred_element_type=f32)
    drate = (drate - cross[0:1, :]).T[:gh]
    ddt = ((drate * twice(faderow[...]) + sdt[...].T[:gh]) * sigrow[...]).astype(bf16)
    for g in range(GROUPS):
        ddtsend[g] = ddt[:, g * tokens : (g + 1) * tokens]
    group_rows = pl.ds(pl.multiple_of(m * gh, gh), gh)
    ddt_copy = go(copy(ddtsend.at[p], ddt_ref.at[group_rows, :], "ddt", 0, "sp", partner))
    ddt_ref[group_rows, :] = ddtsend[m]

    phase("wait_db")
    await_halo("db", dbin)
    phase("conv_g")
    for q in range(2):
        at = slice(q * STATE, (q + 1) * STATE)
        taps = (tapb_ref, tapc_ref)[q][:, lanes(m, STATE)]
        gsend[:, at] = window_conv(dbin[:, at].astype(f32), taps, ch, True).astype(bf16)

    phase("send_g")
    halves = [slice(q * STATE, (q + 1) * STATE) for q in range(2)]

    def g_copy(source, block, name, index, q, peer):
        return go(
            copy(
                source.at[:, halves[q]],
                gall.at[block, :, halves[q]],
                name,
                2 * index + q,
                "dp",
                peer,
            )
        )

    g_y = {}
    g_core = {}
    for q in range(2):
        for o in range(1, ny):
            peer = lax.rem(y + o, ny) * cores + core
            g_y[o, q] = g_copy(gsend, me_dp, "g_y", o, q, peer)
        if cores > 1:
            g_core[q] = g_copy(gsend, me_dp, "g_core", 0, q, other_core)
    theirs = pl.ds(pl.multiple_of(p * tokens, HALO), tokens)
    hid_copy = go(copy(gsend.at[theirs, :], ghid.at[m], "gx_g", 0, "sp", partner))
    ghid[m] = gsend[mine0, :]
    gall[me_dp] = gsend[...]
    phase("wait_g")
    arrive(cols_copy)
    g_fwd = {}

    def forward_g(q):
        for o in range(1, ny):
            src = lax.rem(y - o + ny, ny) * cores + core
            arrive(g_y[o, q])
            if cores > 1:
                g_fwd[o, q] = g_copy(gall.at[src], src, "g_fwd", o, q, other_core)

    w2 = {}
    forward_g(0)
    for q in range(2):
        if cores > 1:
            arrive(g_core[q])
            for o in range(1, ny):
                arrive(g_fwd[o, q])
        if q == 0:
            forward_g(1)
        phase("dw")
        total = None
        for g in range(GROUPS):
            for i in range(dp):
                term = mm_tn(gall[i, g * tokens : (g + 1) * tokens, halves[q]], cols[g, i])
                total = term if total is None else total + term
        wown[q] = total.T.reshape(chunks, rows, STATE)
        wsend[q] = wown[q].astype(bf16)
        for o in range(1, chunks):
            k = lax.rem(c + o, chunks)
            w2[q, o] = go(
                copy(
                    wsend.at[q, k], w2in.at[q, c], "w2", q * chunks + o, "sp", k * GROUPS + m
                )
            )

    phase("d_hidden")
    for item in w_fwd:
        arrive(item)
    arrive(hid_copy)
    gb = jnp.concatenate([ghid[g, :, :STATE] for g in range(GROUPS)], axis=1)
    gc = jnp.concatenate([ghid[g, :, STATE:] for g in range(GROUPS)], axis=1)
    for i in range(dp):
        dh_ref[:, i * cw : (i + 1) * cw] = (mm_nt(gb, wball[i]) + mm_nt(gc, wcall[i])).astype(bf16)

    def input_gradient(g):
        @pl.loop(0, pairs)
        def _(j):
            taps = tapall[:, lanes(g * pairs + j, LANES)]
            part = gx[g, :, lanes(j, LANES)].astype(f32)
            dx_ref[:, lanes(g * pairs + j, LANES)] = window_conv(part, taps, tokens, True).astype(
                bf16
            )

    phase("wait_gx")
    @pl.loop(0, pairs)
    def _(j):
        gx_copy(j).wait_recv()

    await_edges("gx", gx)
    phase("w3")
    w3 = {}
    w4 = []
    for q in range(2):
        share = wown[q, c]
        for o in range(1, chunks):
            arrive(w2[q, o])
            share = share + w2in[q, lax.rem(c - o + chunks, chunks)].astype(f32)
        s3send[q] = share.astype(bf16)
        tall[q, m, c] = s3send[q]
        for o in range(1, chunks):
            k = lax.rem(c + o, chunks)
            w3[q, o] = go(
                copy(
                    s3send.at[q], tall.at[q, m, c], "w3", q * chunks + o, "sp", k * GROUPS + m
                )
            )
        w4.append(go(copy(s3send.at[q], tall.at[q, m, c], "w4", q * chunks, "sp", partner)))
        phase("dx")
        input_gradient(q)
    phase("w4")
    for q in range(2):
        for o in range(1, chunks):
            arrive(w3[q, o])
            piece = tall.at[q, m, lax.rem(c - o + chunks, chunks)]
            w4.append(go(copy(piece, piece, "w4", q * chunks + o, "sp", partner)))
    phase("last")
    arrive(ddt_copy)
    for item in w4:
        arrive(item)

    @pl.loop(0, pairs)
    def _(j):
        gx_copy(j).wait_send()

        @pl.when(jnp.logical_not(last))
        def _():
            for q in range(2):
                chain_copy("right", j, q, rin, rout, GROUPS).wait_send()

        @pl.when(jnp.logical_not(first))
        def _():
            for q in range(2):
                chain_copy("left", j, q, lin, lout, -GROUPS).wait_send()

    for item, cond in sent:
        if cond is None:
            item.wait_send()
        else:

            @pl.when(cond)
            def _():
                item.wait_send()

    phase.end()


def out_kernel(
    dgate, dx, dh, ddt, tall, dgate_out, dx_out, dh_out, ddt_out, dwb_out, dwc_out, wide, sems
):
    copies = [
        pltpu.make_async_copy(source, target, sems.at[at])
        for at, (source, target) in enumerate(
            (
                (dgate, dgate_out),
                (dx, dx_out),
                (dh, dh_out),
                (ddt, ddt_out),
                (wide.at[0], dwb_out),
                (wide.at[1], dwc_out),
            )
        )
    ]
    for item in copies[:4]:
        item.start()
    for q in range(2):
        for g in range(GROUPS):
            at = slice(g * STATE, (g + 1) * STATE)
            wide[q, :, at] = tall[q, g].astype(f32).reshape(wide.shape[1], STATE)
        copies[4 + q].start()
    for item in copies:
        item.wait()


def local(
    layer_activity,
    writer_matrix,
    reader_matrix,
    source_unfiltered,
    switch_raw_signal,
    saved_result,
    final_adjoint,
    delta_raw,
    extra_logdrop,
    source_filter_coefs,
    writer_filter_coefs,
    reader_filter_coefs,
    delta_offset,
    fading_exponents,
    direct_factor,
    rescale_factor,
):
    tokens, width_in = layer_activity.shape[1:]
    inner = source_unfiltered.shape[2]
    dp = lax.axis_size("dp")
    sp = lax.axis_size("sp")
    cores = 2 if dp % 2 == 0 else 1
    heads = delta_offset.shape[0]
    cw, latent = writer_matrix.shape
    xc = heads * HEAD_DIM
    xw = -(-xc // LANES) * LANES
    rows_h = -(-heads // 8) * 8
    chunks = sp // GROUPS
    ch = tokens * GROUPS
    gw = inner // GROUPS
    gh = HEADS // GROUPS
    pairs = gw // LANES
    rows = cw // chunks
    window = tokens * sp
    _, slots = slot_table(sp, dp, cores, pairs)

    vmem = pl.BlockSpec(memory_space=pltpu.VMEM)
    hbm = pl.BlockSpec(memory_space=pltpu.HBM)
    smem = pl.BlockSpec(memory_space=pltpu.SMEM)
    scratch = [
        ((tokens, width_in), bf16),
        ((cw, latent), bf16),
        ((cw, latent), bf16),
        ((tokens, inner), bf16),
        ((tokens, inner), bf16),
        ((tokens, inner), bf16),
        ((tokens, inner), bf16),
        ((dp, cw, latent), bf16),
        ((dp, cw, latent), bf16),
        ((GROUPS, dp, tokens, cw), bf16),
        ((dp // cores, tokens, cores * cw), bf16),
        ((dp // cores, tokens, 2 * latent), bf16),
        ((dp // cores, tokens, 2 * latent), bf16),
        ((tokens, 2 * latent), f32),
        ((ch + 2 * HALO, gw), bf16),
        ((ch, gw), bf16),
        ((tokens, gw), bf16),
        ((gh, ch), bf16),
        ((chunks, rows_h, ch + 2 * LANES), f32),
        ((chunks, rows_h, ch + 2 * LANES), f32),
        ((gh, ch + 2 * LANES), f32),
        ((8, xw), f32),
        ((sp, 8, xw), f32),
        ((8, inner), f32),
        ((GROUPS, tokens, 2 * STATE), bf16),
        ((ch + 2 * HALO, 2 * STATE), bf16),
        ((pairs, ch, LANES), f32),
        ((pairs, ch, LANES), f32),
        ((pairs, ch, LANES), f32),
        ((pairs, ch, LANES), f32),
        ((pairs, ch, LANES), f32),
        ((pairs, 8, LANES), f32),
        ((pairs, ch, LANES), bf16),
        ((pairs, ch, LANES), bf16),
        ((pairs, ch, LANES), bf16),
        ((pairs, ch, LANES), bf16),
        ((pairs, ch, LANES), bf16),
        ((ch, STATE), bf16),
        ((ch, STATE), bf16),
        ((STATE, ch), bf16),
        ((STATE, ch), bf16),
        ((ch, 2 * STATE), f32),
        ((ch, ch), f32),
        ((ch, ch), f32),
        ((ch, ch), f32),
        ((gh, ch, LANES), f32),
        ((gh, ch), f32),
        ((gh, ch), f32),
        ((gh, LANES), f32),
        ((pairs, ch, LANES), f32),
        ((pairs, 2, STATE, LANES), f32),
        ((pairs, 2, STATE, LANES), f32),
        ((pairs, 2, STATE, LANES), bf16),
        ((pairs, 2, STATE, LANES), bf16),
        ((pairs, 2, STATE, LANES), bf16),
        ((pairs, 2, STATE, LANES), bf16),
        ((ch, STATE), f32),
        ((ch, STATE), f32),
        ((ch, LANES), f32),
        ((ch, LANES), f32),
        ((8, LANES), f32),
        ((gh, ch), f32),
        ((ch, gw), bf16),
        ((GROUPS, tokens + 2 * HALO, gw), bf16),
        ((ch + 2 * HALO, 2 * STATE), bf16),
        ((GROUPS, gh, tokens), bf16),
        ((ch, 2 * STATE), bf16),
        ((GROUPS, tokens, 2 * STATE), bf16),
        ((dp, ch, 2 * STATE), bf16),
        ((2, chunks, rows, STATE), bf16),
        ((2, chunks, rows, STATE), f32),
        ((2, chunks, rows, STATE), bf16),
        ((2, rows, STATE), bf16),
    ]
    dgate, dx, ddt, dh, tall = pl.pallas_call(
        functools.partial(mega_kernel, heads, cores),
        in_specs=[hbm] * 7 + [vmem] * 6 + [smem] * 3,
        out_specs=[vmem] * 5,
        out_shape=[
            pltpu.VMEM((tokens, inner), bf16),
            pltpu.VMEM((tokens, inner), bf16),
            pltpu.VMEM((HEADS, tokens), bf16),
            pltpu.VMEM((tokens, width_in), bf16),
            pltpu.VMEM((2, GROUPS, chunks, rows, STATE), bf16),
        ],
        scratch_shapes=[pltpu.VMEM(shape, kind) for shape, kind in scratch]
        + [pltpu.SemaphoreType.DMA((slots,)), pltpu.SemaphoreType.DMA((slots,))]
        + [pltpu.SemaphoreType.DMA((7,))],
        compiler_params=pltpu.CompilerParams(
            collective_id=0, has_side_effects=True, vmem_limit_bytes=60 * 1024 * 1024
        ),
        name="mega",
    )(
        layer_activity.reshape(tokens, width_in),
        writer_matrix,
        reader_matrix,
        source_unfiltered.reshape(tokens, inner),
        switch_raw_signal.reshape(tokens, inner),
        saved_result.reshape(tokens, inner),
        final_adjoint.reshape(tokens, inner),
        delta_raw.reshape(tokens, HEADS).T,
        extra_logdrop.reshape(window, heads).T,
        source_filter_coefs,
        writer_filter_coefs,
        reader_filter_coefs,
        rescale_factor.reshape(1, inner),
        delta_offset,
        fading_exponents,
        direct_factor,
    )
    d_gate, d_x, d_hidden, d_dt, d_w_b, d_w_c = pl.pallas_call(
        out_kernel,
        in_specs=[vmem] * 5,
        out_specs=[hbm] * 6,
        scratch_shapes=[pltpu.VMEM((2, cw, latent), f32), pltpu.SemaphoreType.DMA((6,))],
        out_shape=[
            jax.ShapeDtypeStruct((tokens, inner), bf16),
            jax.ShapeDtypeStruct((tokens, inner), bf16),
            jax.ShapeDtypeStruct((tokens, width_in), bf16),
            jax.ShapeDtypeStruct((HEADS, tokens), bf16),
            jax.ShapeDtypeStruct((cw, latent), f32),
            jax.ShapeDtypeStruct((cw, latent), f32),
        ],
        name="outputs",
    )(*[pltpu.with_memory_space_constraint(v, pltpu.VMEM) for v in (dgate, dx, dh, ddt, tall)])
    return (
        d_hidden.reshape(1, tokens, width_in),
        d_x.reshape(1, tokens, inner),
        d_gate.reshape(1, tokens, inner),
        d_dt.T.reshape(1, tokens, HEADS),
        d_w_b,
        d_w_c,
    )


def solution(mesh):
    in_specs = (
        P("dp", "sp", None),
        P("dp", None),
        P("dp", None),
        P("dp", "sp", None),
        P("dp", "sp", None),
        P("dp", "sp", None),
        P("dp", "sp", None),
        P("dp", "sp", None),
        P("dp", None, "sp"),
        P(None, "sp"),
        P(),
        P(),
        P("sp"),
        P("sp"),
        P("sp"),
        P(),
    )
    out_specs = (
        P("dp", "sp", None),
        P("dp", "sp", None),
        P("dp", "sp", None),
        P("dp", "sp", None),
        P("dp", None),
        P("dp", None),
    )
    return jax.shard_map(local, mesh=mesh, in_specs=in_specs, out_specs=out_specs, check_vma=False)
```

```python
import functools

import jax
import jax.numpy as jnp
from jax import lax
from jax.experimental import pallas as pl
from jax.experimental.pallas import tpu as pltpu
from jax.sharding import PartitionSpec as P

HEADS = 32
HEAD_DIM = 64
STATE = 128
GROUPS = 2
NORM_GROUPS = 8
CONV_K = 5
LANES = 128
HALO = 16
SKEW = 3
PIECES = 4
EPSILON = 1e-06
LOG2E = 1.4426950408889634
highest = lax.Precision.HIGHEST
f32 = jnp.float32
bf16 = jnp.bfloat16
NT = (((1,), (1,)), ((), ()))
TN = (((0,), (0,)), ((), ()))


def sigmoid(v):
    return 1.0 / (1.0 + jnp.exp(-v))


def softplus(v):
    e = jnp.exp(-jnp.abs(v))
    z = e / (2.0 + e)
    z2 = z * z
    series = jnp.full_like(z, 1.0 / 17.0)
    for odd in (15, 13, 11, 9, 7, 5, 3, 1):
        series = series * z2 + 1.0 / odd
    return jnp.maximum(v, 0.0) + 2.0 * z * series


def mm(a, b):
    return jnp.dot(a, b, preferred_element_type=f32)


def mm_nt(a, b):
    return lax.dot_general(a, b, NT, preferred_element_type=f32)


def mm_tn(a, b):
    return lax.dot_general(a, b, TN, preferred_element_type=f32)


def split_mm(a, b):
    hi = a.astype(bf16)
    lo = (a - hi.astype(f32)).astype(bf16)
    return mm(hi, b) + mm(lo, b)


def window_conv(rows, taps, count, flip):
    total = None
    for k in range(CONV_K):
        shift = HALO - CONV_K // 2 + k
        tap = taps[CONV_K - 1 - k if flip else k][None, :]
        term = tap * pltpu.roll(rows, rows.shape[0] - shift, axis=0)[:count]
        total = term if total is None else total + term
    return total


def greet(axes):
    barrier = pltpu.get_barrier_semaphore()
    count = 0
    for axis in axes:
        size = lax.axis_size(axis)
        me = lax.axis_index(axis)
        for o in range(1, size):
            pl.semaphore_signal(
                barrier,
                inc=1,
                device_id={axis: lax.rem(me + o, size)},
                device_id_type=pl.DeviceIdType.MESH,
            )
            count += 1
    pl.semaphore_wait(barrier, count)


class Phases:
    def __init__(self):
        self.scope = None

    def __call__(self, name):
        self.end()
        self.scope = jax.named_scope(name)
        self.scope.__enter__()

    def end(self):
        if self.scope is not None:
            self.scope.__exit__(None, None, None)
            self.scope = None


def slot_tables(sp, dp, cores, pairs):
    others = dp // cores - 1
    chunks = sp // GROUPS
    away = max(chunks - 1, 1)
    counts = (
        ("w_y", 2 * others, 2 * others),
        ("w_core", 2, 2),
        ("w_fwd", 2 * others, 2 * others),
        ("la_y", PIECES * others, PIECES * others),
        ("la", others + 1, others + 1),
        ("p_y", PIECES * others, PIECES * others),
        ("x", 1, 1),
        ("x_left", 1, 1),
        ("x_right", 1, 1),
        ("dt", 1, 1),
        ("drop", 2, 1),
        ("tap", 1, 1),
        ("dy", 1, NORM_GROUPS // GROUPS),
        ("bc", PIECES, PIECES),
        ("bc_left", 1, 1),
        ("bc_right", 1, 1),
        ("right", 4, 2 * pairs),
        ("left", 4, 2 * pairs),
        ("gx", 1, 1),
        ("gx_left", 1, GROUPS),
        ("gx_right", 1, GROUPS),
        ("db_left", 1, 1),
        ("db_right", 1, 1),
        ("gx_g", 1, 1),
        ("cols", 1, 1),
        ("ddt", 1, 1),
        ("g_y", 2 * others, 2 * others),
        ("g_core", 2, 2),
        ("g_fwd", 2 * others, 2 * others),
        ("w2", 2, 2),
        ("w3", 2, 2 * away),
        ("w4", 1, 1),
    )
    sends, arrivals = {}, {}
    send_at = arrive_at = 0
    for name, send_count, arrive_count in counts:
        sends[name], arrivals[name] = send_at, arrive_at
        send_at += send_count
        arrive_at += arrive_count
    return sends, arrivals, max(send_at, 1), max(arrive_at, 1)


def mega_kernel(
    heads,
    cores,
    la_hbm,
    wb_hbm,
    wc_hbm,
    x_hbm,
    gates_hbm,
    values_hbm,
    adjoint_hbm,
    dt_ref,
    drop_ref,
    tapx_ref,
    tapb_ref,
    tapc_ref,
    scale_ref,
    offset_ref,
    fade_ref,
    skip_ref,
    dgate_ref,
    dx_ref,
    ddt_ref,
    dh_ref,
    tall,
    la_ref,
    wb_ref,
    wc_ref,
    x_ref,
    gates_ref,
    values_ref,
    adjoint_ref,
    wball,
    wcall,
    cols,
    lain,
    psend,
    pin,
    psum,
    xin,
    dyin,
    dysend,
    dtin,
    dropsend,
    dropin,
    drow,
    tapsend,
    tapin,
    tapall,
    bcsend,
    bcin,
    u_ref,
    sux_ref,
    dts_ref,
    ef_ref,
    eb_ref,
    tdec,
    vb_ref,
    vef_ref,
    veb_ref,
    dyef_ref,
    dyeb_ref,
    kn,
    rn,
    kt,
    rt,
    sbc_ref,
    score_ref,
    sign_ref,
    gesum,
    lcolb,
    lrow,
    sigrow,
    faderow,
    dv_ref,
    sr_ref,
    sl_ref,
    rin,
    lin,
    rout,
    lout,
    dksum,
    drsum,
    dlev,
    sdt,
    cross,
    colrow,
    dpx,
    gx,
    dbin,
    ddtsend,
    gsend,
    ghid,
    gall,
    wtot,
    wsend,
    wown,
    w2in,
    s3send,
    ss,
    rs,
    ls,
):
    dp = lax.axis_size("dp")
    sp = lax.axis_size("sp")
    me_dp = lax.axis_index("dp")
    me_sp = lax.axis_index("sp")
    ny = dp // cores
    chunks = sp // GROUPS
    y = me_dp // cores
    core = lax.rem(me_dp, cores)
    c = me_sp // GROUPS
    m = lax.rem(me_sp, GROUPS)
    p = GROUPS - 1 - m
    partner = c * GROUPS + p
    other_core = y * cores + (cores - 1 - core)
    tokens, inner = x_ref.shape
    gw = inner // GROUPS
    gh = HEADS // GROUPS
    ch = tokens * GROUPS
    pairs = gw // LANES
    cw = wb_ref.shape[0]
    latent = wb_ref.shape[1]
    xc = heads * HEAD_DIM
    nsrc = sp // GROUPS
    rows = cw // chunks
    first = c == 0
    last = c == chunks - 1
    sends, arrivals, _, _ = slot_tables(sp, dp, cores, pairs)
    sent = []

    def copy(src, dst, name, index, axis, peer, into=None):
        return pltpu.make_async_remote_copy(
            src_ref=src,
            dst_ref=dst,
            send_sem=ss.at[sends[name] + index],
            recv_sem=rs.at[arrivals[name] + (index if into is None else into)],
            device_id={axis: peer},
            device_id_type=pl.DeviceIdType.MESH,
        )

    def go(item, cond=None, alone=True):
        if cond is None:
            item.start()
        else:

            @pl.when(cond)
            def _():
                item.start()

        if alone:
            sent.append((item, cond))
        return item

    def together(name, index, region, cond=None):
        sent.append((copy(region, region, name, index, "sp", partner), cond))

    def arrive(item, cond=None):
        if cond is None:
            item.wait_recv()
        else:

            @pl.when(cond)
            def _():
                item.wait_recv()

    def lanes(index, width):
        return pl.ds(pl.multiple_of(index * width, LANES), width)

    def near(step):
        return lax.rem(me_sp + step + 2 * sp, sp)

    mine = pl.ds(pl.multiple_of(HALO + m * tokens, HALO), tokens)
    mine0 = pl.ds(pl.multiple_of(m * tokens, HALO), tokens)
    body = slice(HALO, HALO + ch)
    left_rows = slice(0, HALO)
    right_rows = slice(HALO + ch, 2 * HALO + ch)
    to_right = jnp.logical_and(m == GROUPS - 1, jnp.logical_not(last))
    to_left = jnp.logical_and(m == 0, jnp.logical_not(first))

    phase = Phases()
    phase("greet")
    loads = {}
    for at, (source, target) in enumerate(
        (
            (wb_hbm, wb_ref),
            (wc_hbm, wc_ref),
            (x_hbm, x_ref),
            (values_hbm, values_ref),
            (gates_hbm, gates_ref),
            (adjoint_hbm, adjoint_ref),
            (la_hbm, la_ref),
        )
    ):
        loads[at] = pltpu.make_async_copy(source, target, ls.at[at])
    for at in (6, 2, 0, 1, 3, 4, 5):
        loads[at].start()
    greet(("dp", "sp"))
    loads[6].wait()

    phase("send_first")
    cwy = cores * cw
    part_rows = tokens // PIECES
    parts = [slice(t * part_rows, (t + 1) * part_rows) for t in range(PIECES)]
    la_y = {}
    for t in range(PIECES):
        for o in range(1, ny):
            there = lax.rem(y + o, ny)
            la_y[o, t] = go(
                copy(
                    la_ref.at[parts[t], lanes(there, cwy)],
                    lain.at[y, parts[t], :],
                    "la_y",
                    PIECES * (o - 1) + t,
                    "dp",
                    there * cores + core,
                )
            )
    loads[2].wait()
    x_copy = go(copy(x_ref.at[:, lanes(p, gw)], xin.at[mine, :], "x", 0, "sp", partner))
    loads[0].wait()
    loads[1].wait()
    w_core = []
    if cores > 1:
        w_core = [
            go(copy(wb_ref, wball.at[me_dp], "w_core", 0, "dp", other_core)),
            go(copy(wc_ref, wcall.at[me_dp], "w_core", 1, "dp", other_core)),
        ]
    dt_copy = go(
        copy(
            dt_ref.at[pl.ds(pl.multiple_of(p * gh, gh), gh), :],
            dtin.at[:, lanes(m, tokens)],
            "dt",
            0,
            "sp",
            partner,
        )
    )

    def send_halo(name, source, target):
        for g in range(GROUPS):
            go(
                copy(
                    source(g, slice(tokens - HALO, tokens)),
                    target.at[left_rows, :],
                    name + "_left",
                    0,
                    "sp",
                    near(1 + g),
                    into=0,
                ),
                to_right,
                alone=False,
            )
            go(
                copy(
                    source(g, slice(0, HALO)),
                    target.at[right_rows, :],
                    name + "_right",
                    0,
                    "sp",
                    near(g - GROUPS),
                    into=0,
                ),
                to_left,
                alone=False,
            )
        together(name + "_left", 0, target.at[: GROUPS * HALO, :], to_right)
        together(name + "_right", 0, target.at[: GROUPS * HALO, :], to_left)

    def await_halo(name, target):
        arrive(
            copy(target.at[left_rows, :], target.at[left_rows, :], name + "_left", 0, "sp", partner),
            jnp.logical_not(first),
        )
        arrive(
            copy(target.at[right_rows, :], target.at[right_rows, :], name + "_right", 0, "sp", partner),
            jnp.logical_not(last),
        )

        @pl.when(first)
        def _():
            target[left_rows, :] = jnp.zeros((HALO, target.shape[1]), bf16)

        @pl.when(last)
        def _():
            target[right_rows, :] = jnp.zeros((HALO, target.shape[1]), bf16)

    send_halo("x", lambda g, r: x_ref.at[r, g * gw : (g + 1) * gw], xin)

    phase("params")
    rows_h = dropsend.shape[1]
    head_row = lax.broadcasted_iota(jnp.int32, (rows_h, LANES), 0)
    offsets = jnp.zeros((rows_h, LANES), f32)
    fades = jnp.zeros((rows_h, LANES), f32)
    for h in range(heads):
        offsets = jnp.where(head_row == h, offset_ref[h], offsets)
        fades = jnp.where(head_row == h, fade_ref[h], fades)
    dropsend[...] = jnp.zeros_like(dropsend)
    for k in range(chunks):
        dropsend[k, :heads, :ch] = drop_ref[:, k * ch : (k + 1) * ch]
        dropsend[k, :, ch : ch + LANES] = offsets
        dropsend[k, :, ch + LANES :] = fades
    owner = (me_sp * heads) // gh
    place = me_sp - owner * nsrc
    for o in range(chunks):
        k = lax.rem(c + o, chunks)
        go(
            copy(
                dropsend.at[k],
                dropin.at[place],
                "drop",
                0 if o else 1,
                "sp",
                k * GROUPS + owner if o else partner,
                into=0,
            ),
            None if o else owner != m,
            alone=not o,
        )
    if chunks > 1:
        together("drop", 0, dropsend.at[: chunks - 1])

    @pl.when(owner == m)
    def _():
        dropin[place] = dropsend[c]

    xw = tapsend.shape[1]
    tap_lane = lax.broadcasted_iota(jnp.int32, (1, xw), 1) // HEAD_DIM
    skips = jnp.zeros((1, xw), f32)
    for h in range(heads):
        skips = jnp.where(tap_lane == h, skip_ref[h], skips)
    tapsend[...] = jnp.zeros_like(tapsend)
    tapsend[:CONV_K, :xc] = tapx_ref[...]
    tapsend[CONV_K : CONV_K + 1, :] = skips
    for o in range(1, sp):
        go(copy(tapsend, tapin.at[me_sp], "tap", 0, "sp", lax.rem(me_sp + o, sp)), alone=False)
    all_taps = tapin.at[: sp - 1]
    together("tap", 0, all_taps)
    tapin[me_sp] = tapsend[...]
    la_copies = []
    if cores > 1:
        la_copies.append(
            go(copy(la_ref.at[:, lanes(other_core, cw)], cols.at[m, me_dp], "la", 0, "dp", other_core))
        )
    cols[m, me_dp] = la_ref[:, lanes(me_dp, cw)]
    wball[me_dp] = wb_ref[...]
    wcall[me_dp] = wc_ref[...]
    xin[mine, :] = x_ref[:, lanes(m, gw)]
    dtin[:, lanes(m, tokens)] = dt_ref[pl.ds(pl.multiple_of(m * gh, gh), gh), :]

    phase("norm")
    width = inner // NORM_GROUPS
    per_half = NORM_GROUPS // GROUPS
    early = per_half // 2
    dy_copies = []
    for at in (3, 4, 5):
        loads[at].wait()
    for half in range(GROUPS):
        who = p if half == 0 else m
        for i in range(per_half):
            span = lanes(who * per_half + i, width)
            values = values_ref[:, span].astype(f32)
            gates = gates_ref[:, span].astype(f32)
            sig = sigmoid(gates)
            act = gates * sig
            g = values * act
            dn = adjoint_ref[:, span].astype(f32) * scale_ref[:, span]
            inv = lax.rsqrt(jnp.sum(g * g, axis=1, keepdims=True) * (1.0 / width) + EPSILON)
            along = jnp.sum(dn * g, axis=1, keepdims=True) * (1.0 / width)
            dg = inv * dn - g * (inv * inv * inv * along)
            dgate_ref[:, span] = (dg * values * (sig + act * (1.0 - sig))).astype(bf16)
            dy = (dg * act).astype(bf16)
            at = slice(i * width, (i + 1) * width)
            if half == 0:
                dysend[:, at] = dy
                dy_copies.append(
                    copy(dysend.at[:, at], dyin.at[mine0, at], "dy", 0, "sp", partner, into=i)
                )
                if i < early:
                    go(dy_copies[i], alone=False)
            else:
                dyin[mine0, at] = dy

    phase("partial")
    for item in w_core:
        arrive(item)
    p_y = {}
    for t in range(PIECES):
        for o in range(1, ny):
            there = lax.rem(y - o + ny, ny)
            arrive(la_y[o, t])
            tb = tc = None
            for k in range(cores):
                part = lain[there, parts[t], k * cw : (k + 1) * cw]
                one, two = mm(part, wball[y * cores + k]), mm(part, wcall[y * cores + k])
                tb, tc = (one, two) if tb is None else (tb + one, tc + two)
            psend[there, parts[t], :latent] = tb.astype(bf16)
            psend[there, parts[t], latent:] = tc.astype(bf16)
            p_y[o, t] = go(
                copy(
                    psend.at[there, parts[t], :],
                    pin.at[y, parts[t], :],
                    "p_y",
                    PIECES * (o - 1) + t,
                    "dp",
                    there * cores + core,
                )
            )
    w_y = []
    for o in range(1, ny):
        peer = lax.rem(y + o, ny) * cores + core
        w_y.append(
            (
                go(copy(wb_ref, wball.at[me_dp], "w_y", 2 * o - 2, "dp", peer)),
                go(copy(wc_ref, wcall.at[me_dp], "w_y", 2 * o - 1, "dp", peer)),
            )
        )
    for o in range(1, ny):
        there = lax.rem(y - o + ny, ny)
        block = there * cores + core
        cols[m, block] = lain[there, :, lanes(core, cw)]
        if cores > 1:
            la_copies.append(
                go(
                    copy(
                        lain.at[there, :, lanes(cores - 1 - core, cw)],
                        cols.at[m, block],
                        "la",
                        o,
                        "dp",
                        other_core,
                    )
                )
            )
    total_b = total_c = None
    for k in range(cores):
        part = la_ref[:, lanes(y * cores + k, cw)]
        one, two = mm(part, wball[y * cores + k]), mm(part, wcall[y * cores + k])
        total_b, total_c = (one, two) if k == 0 else (total_b + one, total_c + two)
    psum[:, :latent] = total_b
    psum[:, latent:] = total_c
    phase("levels")
    arrive(dt_copy)
    if nsrc > 1:
        some = dropin.at[: nsrc - 1]
        arrive(copy(some, some, "drop", 0, "sp", partner), owner == m)
    arrive(copy(dropin, dropin, "drop", 0, "sp", partner), owner != m)
    for i in range(nsrc):
        drow[i * heads : (i + 1) * heads, :] = dropin[i, :heads, :]
    twice = lambda v: jnp.concatenate([v] * (ch // LANES), axis=1)
    fade = jnp.exp(drow[:, ch + LANES :])
    a = dtin[...].astype(f32) + twice(drow[:, ch : ch + LANES])
    dt = softplus(a)
    sigrow[...] = sigmoid(a)
    faderow[...] = fade
    rate = dt * twice(fade) + drow[:, :ch]
    row_i = lax.broadcasted_iota(jnp.int32, (ch, ch), 0)
    col_i = lax.broadcasted_iota(jnp.int32, (ch, ch), 1)
    upper = (row_i <= col_i).astype(f32)
    level = jnp.dot(rate, upper, precision=highest, preferred_element_type=f32) * LOG2E
    lrow[...] = level
    fill = jnp.zeros((LANES - gh, ch), f32)
    lcol = jnp.concatenate([level, fill], axis=0).T
    dtcol = jnp.concatenate([dt, fill], axis=0).T
    low_lane = lax.broadcasted_iota(jnp.int32, (ch, LANES), 1) < HEAD_DIM
    for j in range(pairs):
        pair = []
        for h in (2 * j, 2 * j + 1):
            wide = jnp.broadcast_to(lcol[:, h : h + 1], (ch, LANES))
            lcolb[h] = wide
            pair.append(wide)
        spread = jnp.where(low_lane, pair[0], pair[1])
        end = spread[ch - 1 : ch, :]
        ef_ref[j] = jnp.exp2(-spread)
        eb_ref[j] = jnp.exp2(spread - end)
        tdec[j] = jnp.broadcast_to(jnp.exp2(-end), (8, LANES))
        dts_ref[j] = jnp.where(low_lane, dtcol[:, 2 * j : 2 * j + 1], dtcol[:, 2 * j + 1 : 2 * j + 2])

    phase("project")
    bc_copies = []
    for t in range(PIECES):
        total = psum[parts[t], :]
        for o in range(1, ny):
            arrive(p_y[o, t])
            total = total + pin[lax.rem(y - o + ny, ny), parts[t], :].astype(f32)
        total = total.astype(bf16)
        for g in range(GROUPS):
            at = slice(g * STATE, (g + 1) * STATE)
            bcsend[g, parts[t], :STATE] = total[:, at]
            at = slice(latent + g * STATE, latent + (g + 1) * STATE)
            bcsend[g, parts[t], STATE:] = total[:, at]
        into = pl.ds(pl.multiple_of(HALO + m * tokens + t * part_rows, HALO), part_rows)
        bc_copies.append(
            go(copy(bcsend.at[p, parts[t], :], bcin.at[into, :], "bc", t, "sp", partner))
        )
    send_halo("bc", lambda g, r: bcsend.at[g, r, :], bcin)
    bcin[mine, :] = bcsend[m]
    for item in dy_copies[early:]:
        go(item, alone=False)
    together("dy", 0, dysend)

    phase("wait_x")
    arrive(copy(all_taps, all_taps, "tap", 0, "sp", partner))
    if xc % LANES == 0:
        for i in range(sp):
            tapall[:, i * xc : (i + 1) * xc] = tapin[i]
    else:
        per = LANES // xc
        for i in range(inner // LANES):
            tapall[:, i * LANES : (i + 1) * LANES] = jnp.concatenate(
                [tapin[i * per + q][:, :xc] for q in range(per)], axis=1
            )
    arrive(x_copy)
    await_halo("x", xin)

    phase("prep_x")
    @pl.loop(0, pairs)
    def _(j):
        taps = tapall[:, lanes(m * pairs + j, LANES)]
        pre = window_conv(xin[:, lanes(j, LANES)].astype(f32), taps, ch, False)
        sig = sigmoid(pre)
        u = pre * sig
        u_ref[j] = u
        sux_ref[j] = sig + u * (1.0 - sig)
        v = u * dts_ref[j]
        vb_ref[j] = v.astype(bf16)
        vef_ref[j] = (v * ef_ref[j]).astype(bf16)
        veb_ref[j] = (v * eb_ref[j]).astype(bf16)

    phase("wait_bc")
    for item in bc_copies:
        arrive(item)
    await_halo("bc", bcin)
    phase("conv_bc")
    for q in range(2):
        taps = (tapb_ref, tapc_ref)[q][:, lanes(m, STATE)]
        at = slice(q * STATE, (q + 1) * STATE)
        pre = window_conv(bcin[:, at].astype(f32), taps, ch, False)
        sig = sigmoid(pre)
        kr = pre * sig
        sbc_ref[:, at] = sig + kr * (1.0 - sig)
        (kn, rn)[q][...] = kr.astype(bf16)
        (kt, rt)[q][...] = kr.T.astype(bf16)
    score = mm_nt(kn[...], rn[...])
    score_ref[...] = score
    sign_ref[...] = score * jnp.clip(col_i - row_i, -1, 1).astype(f32)

    gesum[...] = jnp.zeros_like(gesum)
    dksum[...] = jnp.zeros_like(dksum)
    drsum[...] = jnp.zeros_like(drsum)
    dlev[...] = jnp.zeros_like(dlev)
    sdt[...] = jnp.zeros_like(sdt)
    cross[...] = jnp.zeros_like(cross)

    @pl.when(first)
    def _():
        rin[...] = jnp.zeros_like(rin)

    @pl.when(last)
    def _():
        lin[...] = jnp.zeros_like(lin)

    lane_low = lax.broadcasted_iota(jnp.int32, (1, LANES), 1) < HEAD_DIM
    masks = (lane_low.astype(bf16), 1.0 - lane_low.astype(bf16))
    pick_lane = lax.broadcasted_iota(jnp.int32, (LANES, LANES), 1)
    pick_half = lax.broadcasted_iota(jnp.int32, (LANES, LANES), 0) // HEAD_DIM
    block = min(ch, LANES)

    def intra(j):
        dyj = dyin[:, lanes(j, LANES)]
        for a in range(2):
            h = 2 * j + a
            lr = lrow[pl.ds(h, 1), :]
            dym = dyj * masks[a]
            onehot = (pick_lane == h).astype(bf16)
            below = None
            for b in range(ch // block):
                at = slice(b * block, (b + 1) * block)
                gap = twice(lcolb[h, at]) - lr
                decay = jnp.exp2(-jnp.abs(gap))
                ge = mm_nt(vb_ref[j, at] * masks[a], dyj) * decay
                gesum[at, :] += ge
                part = mm((score_ref[at, :] * decay).astype(bf16), dym)
                if a == 0:
                    dv_ref[j, at] = part
                else:
                    dv_ref[j, at] += part
                q = sign_ref[at, :] * ge
                down = jnp.sum(q, axis=0, keepdims=True)
                below = down if below is None else below + down
                part = q[:, :LANES]
                for piece in range(1, ch // LANES):
                    part = part + q[:, piece * LANES : (piece + 1) * LANES]
                dlev[at, :] += split_mm(part, onehot)
            colrow[pl.ds(h, 1), :] = below

    def gx_copy(j):
        return copy(
            dpx.at[pl.ds(pl.multiple_of(p * (tokens - HALO), HALO), tokens + HALO), lanes(j, LANES)],
            gx.at[
                m, pl.ds(pl.multiple_of(HALO - HALO * p, HALO), tokens + HALO), lanes(j, LANES)
            ],
            "gx",
            0,
            "sp",
            partner,
        )

    keep_src = pl.ds(pl.multiple_of(m * (tokens - HALO), HALO), tokens + HALO)
    keep_dst = pl.ds(pl.multiple_of(HALO - HALO * m, HALO), tokens + HALO)

    def consume(j):
        k, r = kn[...], rn[...]
        ra, rb, la, lb = rin[j, 0], rin[j, 1], lin[j, 0], lin[j, 1]
        ef, eb = ef_ref[j], eb_ref[j]
        u = u_ref[j]
        at = lanes(j, LANES)
        dy = dyin[:, at].astype(f32)
        v = vb_ref[j].astype(f32)
        skip = tapall[CONV_K : CONV_K + 1, lanes(m * pairs + j, LANES)]
        onehot = (pick_lane == 2 * j + pick_half).astype(bf16)
        dl, dr = ef * mm(k, rb), eb * mm(k, lb)
        ml, mr = ef * mm(r, ra), eb * mm(r, la)
        dv = dv_ref[j] + dl + dr
        dpx[:, at] = ((dv * dts_ref[j] + skip * dy) * sux_ref[j]).astype(bf16)

        @pl.when(j < pairs - 1)
        def _():
            gx_copy(j).start()

        gx[m, keep_dst, at] = dpx[keep_src, at]
        dksum[...] += mm_nt(vef_ref[j], rb) + mm_nt(veb_ref[j], lb)
        drsum[...] += mm_nt(dyef_ref[j], ra) + mm_nt(dyeb_ref[j], la)
        dlev[...] += split_mm(dy * (mr - ml) + v * (dr - dl), onehot)
        sdt[...] += split_mm(u * dv, onehot)
        over = lb.astype(f32) * rout[j, 0].astype(f32) + la.astype(f32) * rout[j, 1].astype(f32)
        over = jnp.broadcast_to(jnp.sum(over, axis=0, keepdims=True), (8, LANES))
        cross[...] += split_mm(over, onehot)

    def chain_copy(name, j, q, into_ref, out_ref, step):
        return copy(
            out_ref.at[j, q],
            into_ref.at[j, q],
            name,
            2 * lax.rem(j, 2) + q,
            "sp",
            near(step),
            into=2 * j + q,
        )

    def chain(name, j, into_ref, own_ref, out_ref, head, tail, step):
        decay = tdec[j][0:1, :]
        for q in range(2):
            item = chain_copy(name, j, q, into_ref, out_ref, step)

            @pl.when(jnp.logical_not(head))
            def _():
                item.wait_recv()

            out_ref[j, q] = (own_ref[j, q] + decay * into_ref[j, q].astype(f32)).astype(bf16)

            @pl.when(jnp.logical_not(tail))
            def _():
                @pl.when(j >= 2)
                def _():
                    chain_copy(name, j - 2, q, into_ref, out_ref, step).wait_send()

                item.start()

    delay = SKEW * (chunks - 1)

    for item in la_copies:
        arrive(item)
    cols_copy = go(copy(cols.at[m], cols.at[m], "cols", 0, "sp", partner))
    phase("ticks")
    @pl.loop(0, pairs + delay)
    def _(tick):
        per = width // LANES

        @pl.when(jnp.logical_and(tick < pairs, lax.rem(tick, per) == 0))
        def _():
            piece = lanes(tick // per, width)
            block = dyin.at[mine0, piece]
            arrive(copy(block, block, "dy", 0, "sp", partner, into=tick // per))

        @pl.when(tick < pairs)
        def _():
            dy = dyin[:, lanes(tick, LANES)].astype(f32)
            dyef_ref[tick] = (dy * ef_ref[tick]).astype(bf16)
            dyeb_ref[tick] = (dy * eb_ref[tick]).astype(bf16)
            sr_ref[tick, 0] = mm(kt[...], veb_ref[tick])
            sr_ref[tick, 1] = mm(rt[...], dyeb_ref[tick])
            sl_ref[tick, 0] = mm(kt[...], vef_ref[tick])
            sl_ref[tick, 1] = mm(rt[...], dyef_ref[tick])

        jr = tick - SKEW * c

        @pl.when(jnp.logical_and(jr >= 0, jr < pairs))
        def _():
            with jax.named_scope("chain_r"):
                chain("right", jr, rin, sr_ref, rout, first, last, GROUPS)

        jl = tick - SKEW * (chunks - 1 - c)

        @pl.when(jnp.logical_and(jl >= 0, jl < pairs))
        def _():
            with jax.named_scope("chain_l"):
                chain("left", jl, lin, sl_ref, lout, last, first, -GROUPS)

        @pl.when(tick < pairs)
        def _():
            with jax.named_scope("intra"):
                intra(tick)

        @pl.when(tick == pairs - 1)
        def _():
            ge = gesum[...].astype(bf16)
            dksum[...] += mm(ge, rn[...])
            drsum[...] += mm_tn(ge, kn[...])

        @pl.when(tick >= delay)
        def _():
            with jax.named_scope("consume"):
                consume(tick - delay)

    phase("send_dbc")
    sbc = sbc_ref[...]
    dbin[body, :STATE] = (dksum[...] * sbc[:, :STATE]).astype(bf16)
    dbin[body, STATE:] = (drsum[...] * sbc[:, STATE:]).astype(bf16)
    go(
        copy(
            dbin.at[ch : HALO + ch, :], dbin.at[left_rows, :], "db_left", 0, "sp", near(GROUPS)
        ),
        jnp.logical_not(last),
    )
    go(
        copy(
            dbin.at[HALO : 2 * HALO, :], dbin.at[right_rows, :], "db_right", 0, "sp", near(-GROUPS)
        ),
        jnp.logical_not(first),
    )

    def send_edges(name, source, target):
        go(
            copy(
                source.at[ch - HALO :, :],
                target.at[m, :HALO, :],
                name + "_left",
                0,
                "sp",
                lax.rem((c + 1) * GROUPS, sp),
                into=m,
            ),
            jnp.logical_not(last),
        )
        go(
            copy(
                source.at[:HALO, :],
                target.at[m, HALO + tokens :, :],
                name + "_right",
                0,
                "sp",
                lax.rem(c * GROUPS - 1 + sp, sp),
                into=m,
            ),
            jnp.logical_not(first),
        )

    def await_edges(name, target):
        lead, trail = m == 0, m == GROUPS - 1
        for g in range(GROUPS):
            slot = target.at[g, :HALO, :]
            arrive(
                copy(slot, slot, name + "_left", 0, "sp", partner, into=g),
                jnp.logical_and(lead, jnp.logical_not(first)),
            )
            slot = target.at[g, HALO + tokens :, :]
            arrive(
                copy(slot, slot, name + "_right", 0, "sp", partner, into=g),
                jnp.logical_and(trail, jnp.logical_not(last)),
            )

        @pl.when(jnp.logical_and(lead, first))
        def _():
            target[:, :HALO, :] = jnp.zeros((GROUPS, HALO, target.shape[2]), bf16)

        @pl.when(jnp.logical_and(trail, last))
        def _():
            target[:, HALO + tokens :, :] = jnp.zeros((GROUPS, HALO, target.shape[2]), bf16)

    gx_copy(pairs - 1).start()
    send_edges("gx", dpx, gx)

    phase("ddt")
    w_fwd = []
    for o in range(1, ny):
        src = lax.rem(y - o + ny, ny) * cores + core
        for q in range(2):
            arrive(w_y[o - 1][q])
            if cores > 1:
                full = (wball, wcall)[q].at[src]
                w_fwd.append(go(copy(full, full, "w_fwd", 2 * o - 2 + q, "dp", other_core)))

    fill = jnp.zeros((LANES - gh, ch), f32)
    down = jnp.concatenate([colrow[...], fill], axis=0).T
    drate = jnp.dot(upper, dlev[...] - down, precision=highest, preferred_element_type=f32)
    drate = (drate - cross[0:1, :]).T[:gh]
    ddt = ((drate * twice(faderow[...]) + sdt[...].T[:gh]) * sigrow[...]).astype(bf16)
    for g in range(GROUPS):
        ddtsend[g] = ddt[:, g * tokens : (g + 1) * tokens]
    group_rows = pl.ds(pl.multiple_of(m * gh, gh), gh)
    ddt_copy = go(copy(ddtsend.at[p], ddt_ref.at[group_rows, :], "ddt", 0, "sp", partner))
    ddt_ref[group_rows, :] = ddtsend[m]

    phase("wait_db")
    await_halo("db", dbin)
    phase("conv_g")
    for q in range(2):
        at = slice(q * STATE, (q + 1) * STATE)
        taps = (tapb_ref, tapc_ref)[q][:, lanes(m, STATE)]
        gsend[:, at] = window_conv(dbin[:, at].astype(f32), taps, ch, True).astype(bf16)

    phase("send_g")
    halves = [slice(q * STATE, (q + 1) * STATE) for q in range(2)]

    def g_copy(source, block, name, index, q, peer):
        return go(
            copy(
                source.at[:, halves[q]],
                gall.at[block, :, halves[q]],
                name,
                2 * index + q,
                "dp",
                peer,
            )
        )

    g_y = {}
    g_core = {}
    for q in range(2):
        for o in range(1, ny):
            peer = lax.rem(y + o, ny) * cores + core
            g_y[o, q] = g_copy(gsend, me_dp, "g_y", o - 1, q, peer)
        if cores > 1:
            g_core[q] = g_copy(gsend, me_dp, "g_core", 0, q, other_core)
    theirs = pl.ds(pl.multiple_of(p * tokens, HALO), tokens)
    hid_copy = go(copy(gsend.at[theirs, :], ghid.at[m], "gx_g", 0, "sp", partner))
    ghid[m] = gsend[mine0, :]
    gall[me_dp] = gsend[...]
    phase("wait_g")
    arrive(cols_copy)
    sources = {o: lax.rem(y - o + ny, ny) * cores + core for o in range(1, ny)}
    relayed = {o: lax.rem(y - o + ny, ny) * cores + cores - 1 - core for o in range(1, ny)}
    g_fwd = {}
    w2 = {}
    for q in range(2):
        for o in range(1, ny):
            if cores > 1:
                block = gall.at[sources[o], :, halves[q]]
                g_fwd[o, q] = copy(
                    block, block, "g_fwd", 2 * (o - 1) + q, "dp", other_core
                )
                sent.append((g_fwd[o, q], None))
        for o in range(1, chunks):
            k = lax.rem(c + o, chunks)
            w2[q, o] = copy(
                wsend.at[q, k], w2in.at[q, c], "w2", q, "sp", k * GROUPS + m
            )
        if chunks > 1:
            together("w2", q, w2in.at[q, : chunks - 1])

    def add_block(q, i, fresh=False):
        total = None
        for g in range(GROUPS):
            term = mm_tn(gall[i, g * tokens : (g + 1) * tokens, halves[q]], cols[g, i])
            total = term if total is None else total + term
        wtot[q] = total if fresh else wtot[q] + total

    def add_peers(q):
        for o in range(1, ny):
            arrive(g_y[o, q])
            if cores > 1:
                g_fwd[o, q].start()
            add_block(q, sources[o])

    def add_other_core(q):
        if cores > 1:
            arrive(g_core[q])
            add_block(q, other_core)
            for o in range(1, ny):
                arrive(g_fwd[o, q])
                add_block(q, relayed[o])

    def scatter(q):
        total = wtot[q].T.reshape(chunks, rows, STATE)
        wown[q] = total
        wsend[q] = total.astype(bf16)
        for o in range(1, chunks):
            w2[q, o].start()

    for q in range(2):
        add_block(q, me_dp, fresh=True)

    @pl.when(core == 0)
    def _():
        add_other_core(0)
        add_other_core(1)
        for q in range(2):
            add_peers(q)
            scatter(q)

    @pl.when(core != 0)
    def _():
        add_peers(0)
        add_peers(1)
        for q in range(2):
            add_other_core(q)
            scatter(q)

    phase("d_hidden")
    for item in w_fwd:
        arrive(item)
    arrive(hid_copy)
    gb = jnp.concatenate([ghid[g, :, :STATE] for g in range(GROUPS)], axis=1)
    gc = jnp.concatenate([ghid[g, :, STATE:] for g in range(GROUPS)], axis=1)
    for i in range(dp):
        dh_ref[:, i * cw : (i + 1) * cw] = (mm_nt(gb, wball[i]) + mm_nt(gc, wcall[i])).astype(bf16)

    def input_gradient(g):
        @pl.loop(0, pairs)
        def _(j):
            taps = tapall[:, lanes(g * pairs + j, LANES)]
            part = gx[g, :, lanes(j, LANES)].astype(f32)
            dx_ref[:, lanes(g * pairs + j, LANES)] = window_conv(part, taps, tokens, True).astype(
                bf16
            )

    phase("wait_gx")
    all_gx = gx.at[0, : tokens + HALO, :]
    arrive(copy(all_gx, all_gx, "gx", 0, "sp", partner))

    await_edges("gx", gx)
    phase("w3")
    w3 = {}
    for q in range(2):
        share = wown[q, c]
        if chunks > 1:
            arrive(copy(w2in.at[q, : chunks - 1], w2in.at[q, : chunks - 1], "w2", q, "sp", partner))
        for o in range(1, chunks):
            share = share + w2in[q, lax.rem(c - o + chunks, chunks)].astype(f32)
        s3send[q] = share.astype(bf16)
        tall[q, m, c] = s3send[q]
        for o in range(1, chunks):
            k = lax.rem(c + o, chunks)
            w3[q, o] = go(
                copy(
                    s3send.at[q],
                    tall.at[q, m, c],
                    "w3",
                    q,
                    "sp",
                    k * GROUPS + m,
                    into=q * (chunks - 1) + o - 1,
                ),
                alone=False,
            )
        if chunks > 1:
            together("w3", q, tall.at[q, m, : chunks - 1])
        go(copy(s3send.at[q], tall.at[q, m, c], "w4", 0, "sp", partner), alone=False)
        phase("dx")
        input_gradient(q)
    phase("w4")
    for q in range(2):
        for o in range(1, chunks):
            arrive(w3[q, o])
            piece = tall.at[q, m, lax.rem(c - o + chunks, chunks)]
            go(copy(piece, piece, "w4", 0, "sp", partner), alone=False)
    phase("last")
    arrive(ddt_copy)
    arrive(copy(tall.at[:, p], tall.at[:, p], "w4", 0, "sp", partner))
    together("w4", 0, tall.at[:, m])

    together("gx", 0, all_gx)
    for j in range(max(pairs - 2, 0), pairs):
        for q in range(2):
            sent.append((chain_copy("right", j, q, rin, rout, GROUPS), jnp.logical_not(last)))
            sent.append((chain_copy("left", j, q, lin, lout, -GROUPS), jnp.logical_not(first)))

    for item, cond in sent:
        if cond is None:
            item.wait_send()
        else:

            @pl.when(cond)
            def _():
                item.wait_send()

    phase.end()


def out_kernel(
    dgate, dx, dh, ddt, tall, dgate_out, dx_out, dh_out, ddt_out, dwb_out, dwc_out, wide, sems
):
    copies = [
        pltpu.make_async_copy(source, target, sems.at[at])
        for at, (source, target) in enumerate(
            (
                (dgate, dgate_out),
                (dx, dx_out),
                (dh, dh_out),
                (ddt, ddt_out),
                (wide.at[0], dwb_out),
                (wide.at[1], dwc_out),
            )
        )
    ]
    for item in copies[:4]:
        item.start()
    for q in range(2):
        for g in range(GROUPS):
            at = slice(g * STATE, (g + 1) * STATE)
            wide[q, :, at] = tall[q, g].astype(f32).reshape(wide.shape[1], STATE)
        copies[4 + q].start()
    for item in copies:
        item.wait()


def local(
    layer_activity,
    writer_matrix,
    reader_matrix,
    source_unfiltered,
    switch_raw_signal,
    saved_result,
    final_adjoint,
    delta_raw,
    extra_logdrop,
    source_filter_coefs,
    writer_filter_coefs,
    reader_filter_coefs,
    delta_offset,
    fading_exponents,
    direct_factor,
    rescale_factor,
):
    tokens, width_in = layer_activity.shape[1:]
    inner = source_unfiltered.shape[2]
    dp = lax.axis_size("dp")
    sp = lax.axis_size("sp")
    cores = 2 if dp % 2 == 0 else 1
    heads = delta_offset.shape[0]
    cw, latent = writer_matrix.shape
    xc = heads * HEAD_DIM
    xw = -(-xc // LANES) * LANES
    rows_h = -(-heads // 8) * 8
    chunks = sp // GROUPS
    ch = tokens * GROUPS
    gw = inner // GROUPS
    gh = HEADS // GROUPS
    pairs = gw // LANES
    rows = cw // chunks
    window = tokens * sp
    _, _, send_slots, arrival_slots = slot_tables(sp, dp, cores, pairs)

    vmem = pl.BlockSpec(memory_space=pltpu.VMEM)
    hbm = pl.BlockSpec(memory_space=pltpu.HBM)
    smem = pl.BlockSpec(memory_space=pltpu.SMEM)
    scratch = [
        ((tokens, width_in), bf16),
        ((cw, latent), bf16),
        ((cw, latent), bf16),
        ((tokens, inner), bf16),
        ((tokens, inner), bf16),
        ((tokens, inner), bf16),
        ((tokens, inner), bf16),
        ((dp, cw, latent), bf16),
        ((dp, cw, latent), bf16),
        ((GROUPS, dp, tokens, cw), bf16),
        ((dp // cores, tokens, cores * cw), bf16),
        ((dp // cores, tokens, 2 * latent), bf16),
        ((dp // cores, tokens, 2 * latent), bf16),
        ((tokens, 2 * latent), f32),
        ((ch + 2 * HALO, gw), bf16),
        ((ch, gw), bf16),
        ((tokens, gw), bf16),
        ((gh, ch), bf16),
        ((chunks, rows_h, ch + 2 * LANES), f32),
        ((chunks, rows_h, ch + 2 * LANES), f32),
        ((gh, ch + 2 * LANES), f32),
        ((8, xw), f32),
        ((sp, 8, xw), f32),
        ((8, inner), f32),
        ((GROUPS, tokens, 2 * STATE), bf16),
        ((ch + 2 * HALO, 2 * STATE), bf16),
        ((pairs, ch, LANES), f32),
        ((pairs, ch, LANES), f32),
        ((pairs, ch, LANES), f32),
        ((pairs, ch, LANES), f32),
        ((pairs, ch, LANES), f32),
        ((pairs, 8, LANES), f32),
        ((pairs, ch, LANES), bf16),
        ((pairs, ch, LANES), bf16),
        ((pairs, ch, LANES), bf16),
        ((pairs, ch, LANES), bf16),
        ((pairs, ch, LANES), bf16),
        ((ch, STATE), bf16),
        ((ch, STATE), bf16),
        ((STATE, ch), bf16),
        ((STATE, ch), bf16),
        ((ch, 2 * STATE), f32),
        ((ch, ch), f32),
        ((ch, ch), f32),
        ((ch, ch), f32),
        ((gh, ch, LANES), f32),
        ((gh, ch), f32),
        ((gh, ch), f32),
        ((gh, LANES), f32),
        ((pairs, ch, LANES), f32),
        ((pairs, 2, STATE, LANES), f32),
        ((pairs, 2, STATE, LANES), f32),
        ((pairs, 2, STATE, LANES), bf16),
        ((pairs, 2, STATE, LANES), bf16),
        ((pairs, 2, STATE, LANES), bf16),
        ((pairs, 2, STATE, LANES), bf16),
        ((ch, STATE), f32),
        ((ch, STATE), f32),
        ((ch, LANES), f32),
        ((ch, LANES), f32),
        ((8, LANES), f32),
        ((gh, ch), f32),
        ((ch, gw), bf16),
        ((GROUPS, tokens + 2 * HALO, gw), bf16),
        ((ch + 2 * HALO, 2 * STATE), bf16),
        ((GROUPS, gh, tokens), bf16),
        ((ch, 2 * STATE), bf16),
        ((GROUPS, tokens, 2 * STATE), bf16),
        ((dp, ch, 2 * STATE), bf16),
        ((2, STATE, cw), f32),
        ((2, chunks, rows, STATE), bf16),
        ((2, chunks, rows, STATE), f32),
        ((2, chunks, rows, STATE), bf16),
        ((2, rows, STATE), bf16),
    ]
    dgate, dx, ddt, dh, tall = pl.pallas_call(
        functools.partial(mega_kernel, heads, cores),
        in_specs=[hbm] * 7 + [vmem] * 6 + [smem] * 3,
        out_specs=[vmem] * 5,
        out_shape=[
            pltpu.VMEM((tokens, inner), bf16),
            pltpu.VMEM((tokens, inner), bf16),
            pltpu.VMEM((HEADS, tokens), bf16),
            pltpu.VMEM((tokens, width_in), bf16),
            pltpu.VMEM((2, GROUPS, chunks, rows, STATE), bf16),
        ],
        scratch_shapes=[pltpu.VMEM(shape, kind) for shape, kind in scratch]
        + [pltpu.SemaphoreType.DMA((send_slots,)), pltpu.SemaphoreType.DMA((arrival_slots,))]
        + [pltpu.SemaphoreType.DMA((7,))],
        compiler_params=pltpu.CompilerParams(
            collective_id=0, has_side_effects=True, vmem_limit_bytes=60 * 1024 * 1024
        ),
        name="mega",
    )(
        layer_activity.reshape(tokens, width_in),
        writer_matrix,
        reader_matrix,
        source_unfiltered.reshape(tokens, inner),
        switch_raw_signal.reshape(tokens, inner),
        saved_result.reshape(tokens, inner),
        final_adjoint.reshape(tokens, inner),
        delta_raw.reshape(tokens, HEADS).T,
        extra_logdrop.reshape(window, heads).T,
        source_filter_coefs,
        writer_filter_coefs,
        reader_filter_coefs,
        rescale_factor.reshape(1, inner),
        delta_offset,
        fading_exponents,
        direct_factor,
    )
    d_gate, d_x, d_hidden, d_dt, d_w_b, d_w_c = pl.pallas_call(
        out_kernel,
        in_specs=[vmem] * 5,
        out_specs=[hbm] * 6,
        scratch_shapes=[pltpu.VMEM((2, cw, latent), f32), pltpu.SemaphoreType.DMA((6,))],
        out_shape=[
            jax.ShapeDtypeStruct((tokens, inner), bf16),
            jax.ShapeDtypeStruct((tokens, inner), bf16),
            jax.ShapeDtypeStruct((tokens, width_in), bf16),
            jax.ShapeDtypeStruct((HEADS, tokens), bf16),
            jax.ShapeDtypeStruct((cw, latent), f32),
            jax.ShapeDtypeStruct((cw, latent), f32),
        ],
        name="outputs",
    )(*[pltpu.with_memory_space_constraint(v, pltpu.VMEM) for v in (dgate, dx, dh, ddt, tall)])
    return (
        d_hidden.reshape(1, tokens, width_in),
        d_x.reshape(1, tokens, inner),
        d_gate.reshape(1, tokens, inner),
        d_dt.T.reshape(1, tokens, HEADS),
        d_w_b,
        d_w_c,
    )


def solution(mesh):
    in_specs = (
        P("dp", "sp", None),
        P("dp", None),
        P("dp", None),
        P("dp", "sp", None),
        P("dp", "sp", None),
        P("dp", "sp", None),
        P("dp", "sp", None),
        P("dp", "sp", None),
        P("dp", None, "sp"),
        P(None, "sp"),
        P(),
        P(),
        P("sp"),
        P("sp"),
        P("sp"),
        P(),
    )
    out_specs = (
        P("dp", "sp", None),
        P("dp", "sp", None),
        P("dp", "sp", None),
        P("dp", "sp", None),
        P("dp", None),
        P("dp", None),
    )
    return jax.shard_map(local, mesh=mesh, in_specs=in_specs, out_specs=out_specs, check_vma=False)
```

```python
import functools

import jax
import jax.numpy as jnp
from jax import lax
from jax.experimental import pallas as pl
from jax.experimental.pallas import tpu as pltpu
from jax.sharding import PartitionSpec as P

HEADS = 32
HEAD_DIM = 64
STATE = 128
GROUPS = 2
NORM_GROUPS = 8
CONV_K = 5
LANES = 128
HALO = 16
SKEW = 3
PIECES = 4
EPSILON = 1e-06
LOG2E = 1.4426950408889634
highest = lax.Precision.HIGHEST
f32 = jnp.float32
bf16 = jnp.bfloat16
NT = (((1,), (1,)), ((), ()))
TN = (((0,), (0,)), ((), ()))


def sigmoid(v):
    return 1.0 / (1.0 + jnp.exp(-v))


def softplus(v):
    e = jnp.exp(-jnp.abs(v))
    z = e / (2.0 + e)
    z2 = z * z
    series = jnp.full_like(z, 1.0 / 17.0)
    for odd in (15, 13, 11, 9, 7, 5, 3, 1):
        series = series * z2 + 1.0 / odd
    return jnp.maximum(v, 0.0) + 2.0 * z * series


def mm(a, b):
    return jnp.dot(a, b, preferred_element_type=f32)


def mm_nt(a, b):
    return lax.dot_general(a, b, NT, preferred_element_type=f32)


def mm_tn(a, b):
    return lax.dot_general(a, b, TN, preferred_element_type=f32)


def split_mm(a, b):
    hi = a.astype(bf16)
    lo = (a - hi.astype(f32)).astype(bf16)
    return mm(hi, b) + mm(lo, b)


def window_conv(rows, taps, count, flip):
    total = None
    for k in range(CONV_K):
        shift = HALO - CONV_K // 2 + k
        tap = taps[CONV_K - 1 - k if flip else k][None, :]
        term = tap * pltpu.roll(rows, rows.shape[0] - shift, axis=0)[:count]
        total = term if total is None else total + term
    return total


def greet(axes):
    barrier = pltpu.get_barrier_semaphore()
    count = 0
    for axis in axes:
        size = lax.axis_size(axis)
        me = lax.axis_index(axis)
        for o in range(1, size):
            pl.semaphore_signal(
                barrier,
                inc=1,
                device_id={axis: lax.rem(me + o, size)},
                device_id_type=pl.DeviceIdType.MESH,
            )
            count += 1
    pl.semaphore_wait(barrier, count)


class Phases:
    def __init__(self):
        self.scope = None

    def __call__(self, name):
        self.end()
        self.scope = jax.named_scope(name)
        self.scope.__enter__()

    def end(self):
        if self.scope is not None:
            self.scope.__exit__(None, None, None)
            self.scope = None


def slot_tables(sp, dp, cores, pairs):
    others = dp // cores - 1
    chunks = sp // GROUPS
    away = max(chunks - 1, 1)
    counts = (
        ("w_y", 2 * others, 2 * others),
        ("w_core", 2, 2),
        ("w_fwd", 2 * others, 2 * others),
        ("la_y", PIECES * others, PIECES * others),
        ("la", others + 1, others + 1),
        ("p_y", PIECES * others, PIECES * others),
        ("x", 1, 1),
        ("x_left", 1, 1),
        ("x_right", 1, 1),
        ("dt", 1, 1),
        ("drop", 2, 1),
        ("tap", 1, 1),
        ("dy", 1, NORM_GROUPS // GROUPS),
        ("bc", PIECES, PIECES),
        ("bc_left", 1, 1),
        ("bc_right", 1, 1),
        ("right", 4, 2 * pairs),
        ("left", 4, 2 * pairs),
        ("gx", 1, 1),
        ("gx_left", 1, GROUPS),
        ("gx_right", 1, GROUPS),
        ("db_left", 1, 1),
        ("db_right", 1, 1),
        ("gx_g", 1, 1),
        ("cols", 1, 1),
        ("ddt", 1, 1),
        ("g_y", 2 * others, 2 * others),
        ("g_core", 2, 2),
        ("g_fwd", 2 * others, 2 * others),
        ("w2", 2, 2),
        ("w3", 2, 2 * away),
        ("w4", 1, 1),
    )
    sends, arrivals = {}, {}
    send_at = arrive_at = 0
    for name, send_count, arrive_count in counts:
        sends[name], arrivals[name] = send_at, arrive_at
        send_at += send_count
        arrive_at += arrive_count
    return sends, arrivals, max(send_at, 1), max(arrive_at, 1)


def mega_kernel(
    heads,
    cores,
    la_hbm,
    wb_hbm,
    wc_hbm,
    x_hbm,
    gates_hbm,
    values_hbm,
    adjoint_hbm,
    dt_hbm,
    drop_hbm,
    tapx_hbm,
    tapb_hbm,
    tapc_hbm,
    scale_hbm,
    offset_hbm,
    fade_hbm,
    skip_hbm,
    dgate_ref,
    dx_ref,
    ddt_ref,
    dh_ref,
    tall,
    la_ref,
    wb_ref,
    wc_ref,
    x_ref,
    gates_ref,
    values_ref,
    adjoint_ref,
    dt_ref,
    drop_ref,
    tapx_ref,
    tapb_ref,
    tapc_ref,
    scale_ref,
    offset_ref,
    fade_ref,
    skip_ref,
    wball,
    wcall,
    cols,
    lain,
    psend,
    pin,
    psum,
    xin,
    dyin,
    dysend,
    dtin,
    dropsend,
    dropin,
    drow,
    tapsend,
    tapin,
    tapall,
    bcsend,
    bcin,
    u_ref,
    sux_ref,
    dts_ref,
    ef_ref,
    eb_ref,
    tdec,
    vb_ref,
    vef_ref,
    veb_ref,
    dyef_ref,
    dyeb_ref,
    kn,
    rn,
    kt,
    rt,
    sbc_ref,
    score_ref,
    sign_ref,
    gesum,
    lcolb,
    lrow,
    sigrow,
    faderow,
    dv_ref,
    sr_ref,
    sl_ref,
    rin,
    lin,
    rout,
    lout,
    dksum,
    drsum,
    dlev,
    sdt,
    cross,
    colrow,
    dpx,
    gx,
    dbin,
    ddtsend,
    gsend,
    ghid,
    gall,
    wtot,
    wsend,
    wown,
    w2in,
    s3send,
    ss,
    rs,
    ls,
):
    dp = lax.axis_size("dp")
    sp = lax.axis_size("sp")
    me_dp = lax.axis_index("dp")
    me_sp = lax.axis_index("sp")
    ny = dp // cores
    chunks = sp // GROUPS
    y = me_dp // cores
    core = lax.rem(me_dp, cores)
    c = me_sp // GROUPS
    m = lax.rem(me_sp, GROUPS)
    p = GROUPS - 1 - m
    partner = c * GROUPS + p
    other_core = y * cores + (cores - 1 - core)
    tokens, inner = x_ref.shape
    gw = inner // GROUPS
    gh = HEADS // GROUPS
    ch = tokens * GROUPS
    pairs = gw // LANES
    cw = wb_ref.shape[0]
    latent = wb_ref.shape[1]
    xc = heads * HEAD_DIM
    nsrc = sp // GROUPS
    rows = cw // chunks
    first = c == 0
    last = c == chunks - 1
    sends, arrivals, _, _ = slot_tables(sp, dp, cores, pairs)
    sent = []

    def copy(src, dst, name, index, axis, peer, into=None):
        return pltpu.make_async_remote_copy(
            src_ref=src,
            dst_ref=dst,
            send_sem=ss.at[sends[name] + index],
            recv_sem=rs.at[arrivals[name] + (index if into is None else into)],
            device_id={axis: peer},
            device_id_type=pl.DeviceIdType.MESH,
        )

    def go(item, cond=None, alone=True):
        if cond is None:
            item.start()
        else:

            @pl.when(cond)
            def _():
                item.start()

        if alone:
            sent.append((item, cond))
        return item

    def together(name, index, region, cond=None):
        sent.append((copy(region, region, name, index, "sp", partner), cond))

    def arrive(item, cond=None):
        if cond is None:
            item.wait_recv()
        else:

            @pl.when(cond)
            def _():
                item.wait_recv()

    def lanes(index, width):
        return pl.ds(pl.multiple_of(index * width, LANES), width)

    def near(step):
        return lax.rem(me_sp + step + 2 * sp, sp)

    mine = pl.ds(pl.multiple_of(HALO + m * tokens, HALO), tokens)
    mine0 = pl.ds(pl.multiple_of(m * tokens, HALO), tokens)
    body = slice(HALO, HALO + ch)
    left_rows = slice(0, HALO)
    right_rows = slice(HALO + ch, 2 * HALO + ch)
    to_right = jnp.logical_and(m == GROUPS - 1, jnp.logical_not(last))
    to_left = jnp.logical_and(m == 0, jnp.logical_not(first))

    phase = Phases()
    phase("greet")
    loads = {}
    for at, (source, target) in enumerate(
        (
            (wb_hbm, wb_ref),
            (wc_hbm, wc_ref),
            (x_hbm, x_ref),
            (values_hbm, values_ref),
            (gates_hbm, gates_ref),
            (adjoint_hbm, adjoint_ref),
            (la_hbm, la_ref),
            (dt_hbm, dt_ref),
            (drop_hbm, drop_ref),
            (tapx_hbm, tapx_ref),
            (tapb_hbm, tapb_ref),
            (tapc_hbm, tapc_ref),
            (scale_hbm, scale_ref),
            (offset_hbm, offset_ref),
            (fade_hbm, fade_ref),
            (skip_hbm, skip_ref),
        )
    ):
        loads[at] = pltpu.make_async_copy(source, target, ls.at[at])
    for at in (6, 2, 0, 1, *range(7, 16), 3, 4, 5):
        loads[at].start()
    greet(("dp", "sp"))
    loads[6].wait()

    phase("send_first")
    cwy = cores * cw
    part_rows = tokens // PIECES
    parts = [slice(t * part_rows, (t + 1) * part_rows) for t in range(PIECES)]
    la_y = {}
    for t in range(PIECES):
        for o in range(1, ny):
            there = lax.rem(y + o, ny)
            la_y[o, t] = go(
                copy(
                    la_ref.at[parts[t], lanes(there, cwy)],
                    lain.at[y, parts[t], :],
                    "la_y",
                    PIECES * (o - 1) + t,
                    "dp",
                    there * cores + core,
                )
            )
    loads[2].wait()
    x_copy = go(copy(x_ref.at[:, lanes(p, gw)], xin.at[mine, :], "x", 0, "sp", partner))
    loads[0].wait()
    loads[1].wait()
    w_core = []
    if cores > 1:
        w_core = [
            go(copy(wb_ref, wball.at[me_dp], "w_core", 0, "dp", other_core)),
            go(copy(wc_ref, wcall.at[me_dp], "w_core", 1, "dp", other_core)),
        ]
    for at in range(7, 16):
        loads[at].wait()
    dt_copy = go(
        copy(
            dt_ref.at[pl.ds(pl.multiple_of(p * gh, gh), gh), :],
            dtin.at[:, lanes(m, tokens)],
            "dt",
            0,
            "sp",
            partner,
        )
    )

    def send_halo(name, source, target):
        for g in range(GROUPS):
            go(
                copy(
                    source(g, slice(tokens - HALO, tokens)),
                    target.at[left_rows, :],
                    name + "_left",
                    0,
                    "sp",
                    near(1 + g),
                    into=0,
                ),
                to_right,
                alone=False,
            )
            go(
                copy(
                    source(g, slice(0, HALO)),
                    target.at[right_rows, :],
                    name + "_right",
                    0,
                    "sp",
                    near(g - GROUPS),
                    into=0,
                ),
                to_left,
                alone=False,
            )
        together(name + "_left", 0, target.at[: GROUPS * HALO, :], to_right)
        together(name + "_right", 0, target.at[: GROUPS * HALO, :], to_left)

    def await_halo(name, target):
        arrive(
            copy(target.at[left_rows, :], target.at[left_rows, :], name + "_left", 0, "sp", partner),
            jnp.logical_not(first),
        )
        arrive(
            copy(target.at[right_rows, :], target.at[right_rows, :], name + "_right", 0, "sp", partner),
            jnp.logical_not(last),
        )

        @pl.when(first)
        def _():
            target[left_rows, :] = jnp.zeros((HALO, target.shape[1]), bf16)

        @pl.when(last)
        def _():
            target[right_rows, :] = jnp.zeros((HALO, target.shape[1]), bf16)

    send_halo("x", lambda g, r: x_ref.at[r, g * gw : (g + 1) * gw], xin)

    phase("params")
    rows_h = dropsend.shape[1]
    head_row = lax.broadcasted_iota(jnp.int32, (rows_h, LANES), 0)
    offsets = jnp.zeros((rows_h, LANES), f32)
    fades = jnp.zeros((rows_h, LANES), f32)
    head_lane = lax.broadcasted_iota(jnp.int32, (1, heads), 1)

    def pick(ref, h):
        return jnp.sum(jnp.where(head_lane == h, ref[...], 0.0), axis=1, keepdims=True)

    for h in range(heads):
        offsets = jnp.where(head_row == h, pick(offset_ref, h), offsets)
        fades = jnp.where(head_row == h, pick(fade_ref, h), fades)
    dropsend[...] = jnp.zeros_like(dropsend)
    for k in range(chunks):
        dropsend[k, :heads, :ch] = drop_ref[:, k * ch : (k + 1) * ch]
        dropsend[k, :, ch : ch + LANES] = offsets
        dropsend[k, :, ch + LANES :] = fades
    owner = (me_sp * heads) // gh
    place = me_sp - owner * nsrc
    for o in range(chunks):
        k = lax.rem(c + o, chunks)
        go(
            copy(
                dropsend.at[k],
                dropin.at[place],
                "drop",
                0 if o else 1,
                "sp",
                k * GROUPS + owner if o else partner,
                into=0,
            ),
            None if o else owner != m,
            alone=not o,
        )
    if chunks > 1:
        together("drop", 0, dropsend.at[: chunks - 1])

    @pl.when(owner == m)
    def _():
        dropin[place] = dropsend[c]

    xw = tapsend.shape[1]
    tap_lane = lax.broadcasted_iota(jnp.int32, (1, xw), 1) // HEAD_DIM
    skips = jnp.zeros((1, xw), f32)
    for h in range(heads):
        skips = jnp.where(tap_lane == h, pick(skip_ref, h), skips)
    tapsend[...] = jnp.zeros_like(tapsend)
    tapsend[:CONV_K, :xc] = tapx_ref[...]
    tapsend[CONV_K : CONV_K + 1, :] = skips
    for o in range(1, sp):
        go(copy(tapsend, tapin.at[me_sp], "tap", 0, "sp", lax.rem(me_sp + o, sp)), alone=False)
    all_taps = tapin.at[: sp - 1]
    together("tap", 0, all_taps)
    tapin[me_sp] = tapsend[...]
    la_copies = []
    if cores > 1:
        la_copies.append(
            go(copy(la_ref.at[:, lanes(other_core, cw)], cols.at[m, me_dp], "la", 0, "dp", other_core))
        )
    cols[m, me_dp] = la_ref[:, lanes(me_dp, cw)]
    wball[me_dp] = wb_ref[...]
    wcall[me_dp] = wc_ref[...]
    xin[mine, :] = x_ref[:, lanes(m, gw)]
    dtin[:, lanes(m, tokens)] = dt_ref[pl.ds(pl.multiple_of(m * gh, gh), gh), :]

    phase("norm")
    width = inner // NORM_GROUPS
    per_half = NORM_GROUPS // GROUPS
    early = per_half // 2
    dy_copies = []
    for at in (3, 4, 5):
        loads[at].wait()
    for half in range(GROUPS):
        who = p if half == 0 else m
        for i in range(per_half):
            span = lanes(who * per_half + i, width)
            values = values_ref[:, span].astype(f32)
            gates = gates_ref[:, span].astype(f32)
            sig = sigmoid(gates)
            act = gates * sig
            g = values * act
            dn = adjoint_ref[:, span].astype(f32) * scale_ref[:, span]
            inv = lax.rsqrt(jnp.sum(g * g, axis=1, keepdims=True) * (1.0 / width) + EPSILON)
            along = jnp.sum(dn * g, axis=1, keepdims=True) * (1.0 / width)
            dg = inv * dn - g * (inv * inv * inv * along)
            dgate_ref[:, span] = (dg * values * (sig + act * (1.0 - sig))).astype(bf16)
            dy = (dg * act).astype(bf16)
            at = slice(i * width, (i + 1) * width)
            if half == 0:
                dysend[:, at] = dy
                dy_copies.append(
                    copy(dysend.at[:, at], dyin.at[mine0, at], "dy", 0, "sp", partner, into=i)
                )
                if i < early:
                    go(dy_copies[i], alone=False)
            else:
                dyin[mine0, at] = dy

    phase("partial")
    for item in w_core:
        arrive(item)
    p_y = {}
    for t in range(PIECES):
        for o in range(1, ny):
            there = lax.rem(y - o + ny, ny)
            arrive(la_y[o, t])
            tb = tc = None
            for k in range(cores):
                part = lain[there, parts[t], k * cw : (k + 1) * cw]
                one, two = mm(part, wball[y * cores + k]), mm(part, wcall[y * cores + k])
                tb, tc = (one, two) if tb is None else (tb + one, tc + two)
            psend[there, parts[t], :latent] = tb.astype(bf16)
            psend[there, parts[t], latent:] = tc.astype(bf16)
            p_y[o, t] = go(
                copy(
                    psend.at[there, parts[t], :],
                    pin.at[y, parts[t], :],
                    "p_y",
                    PIECES * (o - 1) + t,
                    "dp",
                    there * cores + core,
                )
            )
    w_y = []
    for o in range(1, ny):
        peer = lax.rem(y + o, ny) * cores + core
        w_y.append(
            (
                go(copy(wb_ref, wball.at[me_dp], "w_y", 2 * o - 2, "dp", peer)),
                go(copy(wc_ref, wcall.at[me_dp], "w_y", 2 * o - 1, "dp", peer)),
            )
        )
    for o in range(1, ny):
        there = lax.rem(y - o + ny, ny)
        block = there * cores + core
        cols[m, block] = lain[there, :, lanes(core, cw)]
        if cores > 1:
            la_copies.append(
                go(
                    copy(
                        lain.at[there, :, lanes(cores - 1 - core, cw)],
                        cols.at[m, block],
                        "la",
                        o,
                        "dp",
                        other_core,
                    )
                )
            )
    total_b = total_c = None
    for k in range(cores):
        part = la_ref[:, lanes(y * cores + k, cw)]
        one, two = mm(part, wball[y * cores + k]), mm(part, wcall[y * cores + k])
        total_b, total_c = (one, two) if k == 0 else (total_b + one, total_c + two)
    psum[:, :latent] = total_b
    psum[:, latent:] = total_c
    phase("project")
    bc_copies = []
    for t in range(PIECES):
        total = psum[parts[t], :]
        for o in range(1, ny):
            arrive(p_y[o, t])
            total = total + pin[lax.rem(y - o + ny, ny), parts[t], :].astype(f32)
        total = total.astype(bf16)
        for g in range(GROUPS):
            at = slice(g * STATE, (g + 1) * STATE)
            bcsend[g, parts[t], :STATE] = total[:, at]
            at = slice(latent + g * STATE, latent + (g + 1) * STATE)
            bcsend[g, parts[t], STATE:] = total[:, at]
        into = pl.ds(pl.multiple_of(HALO + m * tokens + t * part_rows, HALO), part_rows)
        bc_copies.append(
            go(copy(bcsend.at[p, parts[t], :], bcin.at[into, :], "bc", t, "sp", partner))
        )
    send_halo("bc", lambda g, r: bcsend.at[g, r, :], bcin)
    bcin[mine, :] = bcsend[m]
    for item in dy_copies[early:]:
        go(item, alone=False)
    together("dy", 0, dysend)

    phase("levels")
    arrive(dt_copy)
    if nsrc > 1:
        some = dropin.at[: nsrc - 1]
        arrive(copy(some, some, "drop", 0, "sp", partner), owner == m)
    arrive(copy(dropin, dropin, "drop", 0, "sp", partner), owner != m)
    for i in range(nsrc):
        drow[i * heads : (i + 1) * heads, :] = dropin[i, :heads, :]
    twice = lambda v: jnp.concatenate([v] * (ch // LANES), axis=1)
    fade = jnp.exp(drow[:, ch + LANES :])
    a = dtin[...].astype(f32) + twice(drow[:, ch : ch + LANES])
    dt = softplus(a)
    sigrow[...] = sigmoid(a)
    faderow[...] = fade
    rate = dt * twice(fade) + drow[:, :ch]
    row_i = lax.broadcasted_iota(jnp.int32, (ch, ch), 0)
    col_i = lax.broadcasted_iota(jnp.int32, (ch, ch), 1)
    upper = (row_i <= col_i).astype(f32)
    level = jnp.dot(rate, upper, precision=highest, preferred_element_type=f32) * LOG2E
    lrow[...] = level
    fill = jnp.zeros((LANES - gh, ch), f32)
    lcol = jnp.concatenate([level, fill], axis=0).T
    dtcol = jnp.concatenate([dt, fill], axis=0).T
    low_lane = lax.broadcasted_iota(jnp.int32, (ch, LANES), 1) < HEAD_DIM
    for j in range(pairs):
        pair = []
        for h in (2 * j, 2 * j + 1):
            wide = jnp.broadcast_to(lcol[:, h : h + 1], (ch, LANES))
            lcolb[h] = wide
            pair.append(wide)
        spread = jnp.where(low_lane, pair[0], pair[1])
        end = spread[ch - 1 : ch, :]
        ef_ref[j] = jnp.exp2(-spread)
        eb_ref[j] = jnp.exp2(spread - end)
        tdec[j] = jnp.broadcast_to(jnp.exp2(-end), (8, LANES))
        dts_ref[j] = jnp.where(low_lane, dtcol[:, 2 * j : 2 * j + 1], dtcol[:, 2 * j + 1 : 2 * j + 2])

    phase("wait_x")
    arrive(copy(all_taps, all_taps, "tap", 0, "sp", partner))
    if xc % LANES == 0:
        for i in range(sp):
            tapall[:, i * xc : (i + 1) * xc] = tapin[i]
    else:
        per = LANES // xc
        for i in range(inner // LANES):
            tapall[:, i * LANES : (i + 1) * LANES] = jnp.concatenate(
                [tapin[i * per + q][:, :xc] for q in range(per)], axis=1
            )
    arrive(x_copy)
    await_halo("x", xin)

    phase("prep_x")
    @pl.loop(0, pairs)
    def _(j):
        taps = tapall[:, lanes(m * pairs + j, LANES)]
        pre = window_conv(xin[:, lanes(j, LANES)].astype(f32), taps, ch, False)
        sig = sigmoid(pre)
        u = pre * sig
        u_ref[j] = u
        sux_ref[j] = sig + u * (1.0 - sig)
        v = u * dts_ref[j]
        vb_ref[j] = v.astype(bf16)
        vef_ref[j] = (v * ef_ref[j]).astype(bf16)
        veb_ref[j] = (v * eb_ref[j]).astype(bf16)

    phase("wait_bc")
    for item in bc_copies:
        arrive(item)
    await_halo("bc", bcin)
    phase("conv_bc")
    for q in range(2):
        taps = (tapb_ref, tapc_ref)[q][:, lanes(m, STATE)]
        at = slice(q * STATE, (q + 1) * STATE)
        pre = window_conv(bcin[:, at].astype(f32), taps, ch, False)
        sig = sigmoid(pre)
        kr = pre * sig
        sbc_ref[:, at] = sig + kr * (1.0 - sig)
        (kn, rn)[q][...] = kr.astype(bf16)
        (kt, rt)[q][...] = kr.T.astype(bf16)
    score = mm_nt(kn[...], rn[...])
    score_ref[...] = score
    sign_ref[...] = score * jnp.clip(col_i - row_i, -1, 1).astype(f32)

    gesum[...] = jnp.zeros_like(gesum)
    dksum[...] = jnp.zeros_like(dksum)
    drsum[...] = jnp.zeros_like(drsum)
    dlev[...] = jnp.zeros_like(dlev)
    sdt[...] = jnp.zeros_like(sdt)
    cross[...] = jnp.zeros_like(cross)

    @pl.when(first)
    def _():
        rin[...] = jnp.zeros_like(rin)

    @pl.when(last)
    def _():
        lin[...] = jnp.zeros_like(lin)

    lane_low = lax.broadcasted_iota(jnp.int32, (1, LANES), 1) < HEAD_DIM
    masks = (lane_low.astype(bf16), 1.0 - lane_low.astype(bf16))
    pick_lane = lax.broadcasted_iota(jnp.int32, (LANES, LANES), 1)
    pick_half = lax.broadcasted_iota(jnp.int32, (LANES, LANES), 0) // HEAD_DIM
    block = min(ch, LANES)

    def intra(j):
        dyj = dyin[:, lanes(j, LANES)]
        for a in range(2):
            h = 2 * j + a
            lr = lrow[pl.ds(h, 1), :]
            dym = dyj * masks[a]
            onehot = (pick_lane == h).astype(bf16)
            below = None
            for b in range(ch // block):
                at = slice(b * block, (b + 1) * block)
                gap = twice(lcolb[h, at]) - lr
                decay = jnp.exp2(-jnp.abs(gap))
                ge = mm_nt(vb_ref[j, at] * masks[a], dyj) * decay
                gesum[at, :] += ge
                part = mm((score_ref[at, :] * decay).astype(bf16), dym)
                if a == 0:
                    dv_ref[j, at] = part
                else:
                    dv_ref[j, at] += part
                q = sign_ref[at, :] * ge
                down = jnp.sum(q, axis=0, keepdims=True)
                below = down if below is None else below + down
                part = q[:, :LANES]
                for piece in range(1, ch // LANES):
                    part = part + q[:, piece * LANES : (piece + 1) * LANES]
                dlev[at, :] += split_mm(part, onehot)
            colrow[pl.ds(h, 1), :] = below

    def gx_copy(j):
        return copy(
            dpx.at[pl.ds(pl.multiple_of(p * (tokens - HALO), HALO), tokens + HALO), lanes(j, LANES)],
            gx.at[
                m, pl.ds(pl.multiple_of(HALO - HALO * p, HALO), tokens + HALO), lanes(j, LANES)
            ],
            "gx",
            0,
            "sp",
            partner,
        )

    keep_src = pl.ds(pl.multiple_of(m * (tokens - HALO), HALO), tokens + HALO)
    keep_dst = pl.ds(pl.multiple_of(HALO - HALO * m, HALO), tokens + HALO)

    def consume(j):
        k, r = kn[...], rn[...]
        ra, rb, la, lb = rin[j, 0], rin[j, 1], lin[j, 0], lin[j, 1]
        ef, eb = ef_ref[j], eb_ref[j]
        u = u_ref[j]
        at = lanes(j, LANES)
        dy = dyin[:, at].astype(f32)
        v = vb_ref[j].astype(f32)
        skip = tapall[CONV_K : CONV_K + 1, lanes(m * pairs + j, LANES)]
        onehot = (pick_lane == 2 * j + pick_half).astype(bf16)
        dl, dr = ef * mm(k, rb), eb * mm(k, lb)
        ml, mr = ef * mm(r, ra), eb * mm(r, la)
        dv = dv_ref[j] + dl + dr
        dpx[:, at] = ((dv * dts_ref[j] + skip * dy) * sux_ref[j]).astype(bf16)

        @pl.when(j < pairs - 1)
        def _():
            gx_copy(j).start()

        gx[m, keep_dst, at] = dpx[keep_src, at]
        dksum[...] += mm_nt(vef_ref[j], rb) + mm_nt(veb_ref[j], lb)
        drsum[...] += mm_nt(dyef_ref[j], ra) + mm_nt(dyeb_ref[j], la)
        dlev[...] += split_mm(dy * (mr - ml) + v * (dr - dl), onehot)
        sdt[...] += split_mm(u * dv, onehot)
        over = lb.astype(f32) * rout[j, 0].astype(f32) + la.astype(f32) * rout[j, 1].astype(f32)
        over = jnp.broadcast_to(jnp.sum(over, axis=0, keepdims=True), (8, LANES))
        cross[...] += split_mm(over, onehot)

    def chain_copy(name, j, q, into_ref, out_ref, step):
        return copy(
            out_ref.at[j, q],
            into_ref.at[j, q],
            name,
            2 * lax.rem(j, 2) + q,
            "sp",
            near(step),
            into=2 * j + q,
        )

    def chain(name, j, into_ref, own_ref, out_ref, head, tail, step):
        decay = tdec[j][0:1, :]
        for q in range(2):
            item = chain_copy(name, j, q, into_ref, out_ref, step)

            @pl.when(jnp.logical_not(head))
            def _():
                item.wait_recv()

            out_ref[j, q] = (own_ref[j, q] + decay * into_ref[j, q].astype(f32)).astype(bf16)

            @pl.when(jnp.logical_not(tail))
            def _():
                @pl.when(j >= 2)
                def _():
                    chain_copy(name, j - 2, q, into_ref, out_ref, step).wait_send()

                item.start()

    delay = SKEW * (chunks - 1)

    for item in la_copies:
        arrive(item)
    cols_copy = go(copy(cols.at[m], cols.at[m], "cols", 0, "sp", partner))
    phase("ticks")
    @pl.loop(0, pairs + delay)
    def _(tick):
        per = width // LANES

        @pl.when(jnp.logical_and(tick < pairs, lax.rem(tick, per) == 0))
        def _():
            piece = lanes(tick // per, width)
            block = dyin.at[mine0, piece]
            arrive(copy(block, block, "dy", 0, "sp", partner, into=tick // per))

        @pl.when(tick < pairs)
        def _():
            dy = dyin[:, lanes(tick, LANES)].astype(f32)
            dyef_ref[tick] = (dy * ef_ref[tick]).astype(bf16)
            dyeb_ref[tick] = (dy * eb_ref[tick]).astype(bf16)
            sr_ref[tick, 0] = mm(kt[...], veb_ref[tick])
            sr_ref[tick, 1] = mm(rt[...], dyeb_ref[tick])
            sl_ref[tick, 0] = mm(kt[...], vef_ref[tick])
            sl_ref[tick, 1] = mm(rt[...], dyef_ref[tick])

        jl = tick - SKEW * (chunks - 1 - c)

        @pl.when(jnp.logical_and(jl >= 0, jl < pairs))
        def _():
            with jax.named_scope("chain_l"):
                chain("left", jl, lin, sl_ref, lout, last, first, -GROUPS)

        jr = tick - SKEW * c

        @pl.when(jnp.logical_and(jr >= 0, jr < pairs))
        def _():
            with jax.named_scope("chain_r"):
                chain("right", jr, rin, sr_ref, rout, first, last, GROUPS)

        @pl.when(tick < pairs)
        def _():
            with jax.named_scope("intra"):
                intra(tick)

        @pl.when(tick == pairs - 1)
        def _():
            ge = gesum[...].astype(bf16)
            dksum[...] += mm(ge, rn[...])
            drsum[...] += mm_tn(ge, kn[...])

        @pl.when(tick >= delay)
        def _():
            with jax.named_scope("consume"):
                consume(tick - delay)

    phase("send_dbc")
    sbc = sbc_ref[...]
    dbin[body, :STATE] = (dksum[...] * sbc[:, :STATE]).astype(bf16)
    dbin[body, STATE:] = (drsum[...] * sbc[:, STATE:]).astype(bf16)
    go(
        copy(
            dbin.at[ch : HALO + ch, :], dbin.at[left_rows, :], "db_left", 0, "sp", near(GROUPS)
        ),
        jnp.logical_not(last),
    )
    go(
        copy(
            dbin.at[HALO : 2 * HALO, :], dbin.at[right_rows, :], "db_right", 0, "sp", near(-GROUPS)
        ),
        jnp.logical_not(first),
    )

    def send_edges(name, source, target):
        go(
            copy(
                source.at[ch - HALO :, :],
                target.at[m, :HALO, :],
                name + "_left",
                0,
                "sp",
                lax.rem((c + 1) * GROUPS, sp),
                into=m,
            ),
            jnp.logical_not(last),
        )
        go(
            copy(
                source.at[:HALO, :],
                target.at[m, HALO + tokens :, :],
                name + "_right",
                0,
                "sp",
                lax.rem(c * GROUPS - 1 + sp, sp),
                into=m,
            ),
            jnp.logical_not(first),
        )

    def await_edges(name, target):
        lead, trail = m == 0, m == GROUPS - 1
        for g in range(GROUPS):
            slot = target.at[g, :HALO, :]
            arrive(
                copy(slot, slot, name + "_left", 0, "sp", partner, into=g),
                jnp.logical_and(lead, jnp.logical_not(first)),
            )
            slot = target.at[g, HALO + tokens :, :]
            arrive(
                copy(slot, slot, name + "_right", 0, "sp", partner, into=g),
                jnp.logical_and(trail, jnp.logical_not(last)),
            )

        @pl.when(jnp.logical_and(lead, first))
        def _():
            target[:, :HALO, :] = jnp.zeros((GROUPS, HALO, target.shape[2]), bf16)

        @pl.when(jnp.logical_and(trail, last))
        def _():
            target[:, HALO + tokens :, :] = jnp.zeros((GROUPS, HALO, target.shape[2]), bf16)

    gx_copy(pairs - 1).start()
    send_edges("gx", dpx, gx)

    phase("wait_db")
    await_halo("db", dbin)
    phase("conv_g")
    for q in range(2):
        at = slice(q * STATE, (q + 1) * STATE)
        taps = (tapb_ref, tapc_ref)[q][:, lanes(m, STATE)]
        gsend[:, at] = window_conv(dbin[:, at].astype(f32), taps, ch, True).astype(bf16)

    phase("send_g")
    halves = [slice(q * STATE, (q + 1) * STATE) for q in range(2)]

    def g_copy(source, block, name, index, q, peer):
        return go(
            copy(
                source.at[:, halves[q]],
                gall.at[block, :, halves[q]],
                name,
                2 * index + q,
                "dp",
                peer,
            )
        )

    g_y = {}
    g_core = {}
    for q in range(2):
        for o in range(1, ny):
            peer = lax.rem(y + o, ny) * cores + core
            g_y[o, q] = g_copy(gsend, me_dp, "g_y", o - 1, q, peer)
        if cores > 1:
            g_core[q] = g_copy(gsend, me_dp, "g_core", 0, q, other_core)
    theirs = pl.ds(pl.multiple_of(p * tokens, HALO), tokens)
    hid_copy = go(copy(gsend.at[theirs, :], ghid.at[m], "gx_g", 0, "sp", partner))
    ghid[m] = gsend[mine0, :]
    gall[me_dp] = gsend[...]
    phase("ddt")
    w_fwd = []
    for o in range(1, ny):
        src = lax.rem(y - o + ny, ny) * cores + core
        for q in range(2):
            arrive(w_y[o - 1][q])
            if cores > 1:
                full = (wball, wcall)[q].at[src]
                w_fwd.append(go(copy(full, full, "w_fwd", 2 * o - 2 + q, "dp", other_core)))

    fill = jnp.zeros((LANES - gh, ch), f32)
    down = jnp.concatenate([colrow[...], fill], axis=0).T
    drate = jnp.dot(upper, dlev[...] - down, precision=highest, preferred_element_type=f32)
    drate = (drate - cross[0:1, :]).T[:gh]
    ddt = ((drate * twice(faderow[...]) + sdt[...].T[:gh]) * sigrow[...]).astype(bf16)
    for g in range(GROUPS):
        ddtsend[g] = ddt[:, g * tokens : (g + 1) * tokens]
    group_rows = pl.ds(pl.multiple_of(m * gh, gh), gh)
    ddt_copy = go(copy(ddtsend.at[p], ddt_ref.at[group_rows, :], "ddt", 0, "sp", partner))
    ddt_ref[group_rows, :] = ddtsend[m]

    phase("wait_g")
    arrive(cols_copy)
    sources = {o: lax.rem(y - o + ny, ny) * cores + core for o in range(1, ny)}
    relayed = {o: lax.rem(y - o + ny, ny) * cores + cores - 1 - core for o in range(1, ny)}
    g_fwd = {}
    w2 = {}
    for q in range(2):
        for o in range(1, ny):
            if cores > 1:
                block = gall.at[sources[o], :, halves[q]]
                g_fwd[o, q] = copy(
                    block, block, "g_fwd", 2 * (o - 1) + q, "dp", other_core
                )
                sent.append((g_fwd[o, q], None))
        for o in range(1, chunks):
            k = lax.rem(c + o, chunks)
            w2[q, o] = copy(
                wsend.at[q, k], w2in.at[q, c], "w2", q, "sp", k * GROUPS + m
            )
        if chunks > 1:
            together("w2", q, w2in.at[q, : chunks - 1])

    def add_block(q, i, fresh=False):
        total = None
        for g in range(GROUPS):
            term = mm_tn(gall[i, g * tokens : (g + 1) * tokens, halves[q]], cols[g, i])
            total = term if total is None else total + term
        wtot[q] = total if fresh else wtot[q] + total

    def add_peers(q):
        for o in range(1, ny):
            arrive(g_y[o, q])
            if cores > 1:
                g_fwd[o, q].start()
            add_block(q, sources[o])

    def add_other_core(q):
        if cores > 1:
            arrive(g_core[q])
            add_block(q, other_core)
            for o in range(1, ny):
                arrive(g_fwd[o, q])
                add_block(q, relayed[o])

    def scatter(q):
        total = wtot[q].T.reshape(chunks, rows, STATE)
        wown[q] = total
        wsend[q] = total.astype(bf16)
        for o in range(1, chunks):
            w2[q, o].start()

    for q in range(2):
        add_block(q, me_dp, fresh=True)

    @pl.when(core == 0)
    def _():
        add_other_core(0)
        add_other_core(1)
        for q in range(2):
            add_peers(q)
            scatter(q)

    @pl.when(core != 0)
    def _():
        add_peers(0)
        add_peers(1)
        for q in range(2):
            add_other_core(q)
            scatter(q)

    phase("d_hidden")
    for item in w_fwd:
        arrive(item)
    arrive(hid_copy)
    gb = jnp.concatenate([ghid[g, :, :STATE] for g in range(GROUPS)], axis=1)
    gc = jnp.concatenate([ghid[g, :, STATE:] for g in range(GROUPS)], axis=1)
    for i in range(dp):
        dh_ref[:, i * cw : (i + 1) * cw] = (mm_nt(gb, wball[i]) + mm_nt(gc, wcall[i])).astype(bf16)

    def input_gradient(g):
        @pl.loop(0, pairs)
        def _(j):
            taps = tapall[:, lanes(g * pairs + j, LANES)]
            part = gx[g, :, lanes(j, LANES)].astype(f32)
            dx_ref[:, lanes(g * pairs + j, LANES)] = window_conv(part, taps, tokens, True).astype(
                bf16
            )

    phase("wait_gx")
    all_gx = gx.at[0, : tokens + HALO, :]
    arrive(copy(all_gx, all_gx, "gx", 0, "sp", partner))

    await_edges("gx", gx)
    phase("w3")
    w3 = {}
    for q in range(2):
        share = wown[q, c]
        if chunks > 1:
            arrive(copy(w2in.at[q, : chunks - 1], w2in.at[q, : chunks - 1], "w2", q, "sp", partner))
        for o in range(1, chunks):
            share = share + w2in[q, lax.rem(c - o + chunks, chunks)].astype(f32)
        s3send[q] = share.astype(bf16)
        tall[q, m, c] = s3send[q]
        for o in range(1, chunks):
            k = lax.rem(c + o, chunks)
            w3[q, o] = go(
                copy(
                    s3send.at[q],
                    tall.at[q, m, c],
                    "w3",
                    q,
                    "sp",
                    k * GROUPS + m,
                    into=q * (chunks - 1) + o - 1,
                ),
                alone=False,
            )
        if chunks > 1:
            together("w3", q, tall.at[q, m, : chunks - 1])
        go(copy(s3send.at[q], tall.at[q, m, c], "w4", 0, "sp", partner), alone=False)
        phase("dx")
        input_gradient(q)
    phase("w4")
    for q in range(2):
        for o in range(1, chunks):
            arrive(w3[q, o])
            piece = tall.at[q, m, lax.rem(c - o + chunks, chunks)]
            go(copy(piece, piece, "w4", 0, "sp", partner), alone=False)
    phase("last")
    arrive(ddt_copy)
    arrive(copy(tall.at[:, p], tall.at[:, p], "w4", 0, "sp", partner))
    together("w4", 0, tall.at[:, m])

    together("gx", 0, all_gx)
    for j in range(max(pairs - 2, 0), pairs):
        for q in range(2):
            sent.append((chain_copy("right", j, q, rin, rout, GROUPS), jnp.logical_not(last)))
            sent.append((chain_copy("left", j, q, lin, lout, -GROUPS), jnp.logical_not(first)))

    for item, cond in sent:
        if cond is None:
            item.wait_send()
        else:

            @pl.when(cond)
            def _():
                item.wait_send()

    phase.end()


def out_kernel(
    dgate, dx, dh, ddt, tall, dgate_out, dx_out, dh_out, ddt_out, dwb_out, dwc_out, wide, sems
):
    copies = [
        pltpu.make_async_copy(source, target, sems.at[at])
        for at, (source, target) in enumerate(
            (
                (dgate, dgate_out),
                (dx, dx_out),
                (dh, dh_out),
                (ddt, ddt_out),
                (wide.at[0], dwb_out),
                (wide.at[1], dwc_out),
            )
        )
    ]
    for item in copies[:4]:
        item.start()
    for q in range(2):
        for g in range(GROUPS):
            at = slice(g * STATE, (g + 1) * STATE)
            wide[q, :, at] = tall[q, g].astype(f32).reshape(wide.shape[1], STATE)
        copies[4 + q].start()
    for item in copies:
        item.wait()


def local(
    layer_activity,
    writer_matrix,
    reader_matrix,
    source_unfiltered,
    switch_raw_signal,
    saved_result,
    final_adjoint,
    delta_raw,
    extra_logdrop,
    source_filter_coefs,
    writer_filter_coefs,
    reader_filter_coefs,
    delta_offset,
    fading_exponents,
    direct_factor,
    rescale_factor,
):
    tokens, width_in = layer_activity.shape[1:]
    inner = source_unfiltered.shape[2]
    dp = lax.axis_size("dp")
    sp = lax.axis_size("sp")
    cores = 2 if dp % 2 == 0 else 1
    heads = delta_offset.shape[0]
    cw, latent = writer_matrix.shape
    xc = heads * HEAD_DIM
    xw = -(-xc // LANES) * LANES
    rows_h = -(-heads // 8) * 8
    chunks = sp // GROUPS
    ch = tokens * GROUPS
    gw = inner // GROUPS
    gh = HEADS // GROUPS
    pairs = gw // LANES
    rows = cw // chunks
    window = tokens * sp
    _, _, send_slots, arrival_slots = slot_tables(sp, dp, cores, pairs)

    vmem = pl.BlockSpec(memory_space=pltpu.VMEM)
    hbm = pl.BlockSpec(memory_space=pltpu.HBM)
    scratch = [
        ((tokens, width_in), bf16),
        ((cw, latent), bf16),
        ((cw, latent), bf16),
        ((tokens, inner), bf16),
        ((tokens, inner), bf16),
        ((tokens, inner), bf16),
        ((tokens, inner), bf16),
        ((HEADS, tokens), bf16),
        ((heads, window), f32),
        ((CONV_K, xc), f32),
        ((CONV_K, latent), f32),
        ((CONV_K, latent), f32),
        ((1, inner), f32),
        ((1, heads), f32),
        ((1, heads), f32),
        ((1, heads), f32),
        ((dp, cw, latent), bf16),
        ((dp, cw, latent), bf16),
        ((GROUPS, dp, tokens, cw), bf16),
        ((dp // cores, tokens, cores * cw), bf16),
        ((dp // cores, tokens, 2 * latent), bf16),
        ((dp // cores, tokens, 2 * latent), bf16),
        ((tokens, 2 * latent), f32),
        ((ch + 2 * HALO, gw), bf16),
        ((ch, gw), bf16),
        ((tokens, gw), bf16),
        ((gh, ch), bf16),
        ((chunks, rows_h, ch + 2 * LANES), f32),
        ((chunks, rows_h, ch + 2 * LANES), f32),
        ((gh, ch + 2 * LANES), f32),
        ((8, xw), f32),
        ((sp, 8, xw), f32),
        ((8, inner), f32),
        ((GROUPS, tokens, 2 * STATE), bf16),
        ((ch + 2 * HALO, 2 * STATE), bf16),
        ((pairs, ch, LANES), f32),
        ((pairs, ch, LANES), f32),
        ((pairs, ch, LANES), f32),
        ((pairs, ch, LANES), f32),
        ((pairs, ch, LANES), f32),
        ((pairs, 8, LANES), f32),
        ((pairs, ch, LANES), bf16),
        ((pairs, ch, LANES), bf16),
        ((pairs, ch, LANES), bf16),
        ((pairs, ch, LANES), bf16),
        ((pairs, ch, LANES), bf16),
        ((ch, STATE), bf16),
        ((ch, STATE), bf16),
        ((STATE, ch), bf16),
        ((STATE, ch), bf16),
        ((ch, 2 * STATE), f32),
        ((ch, ch), f32),
        ((ch, ch), f32),
        ((ch, ch), f32),
        ((gh, ch, LANES), f32),
        ((gh, ch), f32),
        ((gh, ch), f32),
        ((gh, LANES), f32),
        ((pairs, ch, LANES), f32),
        ((pairs, 2, STATE, LANES), f32),
        ((pairs, 2, STATE, LANES), f32),
        ((pairs, 2, STATE, LANES), bf16),
        ((pairs, 2, STATE, LANES), bf16),
        ((pairs, 2, STATE, LANES), bf16),
        ((pairs, 2, STATE, LANES), bf16),
        ((ch, STATE), f32),
        ((ch, STATE), f32),
        ((ch, LANES), f32),
        ((ch, LANES), f32),
        ((8, LANES), f32),
        ((gh, ch), f32),
        ((ch, gw), bf16),
        ((GROUPS, tokens + 2 * HALO, gw), bf16),
        ((ch + 2 * HALO, 2 * STATE), bf16),
        ((GROUPS, gh, tokens), bf16),
        ((ch, 2 * STATE), bf16),
        ((GROUPS, tokens, 2 * STATE), bf16),
        ((dp, ch, 2 * STATE), bf16),
        ((2, STATE, cw), f32),
        ((2, chunks, rows, STATE), bf16),
        ((2, chunks, rows, STATE), f32),
        ((2, chunks, rows, STATE), bf16),
        ((2, rows, STATE), bf16),
    ]
    dgate, dx, ddt, dh, tall = pl.pallas_call(
        functools.partial(mega_kernel, heads, cores),
        in_specs=[hbm] * 16,
        out_specs=[vmem] * 5,
        out_shape=[
            pltpu.VMEM((tokens, inner), bf16),
            pltpu.VMEM((tokens, inner), bf16),
            pltpu.VMEM((HEADS, tokens), bf16),
            pltpu.VMEM((tokens, width_in), bf16),
            pltpu.VMEM((2, GROUPS, chunks, rows, STATE), bf16),
        ],
        scratch_shapes=[pltpu.VMEM(shape, kind) for shape, kind in scratch]
        + [pltpu.SemaphoreType.DMA((send_slots,)), pltpu.SemaphoreType.DMA((arrival_slots,))]
        + [pltpu.SemaphoreType.DMA((16,))],
        compiler_params=pltpu.CompilerParams(
            collective_id=0, has_side_effects=True, vmem_limit_bytes=60 * 1024 * 1024
        ),
        name="mega",
    )(
        layer_activity.reshape(tokens, width_in),
        writer_matrix,
        reader_matrix,
        source_unfiltered.reshape(tokens, inner),
        switch_raw_signal.reshape(tokens, inner),
        saved_result.reshape(tokens, inner),
        final_adjoint.reshape(tokens, inner),
        delta_raw.reshape(tokens, HEADS).T,
        extra_logdrop.reshape(window, heads).T,
        source_filter_coefs,
        writer_filter_coefs,
        reader_filter_coefs,
        rescale_factor.reshape(1, inner),
        delta_offset.reshape(1, heads),
        fading_exponents.reshape(1, heads),
        direct_factor.reshape(1, heads),
    )
    d_gate, d_x, d_hidden, d_dt, d_w_b, d_w_c = pl.pallas_call(
        out_kernel,
        in_specs=[vmem] * 5,
        out_specs=[hbm] * 6,
        scratch_shapes=[pltpu.VMEM((2, cw, latent), f32), pltpu.SemaphoreType.DMA((6,))],
        out_shape=[
            jax.ShapeDtypeStruct((tokens, inner), bf16),
            jax.ShapeDtypeStruct((tokens, inner), bf16),
            jax.ShapeDtypeStruct((tokens, width_in), bf16),
            jax.ShapeDtypeStruct((HEADS, tokens), bf16),
            jax.ShapeDtypeStruct((cw, latent), f32),
            jax.ShapeDtypeStruct((cw, latent), f32),
        ],
        name="outputs",
    )(*[pltpu.with_memory_space_constraint(v, pltpu.VMEM) for v in (dgate, dx, dh, ddt, tall)])
    return (
        d_hidden.reshape(1, tokens, width_in),
        d_x.reshape(1, tokens, inner),
        d_gate.reshape(1, tokens, inner),
        d_dt.T.reshape(1, tokens, HEADS),
        d_w_b,
        d_w_c,
    )


def solution(mesh):
    in_specs = (
        P("dp", "sp", None),
        P("dp", None),
        P("dp", None),
        P("dp", "sp", None),
        P("dp", "sp", None),
        P("dp", "sp", None),
        P("dp", "sp", None),
        P("dp", "sp", None),
        P("dp", None, "sp"),
        P(None, "sp"),
        P(),
        P(),
        P("sp"),
        P("sp"),
        P("sp"),
        P(),
    )
    out_specs = (
        P("dp", "sp", None),
        P("dp", "sp", None),
        P("dp", "sp", None),
        P("dp", "sp", None),
        P("dp", None),
        P("dp", None),
    )
    return jax.shard_map(local, mesh=mesh, in_specs=in_specs, out_specs=out_specs, check_vma=False)
```

```python
import functools

import jax
import jax.numpy as jnp
from jax import lax
from jax.experimental import pallas as pl
from jax.experimental.pallas import tpu as pltpu
from jax.sharding import PartitionSpec as P

HEADS = 32
HEAD_DIM = 64
STATE = 128
GROUPS = 2
NORM_GROUPS = 8
CONV_K = 5
LANES = 128
HALO = 16
SKEW = 3
PIECES = 4
EPSILON = 1e-06
LOG2E = 1.4426950408889634
highest = lax.Precision.HIGHEST
f32 = jnp.float32
bf16 = jnp.bfloat16
NT = (((1,), (1,)), ((), ()))
TN = (((0,), (0,)), ((), ()))


def sigmoid(v):
    return 1.0 / (1.0 + jnp.exp(-v))


def softplus(v):
    e = jnp.exp(-jnp.abs(v))
    z = e / (2.0 + e)
    z2 = z * z
    series = jnp.full_like(z, 1.0 / 17.0)
    for odd in (15, 13, 11, 9, 7, 5, 3, 1):
        series = series * z2 + 1.0 / odd
    return jnp.maximum(v, 0.0) + 2.0 * z * series


def mm(a, b):
    return jnp.dot(a, b, preferred_element_type=f32)


def mm_nt(a, b):
    return lax.dot_general(a, b, NT, preferred_element_type=f32)


def mm_tn(a, b):
    return lax.dot_general(a, b, TN, preferred_element_type=f32)


def split_mm(a, b):
    hi = a.astype(bf16)
    lo = (a - hi.astype(f32)).astype(bf16)
    return mm(hi, b) + mm(lo, b)


def window_conv(rows, taps, count, flip):
    total = None
    for k in range(CONV_K):
        shift = HALO - CONV_K // 2 + k
        tap = taps[CONV_K - 1 - k if flip else k][None, :]
        term = tap * pltpu.roll(rows, rows.shape[0] - shift, axis=0)[:count]
        total = term if total is None else total + term
    return total


def greet(axes):
    barrier = pltpu.get_barrier_semaphore()
    count = 0
    for axis in axes:
        size = lax.axis_size(axis)
        me = lax.axis_index(axis)
        for o in range(1, size):
            pl.semaphore_signal(
                barrier,
                inc=1,
                device_id={axis: lax.rem(me + o, size)},
                device_id_type=pl.DeviceIdType.MESH,
            )
            count += 1
    pl.semaphore_wait(barrier, count)


class Phases:
    def __init__(self):
        self.scope = None

    def __call__(self, name):
        self.end()
        self.scope = jax.named_scope(name)
        self.scope.__enter__()

    def end(self):
        if self.scope is not None:
            self.scope.__exit__(None, None, None)
            self.scope = None


def slot_tables(sp, dp, cores, pairs):
    others = dp // cores - 1
    chunks = sp // GROUPS
    counts = (
        ("w_y", 2 * others, 2 * others),
        ("w_core", 2, 2),
        ("w_fwd", 2 * others, 2 * others),
        ("la_y", PIECES * others, PIECES * others),
        ("la", others + 1, others + 1),
        ("p_y", PIECES * others, PIECES * others),
        ("x", 1, 1),
        ("x_left", 1, 1),
        ("x_right", 1, 1),
        ("dt", 1, 1),
        ("drop", 2, 1),
        ("tap", 1, 1),
        ("dy", 1, NORM_GROUPS // GROUPS),
        ("bc", PIECES, PIECES),
        ("bc_left", 1, 1),
        ("bc_right", 1, 1),
        ("right", 4, 2 * pairs),
        ("left", 4, 2 * pairs),
        ("gx", 1, 1),
        ("gx_left", 1, GROUPS),
        ("gx_right", 1, GROUPS),
        ("db_left", 1, 1),
        ("db_right", 1, 1),
        ("gx_g", 1, 1),
        ("cols", 1, 1),
        ("ddt", 1, 1),
        ("g_y", 2 * others, 2 * others),
        ("g_core", 2, 2),
        ("g_fwd", 2 * others, 2 * others),
        ("w2", 2, 2),
        ("w3", 2, 2 * chunks),
        ("w4", 1, 1),
    )
    sends, arrivals = {}, {}
    send_at = arrive_at = 0
    for name, send_count, arrive_count in counts:
        sends[name], arrivals[name] = send_at, arrive_at
        send_at += send_count
        arrive_at += arrive_count
    return sends, arrivals, max(send_at, 1), max(arrive_at, 1)


def mega_kernel(
    heads,
    cores,
    la_hbm,
    wb_hbm,
    wc_hbm,
    x_hbm,
    gates_hbm,
    values_hbm,
    adjoint_hbm,
    dt_hbm,
    drop_hbm,
    tapx_hbm,
    tapb_hbm,
    tapc_hbm,
    scale_hbm,
    offset_hbm,
    fade_hbm,
    skip_hbm,
    dgate_ref,
    dx_ref,
    ddt_ref,
    dh_ref,
    tall,
    la_ref,
    wb_ref,
    wc_ref,
    x_ref,
    gates_ref,
    values_ref,
    adjoint_ref,
    dt_ref,
    drop_ref,
    tapx_ref,
    tapb_ref,
    tapc_ref,
    scale_ref,
    offset_ref,
    fade_ref,
    skip_ref,
    wball,
    wcall,
    cols,
    lain,
    psend,
    pin,
    psum,
    xin,
    dyin,
    dysend,
    dtin,
    dropsend,
    dropin,
    drow,
    tapsend,
    tapin,
    tapall,
    bcsend,
    bcin,
    u_ref,
    sux_ref,
    dts_ref,
    ef_ref,
    eb_ref,
    tdec,
    vb_ref,
    vef_ref,
    veb_ref,
    dyef_ref,
    dyeb_ref,
    kn,
    rn,
    kt,
    rt,
    sbc_ref,
    score_ref,
    sign_ref,
    gesum,
    lcolb,
    lrow,
    sigrow,
    faderow,
    dv_ref,
    sr_ref,
    sl_ref,
    rin,
    lin,
    rout,
    lout,
    dksum,
    drsum,
    dlev,
    sdt,
    cross,
    colrow,
    dpx,
    gx,
    dbin,
    ddtsend,
    gsend,
    ghid,
    gall,
    wtot,
    wsend,
    wown,
    w2in,
    s3send,
    ss,
    rs,
    ls,
):
    dp = lax.axis_size("dp")
    sp = lax.axis_size("sp")
    me_dp = lax.axis_index("dp")
    me_sp = lax.axis_index("sp")
    ny = dp // cores
    chunks = sp // GROUPS
    y = me_dp // cores
    core = lax.rem(me_dp, cores)
    c = me_sp // GROUPS
    m = lax.rem(me_sp, GROUPS)
    p = GROUPS - 1 - m
    partner = c * GROUPS + p
    other_core = y * cores + (cores - 1 - core)
    tokens, inner = x_ref.shape
    gw = inner // GROUPS
    gh = HEADS // GROUPS
    ch = tokens * GROUPS
    pairs = gw // LANES
    cw = wb_ref.shape[0]
    latent = wb_ref.shape[1]
    xc = heads * HEAD_DIM
    nsrc = sp // GROUPS
    rows = cw // chunks
    first = c == 0
    last = c == chunks - 1
    sends, arrivals, _, _ = slot_tables(sp, dp, cores, pairs)
    sent = []

    def copy(src, dst, name, index, axis, peer, into=None):
        return pltpu.make_async_remote_copy(
            src_ref=src,
            dst_ref=dst,
            send_sem=ss.at[sends[name] + index],
            recv_sem=rs.at[arrivals[name] + (index if into is None else into)],
            device_id={axis: peer},
            device_id_type=pl.DeviceIdType.MESH,
        )

    def go(item, cond=None, alone=True):
        if cond is None:
            item.start()
        else:

            @pl.when(cond)
            def _():
                item.start()

        if alone:
            sent.append((item, cond))
        return item

    def together(name, index, region, cond=None):
        sent.append((copy(region, region, name, index, "sp", partner), cond))

    def arrive(item, cond=None):
        if cond is None:
            item.wait_recv()
        else:

            @pl.when(cond)
            def _():
                item.wait_recv()

    def lanes(index, width):
        return pl.ds(pl.multiple_of(index * width, LANES), width)

    def near(step):
        return lax.rem(me_sp + step + 2 * sp, sp)

    mine = pl.ds(pl.multiple_of(HALO + m * tokens, HALO), tokens)
    mine0 = pl.ds(pl.multiple_of(m * tokens, HALO), tokens)
    body = slice(HALO, HALO + ch)
    left_rows = slice(0, HALO)
    right_rows = slice(HALO + ch, 2 * HALO + ch)
    to_right = jnp.logical_and(m == GROUPS - 1, jnp.logical_not(last))
    to_left = jnp.logical_and(m == 0, jnp.logical_not(first))

    phase = Phases()
    phase("greet")
    loads = {}
    for at, (source, target) in enumerate(
        (
            (wb_hbm, wb_ref),
            (wc_hbm, wc_ref),
            (x_hbm, x_ref),
            (values_hbm, values_ref),
            (gates_hbm, gates_ref),
            (adjoint_hbm, adjoint_ref),
            (la_hbm, la_ref),
            (dt_hbm, dt_ref),
            (drop_hbm, drop_ref),
            (tapx_hbm, tapx_ref),
            (tapb_hbm, tapb_ref),
            (tapc_hbm, tapc_ref),
            (scale_hbm, scale_ref),
            (offset_hbm, offset_ref),
            (fade_hbm, fade_ref),
            (skip_hbm, skip_ref),
        )
    ):
        loads[at] = pltpu.make_async_copy(source, target, ls.at[at])
    for at in (6, 2, 0, 1, *range(7, 16), 3, 4, 5):
        loads[at].start()
    greet(("dp", "sp"))
    loads[6].wait()

    phase("send_first")
    cwy = cores * cw
    part_rows = tokens // PIECES
    parts = [slice(t * part_rows, (t + 1) * part_rows) for t in range(PIECES)]
    la_y = {}
    for t in range(PIECES):
        for o in range(1, ny):
            there = lax.rem(y + o, ny)
            la_y[o, t] = go(
                copy(
                    la_ref.at[parts[t], lanes(there, cwy)],
                    lain.at[y, parts[t], :],
                    "la_y",
                    PIECES * (o - 1) + t,
                    "dp",
                    there * cores + core,
                )
            )
    loads[2].wait()
    x_copy = go(copy(x_ref.at[:, lanes(p, gw)], xin.at[mine, :], "x", 0, "sp", partner))
    loads[0].wait()
    loads[1].wait()
    w_core = []
    if cores > 1:
        w_core = [
            go(copy(wb_ref, wball.at[me_dp], "w_core", 0, "dp", other_core)),
            go(copy(wc_ref, wcall.at[me_dp], "w_core", 1, "dp", other_core)),
        ]
    for at in range(7, 16):
        loads[at].wait()
    dt_copy = go(
        copy(
            dt_ref.at[pl.ds(pl.multiple_of(p * gh, gh), gh), :],
            dtin.at[:, lanes(m, tokens)],
            "dt",
            0,
            "sp",
            partner,
        )
    )

    def send_halo(name, source, target):
        for g in range(GROUPS):
            go(
                copy(
                    source(g, slice(tokens - HALO, tokens)),
                    target.at[left_rows, :],
                    name + "_left",
                    0,
                    "sp",
                    near(1 + g),
                    into=0,
                ),
                to_right,
                alone=False,
            )
            go(
                copy(
                    source(g, slice(0, HALO)),
                    target.at[right_rows, :],
                    name + "_right",
                    0,
                    "sp",
                    near(g - GROUPS),
                    into=0,
                ),
                to_left,
                alone=False,
            )
        together(name + "_left", 0, target.at[: GROUPS * HALO, :], to_right)
        together(name + "_right", 0, target.at[: GROUPS * HALO, :], to_left)

    def await_halo(name, target):
        arrive(
            copy(target.at[left_rows, :], target.at[left_rows, :], name + "_left", 0, "sp", partner),
            jnp.logical_not(first),
        )
        arrive(
            copy(target.at[right_rows, :], target.at[right_rows, :], name + "_right", 0, "sp", partner),
            jnp.logical_not(last),
        )

        @pl.when(first)
        def _():
            target[left_rows, :] = jnp.zeros((HALO, target.shape[1]), bf16)

        @pl.when(last)
        def _():
            target[right_rows, :] = jnp.zeros((HALO, target.shape[1]), bf16)

    send_halo("x", lambda g, r: x_ref.at[r, g * gw : (g + 1) * gw], xin)

    phase("params")
    rows_h = dropsend.shape[1]
    head_row = lax.broadcasted_iota(jnp.int32, (rows_h, LANES), 0)
    offsets = jnp.zeros((rows_h, LANES), f32)
    fades = jnp.zeros((rows_h, LANES), f32)
    head_lane = lax.broadcasted_iota(jnp.int32, (1, heads), 1)

    def pick(ref, h):
        return jnp.sum(jnp.where(head_lane == h, ref[...], 0.0), axis=1, keepdims=True)

    for h in range(heads):
        offsets = jnp.where(head_row == h, pick(offset_ref, h), offsets)
        fades = jnp.where(head_row == h, pick(fade_ref, h), fades)
    dropsend[...] = jnp.zeros_like(dropsend)
    for k in range(chunks):
        dropsend[k, :heads, :ch] = drop_ref[:, k * ch : (k + 1) * ch]
        dropsend[k, :, ch : ch + LANES] = offsets
        dropsend[k, :, ch + LANES :] = fades
    owner = (me_sp * heads) // gh
    place = me_sp - owner * nsrc
    for o in range(chunks):
        k = lax.rem(c + o, chunks)
        go(
            copy(
                dropsend.at[k],
                dropin.at[place],
                "drop",
                0 if o else 1,
                "sp",
                k * GROUPS + owner if o else partner,
                into=0,
            ),
            None if o else owner != m,
            alone=not o,
        )
    if chunks > 1:
        together("drop", 0, dropsend.at[: chunks - 1])

    @pl.when(owner == m)
    def _():
        dropin[place] = dropsend[c]

    xw = tapsend.shape[1]
    tap_lane = lax.broadcasted_iota(jnp.int32, (1, xw), 1) // HEAD_DIM
    skips = jnp.zeros((1, xw), f32)
    for h in range(heads):
        skips = jnp.where(tap_lane == h, pick(skip_ref, h), skips)
    tapsend[...] = jnp.zeros_like(tapsend)
    tapsend[:CONV_K, :xc] = tapx_ref[...]
    tapsend[CONV_K : CONV_K + 1, :] = skips
    for o in range(1, sp):
        go(copy(tapsend, tapin.at[me_sp], "tap", 0, "sp", lax.rem(me_sp + o, sp)), alone=False)
    all_taps = tapin.at[: sp - 1]
    together("tap", 0, all_taps)
    tapin[me_sp] = tapsend[...]
    la_copies = []
    if cores > 1:
        la_copies.append(
            go(copy(la_ref.at[:, lanes(other_core, cw)], cols.at[m, me_dp], "la", 0, "dp", other_core))
        )
    cols[m, me_dp] = la_ref[:, lanes(me_dp, cw)]
    wball[me_dp] = wb_ref[...]
    wcall[me_dp] = wc_ref[...]
    xin[mine, :] = x_ref[:, lanes(m, gw)]
    dtin[:, lanes(m, tokens)] = dt_ref[pl.ds(pl.multiple_of(m * gh, gh), gh), :]

    phase("norm")
    width = inner // NORM_GROUPS
    per_half = NORM_GROUPS // GROUPS
    early = per_half // 2
    dy_copies = []
    for at in (3, 4, 5):
        loads[at].wait()
    for half in range(GROUPS):
        who = p if half == 0 else m
        for i in range(per_half):
            span = lanes(who * per_half + i, width)
            values = values_ref[:, span].astype(f32)
            gates = gates_ref[:, span].astype(f32)
            sig = sigmoid(gates)
            act = gates * sig
            g = values * act
            dn = adjoint_ref[:, span].astype(f32) * scale_ref[:, span]
            inv = lax.rsqrt(jnp.sum(g * g, axis=1, keepdims=True) * (1.0 / width) + EPSILON)
            along = jnp.sum(dn * g, axis=1, keepdims=True) * (1.0 / width)
            dg = inv * dn - g * (inv * inv * inv * along)
            dgate_ref[:, span] = (dg * values * (sig + act * (1.0 - sig))).astype(bf16)
            dy = (dg * act).astype(bf16)
            at = slice(i * width, (i + 1) * width)
            if half == 0:
                dysend[:, at] = dy
                dy_copies.append(
                    copy(dysend.at[:, at], dyin.at[mine0, at], "dy", 0, "sp", partner, into=i)
                )
                if i < early:
                    go(dy_copies[i], alone=False)
            else:
                dyin[mine0, at] = dy

    phase("partial")
    for item in w_core:
        arrive(item)
    p_y = {}
    for t in range(PIECES):
        for o in range(1, ny):
            there = lax.rem(y - o + ny, ny)
            arrive(la_y[o, t])
            tb = tc = None
            for k in range(cores):
                part = lain[there, parts[t], k * cw : (k + 1) * cw]
                one, two = mm(part, wball[y * cores + k]), mm(part, wcall[y * cores + k])
                tb, tc = (one, two) if tb is None else (tb + one, tc + two)
            psend[there, parts[t], :latent] = tb.astype(bf16)
            psend[there, parts[t], latent:] = tc.astype(bf16)
            p_y[o, t] = go(
                copy(
                    psend.at[there, parts[t], :],
                    pin.at[y, parts[t], :],
                    "p_y",
                    PIECES * (o - 1) + t,
                    "dp",
                    there * cores + core,
                )
            )
    for o in range(1, ny):
        there = lax.rem(y - o + ny, ny)
        block = there * cores + core
        cols[m, block] = lain[there, :, lanes(core, cw)]
        if cores > 1:
            la_copies.append(
                go(
                    copy(
                        lain.at[there, :, lanes(cores - 1 - core, cw)],
                        cols.at[m, block],
                        "la",
                        o,
                        "dp",
                        other_core,
                    )
                )
            )
    total_b = total_c = None
    for k in range(cores):
        part = la_ref[:, lanes(y * cores + k, cw)]
        one, two = mm(part, wball[y * cores + k]), mm(part, wcall[y * cores + k])
        total_b, total_c = (one, two) if k == 0 else (total_b + one, total_c + two)
    psum[:, :latent] = total_b
    psum[:, latent:] = total_c
    phase("project")
    bc_copies = []
    for t in range(PIECES):
        total = psum[parts[t], :]
        for o in range(1, ny):
            arrive(p_y[o, t])
            total = total + pin[lax.rem(y - o + ny, ny), parts[t], :].astype(f32)
        total = total.astype(bf16)
        for g in range(GROUPS):
            at = slice(g * STATE, (g + 1) * STATE)
            bcsend[g, parts[t], :STATE] = total[:, at]
            at = slice(latent + g * STATE, latent + (g + 1) * STATE)
            bcsend[g, parts[t], STATE:] = total[:, at]
        into = pl.ds(pl.multiple_of(HALO + m * tokens + t * part_rows, HALO), part_rows)
        bc_copies.append(
            go(copy(bcsend.at[p, parts[t], :], bcin.at[into, :], "bc", t, "sp", partner))
        )
    send_halo("bc", lambda g, r: bcsend.at[g, r, :], bcin)
    bcin[mine, :] = bcsend[m]

    phase("levels")
    arrive(dt_copy)
    if nsrc > 1:
        some = dropin.at[: nsrc - 1]
        arrive(copy(some, some, "drop", 0, "sp", partner), owner == m)
    arrive(copy(dropin, dropin, "drop", 0, "sp", partner), owner != m)
    for i in range(nsrc):
        drow[i * heads : (i + 1) * heads, :] = dropin[i, :heads, :]
    twice = lambda v: jnp.concatenate([v] * (ch // LANES), axis=1)
    fade = jnp.exp(drow[:, ch + LANES :])
    a = dtin[...].astype(f32) + twice(drow[:, ch : ch + LANES])
    dt = softplus(a)
    sigrow[...] = sigmoid(a)
    faderow[...] = fade
    rate = dt * twice(fade) + drow[:, :ch]
    row_i = lax.broadcasted_iota(jnp.int32, (ch, ch), 0)
    col_i = lax.broadcasted_iota(jnp.int32, (ch, ch), 1)
    upper = (row_i <= col_i).astype(f32)
    level = jnp.dot(rate, upper, precision=highest, preferred_element_type=f32) * LOG2E
    lrow[...] = level
    fill = jnp.zeros((LANES - gh, ch), f32)
    lcol = jnp.concatenate([level, fill], axis=0).T
    dtcol = jnp.concatenate([dt, fill], axis=0).T
    low_lane = lax.broadcasted_iota(jnp.int32, (ch, LANES), 1) < HEAD_DIM
    for j in range(pairs):
        pair = []
        for h in (2 * j, 2 * j + 1):
            wide = jnp.broadcast_to(lcol[:, h : h + 1], (ch, LANES))
            lcolb[h] = wide
            pair.append(wide)
        spread = jnp.where(low_lane, pair[0], pair[1])
        end = spread[ch - 1 : ch, :]
        ef_ref[j] = jnp.exp2(-spread)
        eb_ref[j] = jnp.exp2(spread - end)
        tdec[j] = jnp.broadcast_to(jnp.exp2(-end), (8, LANES))
        dts_ref[j] = jnp.where(low_lane, dtcol[:, 2 * j : 2 * j + 1], dtcol[:, 2 * j + 1 : 2 * j + 2])

    phase("wait_x")
    arrive(copy(all_taps, all_taps, "tap", 0, "sp", partner))
    if xc % LANES == 0:
        for i in range(sp):
            tapall[:, i * xc : (i + 1) * xc] = tapin[i]
    else:
        per = LANES // xc
        for i in range(inner // LANES):
            tapall[:, i * LANES : (i + 1) * LANES] = jnp.concatenate(
                [tapin[i * per + q][:, :xc] for q in range(per)], axis=1
            )
    arrive(x_copy)
    await_halo("x", xin)

    phase("prep_x")
    @pl.loop(0, pairs)
    def _(j):
        taps = tapall[:, lanes(m * pairs + j, LANES)]
        pre = window_conv(xin[:, lanes(j, LANES)].astype(f32), taps, ch, False)
        sig = sigmoid(pre)
        u = pre * sig
        u_ref[j] = u
        sux_ref[j] = sig + u * (1.0 - sig)
        v = u * dts_ref[j]
        vb_ref[j] = v.astype(bf16)
        vef_ref[j] = (v * ef_ref[j]).astype(bf16)
        veb_ref[j] = (v * eb_ref[j]).astype(bf16)

    phase("wait_bc")
    for item in dy_copies[early:]:
        go(item, alone=False)
    together("dy", 0, dysend)
    for item in bc_copies:
        arrive(item)
    await_halo("bc", bcin)
    phase("conv_bc")
    for q in range(2):
        taps = (tapb_ref, tapc_ref)[q][:, lanes(m, STATE)]
        at = slice(q * STATE, (q + 1) * STATE)
        pre = window_conv(bcin[:, at].astype(f32), taps, ch, False)
        sig = sigmoid(pre)
        kr = pre * sig
        sbc_ref[:, at] = sig + kr * (1.0 - sig)
        (kn, rn)[q][...] = kr.astype(bf16)
        (kt, rt)[q][...] = kr.T.astype(bf16)
    score = mm_nt(kn[...], rn[...])
    score_ref[...] = score
    sign_ref[...] = score * jnp.clip(col_i - row_i, -1, 1).astype(f32)

    gesum[...] = jnp.zeros_like(gesum)
    dksum[...] = jnp.zeros_like(dksum)
    drsum[...] = jnp.zeros_like(drsum)
    dlev[...] = jnp.zeros_like(dlev)
    sdt[...] = jnp.zeros_like(sdt)
    cross[...] = jnp.zeros_like(cross)

    @pl.when(first)
    def _():
        rin[...] = jnp.zeros_like(rin)

    @pl.when(last)
    def _():
        lin[...] = jnp.zeros_like(lin)

    lane_low = lax.broadcasted_iota(jnp.int32, (1, LANES), 1) < HEAD_DIM
    masks = (lane_low.astype(bf16), 1.0 - lane_low.astype(bf16))
    pick_lane = lax.broadcasted_iota(jnp.int32, (LANES, LANES), 1)
    pick_half = lax.broadcasted_iota(jnp.int32, (LANES, LANES), 0) // HEAD_DIM
    block = min(ch, LANES)

    def intra(j):
        dyj = dyin[:, lanes(j, LANES)]
        for a in range(2):
            h = 2 * j + a
            lr = lrow[pl.ds(h, 1), :]
            dym = dyj * masks[a]
            onehot = (pick_lane == h).astype(bf16)
            below = None
            for b in range(ch // block):
                at = slice(b * block, (b + 1) * block)
                gap = twice(lcolb[h, at]) - lr
                decay = jnp.exp2(-jnp.abs(gap))
                ge = mm_nt(vb_ref[j, at] * masks[a], dyj) * decay
                gesum[at, :] += ge
                part = mm((score_ref[at, :] * decay).astype(bf16), dym)
                if a == 0:
                    dv_ref[j, at] = part
                else:
                    dv_ref[j, at] += part
                q = sign_ref[at, :] * ge
                down = jnp.sum(q, axis=0, keepdims=True)
                below = down if below is None else below + down
                part = q[:, :LANES]
                for piece in range(1, ch // LANES):
                    part = part + q[:, piece * LANES : (piece + 1) * LANES]
                dlev[at, :] += split_mm(part, onehot)
            colrow[pl.ds(h, 1), :] = below

    def gx_copy(j):
        return copy(
            dpx.at[pl.ds(pl.multiple_of(p * (tokens - HALO), HALO), tokens + HALO), lanes(j, LANES)],
            gx.at[
                m, pl.ds(pl.multiple_of(HALO - HALO * p, HALO), tokens + HALO), lanes(j, LANES)
            ],
            "gx",
            0,
            "sp",
            partner,
        )

    keep_src = pl.ds(pl.multiple_of(m * (tokens - HALO), HALO), tokens + HALO)
    keep_dst = pl.ds(pl.multiple_of(HALO - HALO * m, HALO), tokens + HALO)

    def consume(j):
        k, r = kn[...], rn[...]
        ra, rb, la, lb = rin[j, 0], rin[j, 1], lin[j, 0], lin[j, 1]
        ef, eb = ef_ref[j], eb_ref[j]
        u = u_ref[j]
        at = lanes(j, LANES)
        dy = dyin[:, at].astype(f32)
        v = vb_ref[j].astype(f32)
        skip = tapall[CONV_K : CONV_K + 1, lanes(m * pairs + j, LANES)]
        onehot = (pick_lane == 2 * j + pick_half).astype(bf16)
        dl, dr = ef * mm(k, rb), eb * mm(k, lb)
        ml, mr = ef * mm(r, ra), eb * mm(r, la)
        dv = dv_ref[j] + dl + dr
        dpx[:, at] = ((dv * dts_ref[j] + skip * dy) * sux_ref[j]).astype(bf16)

        @pl.when(j < pairs - 1)
        def _():
            gx_copy(j).start()

        gx[m, keep_dst, at] = dpx[keep_src, at]
        dksum[...] += mm_nt(vef_ref[j], rb) + mm_nt(veb_ref[j], lb)
        drsum[...] += mm_nt(dyef_ref[j], ra) + mm_nt(dyeb_ref[j], la)
        dlev[...] += split_mm(dy * (mr - ml) + v * (dr - dl), onehot)
        sdt[...] += split_mm(u * dv, onehot)
        over = lb.astype(f32) * rout[j, 0].astype(f32) + la.astype(f32) * rout[j, 1].astype(f32)
        over = jnp.broadcast_to(jnp.sum(over, axis=0, keepdims=True), (8, LANES))
        cross[...] += split_mm(over, onehot)

    def chain_copy(name, j, q, into_ref, out_ref, step):
        return copy(
            out_ref.at[j, q],
            into_ref.at[j, q],
            name,
            2 * lax.rem(j, 2) + q,
            "sp",
            near(step),
            into=2 * j + q,
        )

    def chain(name, j, into_ref, own_ref, out_ref, head, tail, step):
        decay = tdec[j][0:1, :]
        for q in range(2):
            item = chain_copy(name, j, q, into_ref, out_ref, step)

            @pl.when(jnp.logical_not(head))
            def _():
                item.wait_recv()

            out_ref[j, q] = (own_ref[j, q] + decay * into_ref[j, q].astype(f32)).astype(bf16)

            @pl.when(jnp.logical_not(tail))
            def _():
                @pl.when(j >= 2)
                def _():
                    chain_copy(name, j - 2, q, into_ref, out_ref, step).wait_send()

                item.start()

    delay = SKEW * (chunks - 1)

    for item in la_copies:
        arrive(item)
    w_y = []
    for o in range(1, ny):
        peer = lax.rem(y + o, ny) * cores + core
        w_y.append(
            (
                go(copy(wb_ref, wball.at[me_dp], "w_y", 2 * o - 2, "dp", peer)),
                go(copy(wc_ref, wcall.at[me_dp], "w_y", 2 * o - 1, "dp", peer)),
            )
        )
    cols_copy = go(copy(cols.at[m], cols.at[m], "cols", 0, "sp", partner))
    phase("ticks")
    @pl.loop(0, pairs + delay)
    def _(tick):
        per = width // LANES

        @pl.when(jnp.logical_and(tick < pairs, lax.rem(tick, per) == 0))
        def _():
            piece = lanes(tick // per, width)
            block = dyin.at[mine0, piece]
            arrive(copy(block, block, "dy", 0, "sp", partner, into=tick // per))

        @pl.when(tick < pairs)
        def _():
            dy = dyin[:, lanes(tick, LANES)].astype(f32)
            dyef_ref[tick] = (dy * ef_ref[tick]).astype(bf16)
            dyeb_ref[tick] = (dy * eb_ref[tick]).astype(bf16)
            sr_ref[tick, 0] = mm(kt[...], veb_ref[tick])
            sr_ref[tick, 1] = mm(rt[...], dyeb_ref[tick])
            sl_ref[tick, 0] = mm(kt[...], vef_ref[tick])
            sl_ref[tick, 1] = mm(rt[...], dyef_ref[tick])

        jl = tick - SKEW * (chunks - 1 - c)

        @pl.when(jnp.logical_and(jl >= 0, jl < pairs))
        def _():
            with jax.named_scope("chain_l"):
                chain("left", jl, lin, sl_ref, lout, last, first, -GROUPS)

        jr = tick - SKEW * c

        @pl.when(jnp.logical_and(jr >= 0, jr < pairs))
        def _():
            with jax.named_scope("chain_r"):
                chain("right", jr, rin, sr_ref, rout, first, last, GROUPS)

        @pl.when(tick < pairs)
        def _():
            with jax.named_scope("intra"):
                intra(tick)

        @pl.when(tick == pairs - 1)
        def _():
            ge = gesum[...].astype(bf16)
            dksum[...] += mm(ge, rn[...])
            drsum[...] += mm_tn(ge, kn[...])

        @pl.when(tick >= delay)
        def _():
            with jax.named_scope("consume"):
                consume(tick - delay)

    phase("send_dbc")
    sbc = sbc_ref[...]
    dbin[body, :STATE] = (dksum[...] * sbc[:, :STATE]).astype(bf16)
    dbin[body, STATE:] = (drsum[...] * sbc[:, STATE:]).astype(bf16)
    go(
        copy(
            dbin.at[ch : HALO + ch, :], dbin.at[left_rows, :], "db_left", 0, "sp", near(GROUPS)
        ),
        jnp.logical_not(last),
    )
    go(
        copy(
            dbin.at[HALO : 2 * HALO, :], dbin.at[right_rows, :], "db_right", 0, "sp", near(-GROUPS)
        ),
        jnp.logical_not(first),
    )

    def send_edges(name, source, target):
        go(
            copy(
                source.at[ch - HALO :, :],
                target.at[m, :HALO, :],
                name + "_left",
                0,
                "sp",
                lax.rem((c + 1) * GROUPS, sp),
                into=m,
            ),
            jnp.logical_not(last),
        )
        go(
            copy(
                source.at[:HALO, :],
                target.at[m, HALO + tokens :, :],
                name + "_right",
                0,
                "sp",
                lax.rem(c * GROUPS - 1 + sp, sp),
                into=m,
            ),
            jnp.logical_not(first),
        )

    def await_edges(name, target):
        lead, trail = m == 0, m == GROUPS - 1
        for g in range(GROUPS):
            slot = target.at[g, :HALO, :]
            arrive(
                copy(slot, slot, name + "_left", 0, "sp", partner, into=g),
                jnp.logical_and(lead, jnp.logical_not(first)),
            )
            slot = target.at[g, HALO + tokens :, :]
            arrive(
                copy(slot, slot, name + "_right", 0, "sp", partner, into=g),
                jnp.logical_and(trail, jnp.logical_not(last)),
            )

        @pl.when(jnp.logical_and(lead, first))
        def _():
            target[:, :HALO, :] = jnp.zeros((GROUPS, HALO, target.shape[2]), bf16)

        @pl.when(jnp.logical_and(trail, last))
        def _():
            target[:, HALO + tokens :, :] = jnp.zeros((GROUPS, HALO, target.shape[2]), bf16)

    gx_copy(pairs - 1).start()
    send_edges("gx", dpx, gx)

    phase("wait_db")
    await_halo("db", dbin)
    phase("conv_g")
    for q in range(2):
        at = slice(q * STATE, (q + 1) * STATE)
        taps = (tapb_ref, tapc_ref)[q][:, lanes(m, STATE)]
        gsend[:, at] = window_conv(dbin[:, at].astype(f32), taps, ch, True).astype(bf16)

    phase("send_g")
    halves = [slice(q * STATE, (q + 1) * STATE) for q in range(2)]

    def g_copy(source, block, name, index, q, peer):
        return go(
            copy(
                source.at[:, halves[q]],
                gall.at[block, :, halves[q]],
                name,
                2 * index + q,
                "dp",
                peer,
            )
        )

    g_y = {}
    g_core = {}
    for q in range(2):
        for o in range(1, ny):
            peer = lax.rem(y + o, ny) * cores + core
            g_y[o, q] = g_copy(gsend, me_dp, "g_y", o - 1, q, peer)
        if cores > 1:
            g_core[q] = g_copy(gsend, me_dp, "g_core", 0, q, other_core)
    theirs = pl.ds(pl.multiple_of(p * tokens, HALO), tokens)
    hid_copy = go(copy(gsend.at[theirs, :], ghid.at[m], "gx_g", 0, "sp", partner))
    ghid[m] = gsend[mine0, :]
    gall[me_dp] = gsend[...]
    phase("ddt")
    w_fwd = []
    for o in range(1, ny):
        src = lax.rem(y - o + ny, ny) * cores + core
        for q in range(2):
            arrive(w_y[o - 1][q])
            if cores > 1:
                full = (wball, wcall)[q].at[src]
                w_fwd.append(go(copy(full, full, "w_fwd", 2 * o - 2 + q, "dp", other_core)))

    fill = jnp.zeros((LANES - gh, ch), f32)
    down = jnp.concatenate([colrow[...], fill], axis=0).T
    drate = jnp.dot(upper, dlev[...] - down, precision=highest, preferred_element_type=f32)
    drate = (drate - cross[0:1, :]).T[:gh]
    ddt = ((drate * twice(faderow[...]) + sdt[...].T[:gh]) * sigrow[...]).astype(bf16)
    for g in range(GROUPS):
        ddtsend[g] = ddt[:, g * tokens : (g + 1) * tokens]
    group_rows = pl.ds(pl.multiple_of(m * gh, gh), gh)
    ddt_copy = go(copy(ddtsend.at[p], ddt_ref.at[group_rows, :], "ddt", 0, "sp", partner))
    ddt_ref[group_rows, :] = ddtsend[m]

    phase("wait_g")
    arrive(cols_copy)
    sources = {o: lax.rem(y - o + ny, ny) * cores + core for o in range(1, ny)}
    relayed = {o: lax.rem(y - o + ny, ny) * cores + cores - 1 - core for o in range(1, ny)}
    g_fwd = {}
    for q in range(2):
        for o in range(1, ny):
            if cores > 1:
                block = gall.at[sources[o], :, halves[q]]
                g_fwd[o, q] = copy(
                    block, block, "g_fwd", 2 * (o - 1) + q, "dp", other_core
                )
                sent.append((g_fwd[o, q], None))
        if chunks > 1:
            together("w2", q, w2in.at[q, : chunks - 1])

    def by_distance(distances, act):
        for d in distances:
            for k in (c + d, c - d):

                @pl.when(jnp.logical_and(k >= 0, k < chunks))
                def _():
                    act(k)

    def add_block(q, i, fresh=False):
        total = None
        for g in range(GROUPS):
            term = mm_tn(gall[i, g * tokens : (g + 1) * tokens, halves[q]], cols[g, i])
            total = term if total is None else total + term
        wtot[q] = total if fresh else wtot[q] + total

    def add_peers(q):
        for o in range(1, ny):
            arrive(g_y[o, q])
            if cores > 1:
                g_fwd[o, q].start()
            add_block(q, sources[o])

    def add_other_core(q):
        if cores > 1:
            arrive(g_core[q])
            add_block(q, other_core)
            for o in range(1, ny):
                arrive(g_fwd[o, q])
                add_block(q, relayed[o])

    def scatter(q):
        total = wtot[q].T.reshape(chunks, rows, STATE)
        wown[q] = total
        wsend[q] = total.astype(bf16)

        def send(k):
            copy(wsend.at[q, k], w2in.at[q, c], "w2", q, "sp", k * GROUPS + m).start()

        by_distance(reversed(range(1, chunks)), send)

    for q in range(2):
        add_block(q, me_dp, fresh=True)

    @pl.when(core == 0)
    def _():
        add_other_core(0)
        add_other_core(1)
        for q in range(2):
            add_peers(q)
            scatter(q)

    @pl.when(core != 0)
    def _():
        add_peers(0)
        add_peers(1)
        for q in range(2):
            add_other_core(q)
            scatter(q)

    phase("d_hidden")
    for item in w_fwd:
        arrive(item)
    arrive(hid_copy)
    gb = jnp.concatenate([ghid[g, :, :STATE] for g in range(GROUPS)], axis=1)
    gc = jnp.concatenate([ghid[g, :, STATE:] for g in range(GROUPS)], axis=1)
    for i in range(dp):
        dh_ref[:, i * cw : (i + 1) * cw] = (mm_nt(gb, wball[i]) + mm_nt(gc, wcall[i])).astype(bf16)

    def input_gradient(g):
        @pl.loop(0, pairs)
        def _(j):
            taps = tapall[:, lanes(g * pairs + j, LANES)]
            part = gx[g, :, lanes(j, LANES)].astype(f32)
            dx_ref[:, lanes(g * pairs + j, LANES)] = window_conv(part, taps, tokens, True).astype(
                bf16
            )

    phase("wait_gx")
    all_gx = gx.at[0, : tokens + HALO, :]
    arrive(copy(all_gx, all_gx, "gx", 0, "sp", partner))

    await_edges("gx", gx)
    phase("w3")
    for q in range(2):
        share = wown[q, c]
        if chunks > 1:
            arrive(copy(w2in.at[q, : chunks - 1], w2in.at[q, : chunks - 1], "w2", q, "sp", partner))
        for o in range(1, chunks):
            share = share + w2in[q, lax.rem(c - o + chunks, chunks)].astype(f32)
        s3send[q] = share.astype(bf16)
        tall[q, m, c] = s3send[q]

        def share_out(k):
            copy(
                s3send.at[q],
                tall.at[q, m, c],
                "w3",
                q,
                "sp",
                k * GROUPS + m,
                into=q * chunks + c,
            ).start()

        by_distance(reversed(range(1, chunks)), share_out)
        if chunks > 1:
            together("w3", q, tall.at[q, m, : chunks - 1])
        go(copy(s3send.at[q], tall.at[q, m, c], "w4", 0, "sp", partner), alone=False)
        phase("dx")
        input_gradient(q)
    phase("w4")
    for q in range(2):

        def pass_on(k):
            piece = tall.at[q, m, k]
            copy(piece, piece, "w3", q, "sp", partner, into=q * chunks + k).wait_recv()
            copy(piece, piece, "w4", 0, "sp", partner).start()

        by_distance(range(1, chunks), pass_on)
    phase("last")
    arrive(ddt_copy)
    arrive(copy(tall.at[:, p], tall.at[:, p], "w4", 0, "sp", partner))
    together("w4", 0, tall.at[:, m])

    together("gx", 0, all_gx)
    for j in range(max(pairs - 2, 0), pairs):
        for q in range(2):
            sent.append((chain_copy("right", j, q, rin, rout, GROUPS), jnp.logical_not(last)))
            sent.append((chain_copy("left", j, q, lin, lout, -GROUPS), jnp.logical_not(first)))

    for item, cond in sent:
        if cond is None:
            item.wait_send()
        else:

            @pl.when(cond)
            def _():
                item.wait_send()

    phase.end()


def out_kernel(
    dgate, dx, dh, ddt, tall, dgate_out, dx_out, dh_out, ddt_out, dwb_out, dwc_out, wide, sems
):
    copies = [
        pltpu.make_async_copy(source, target, sems.at[at])
        for at, (source, target) in enumerate(
            (
                (dgate, dgate_out),
                (dx, dx_out),
                (dh, dh_out),
                (ddt, ddt_out),
                (wide.at[0], dwb_out),
                (wide.at[1], dwc_out),
            )
        )
    ]
    for item in copies[:4]:
        item.start()
    for q in range(2):
        for g in range(GROUPS):
            at = slice(g * STATE, (g + 1) * STATE)
            wide[q, :, at] = tall[q, g].astype(f32).reshape(wide.shape[1], STATE)
        copies[4 + q].start()
    for item in copies:
        item.wait()


def local(
    layer_activity,
    writer_matrix,
    reader_matrix,
    source_unfiltered,
    switch_raw_signal,
    saved_result,
    final_adjoint,
    delta_raw,
    extra_logdrop,
    source_filter_coefs,
    writer_filter_coefs,
    reader_filter_coefs,
    delta_offset,
    fading_exponents,
    direct_factor,
    rescale_factor,
):
    tokens, width_in = layer_activity.shape[1:]
    inner = source_unfiltered.shape[2]
    dp = lax.axis_size("dp")
    sp = lax.axis_size("sp")
    cores = 2 if dp % 2 == 0 else 1
    heads = delta_offset.shape[0]
    cw, latent = writer_matrix.shape
    xc = heads * HEAD_DIM
    xw = -(-xc // LANES) * LANES
    rows_h = -(-heads // 8) * 8
    chunks = sp // GROUPS
    ch = tokens * GROUPS
    gw = inner // GROUPS
    gh = HEADS // GROUPS
    pairs = gw // LANES
    rows = cw // chunks
    window = tokens * sp
    _, _, send_slots, arrival_slots = slot_tables(sp, dp, cores, pairs)

    vmem = pl.BlockSpec(memory_space=pltpu.VMEM)
    hbm = pl.BlockSpec(memory_space=pltpu.HBM)
    scratch = [
        ((tokens, width_in), bf16),
        ((cw, latent), bf16),
        ((cw, latent), bf16),
        ((tokens, inner), bf16),
        ((tokens, inner), bf16),
        ((tokens, inner), bf16),
        ((tokens, inner), bf16),
        ((HEADS, tokens), bf16),
        ((heads, window), f32),
        ((CONV_K, xc), f32),
        ((CONV_K, latent), f32),
        ((CONV_K, latent), f32),
        ((1, inner), f32),
        ((1, heads), f32),
        ((1, heads), f32),
        ((1, heads), f32),
        ((dp, cw, latent), bf16),
        ((dp, cw, latent), bf16),
        ((GROUPS, dp, tokens, cw), bf16),
        ((dp // cores, tokens, cores * cw), bf16),
        ((dp // cores, tokens, 2 * latent), bf16),
        ((dp // cores, tokens, 2 * latent), bf16),
        ((tokens, 2 * latent), f32),
        ((ch + 2 * HALO, gw), bf16),
        ((ch, gw), bf16),
        ((tokens, gw), bf16),
        ((gh, ch), bf16),
        ((chunks, rows_h, ch + 2 * LANES), f32),
        ((chunks, rows_h, ch + 2 * LANES), f32),
        ((gh, ch + 2 * LANES), f32),
        ((8, xw), f32),
        ((sp, 8, xw), f32),
        ((8, inner), f32),
        ((GROUPS, tokens, 2 * STATE), bf16),
        ((ch + 2 * HALO, 2 * STATE), bf16),
        ((pairs, ch, LANES), f32),
        ((pairs, ch, LANES), f32),
        ((pairs, ch, LANES), f32),
        ((pairs, ch, LANES), f32),
        ((pairs, ch, LANES), f32),
        ((pairs, 8, LANES), f32),
        ((pairs, ch, LANES), bf16),
        ((pairs, ch, LANES), bf16),
        ((pairs, ch, LANES), bf16),
        ((pairs, ch, LANES), bf16),
        ((pairs, ch, LANES), bf16),
        ((ch, STATE), bf16),
        ((ch, STATE), bf16),
        ((STATE, ch), bf16),
        ((STATE, ch), bf16),
        ((ch, 2 * STATE), f32),
        ((ch, ch), f32),
        ((ch, ch), f32),
        ((ch, ch), f32),
        ((gh, ch, LANES), f32),
        ((gh, ch), f32),
        ((gh, ch), f32),
        ((gh, LANES), f32),
        ((pairs, ch, LANES), f32),
        ((pairs, 2, STATE, LANES), f32),
        ((pairs, 2, STATE, LANES), f32),
        ((pairs, 2, STATE, LANES), bf16),
        ((pairs, 2, STATE, LANES), bf16),
        ((pairs, 2, STATE, LANES), bf16),
        ((pairs, 2, STATE, LANES), bf16),
        ((ch, STATE), f32),
        ((ch, STATE), f32),
        ((ch, LANES), f32),
        ((ch, LANES), f32),
        ((8, LANES), f32),
        ((gh, ch), f32),
        ((ch, gw), bf16),
        ((GROUPS, tokens + 2 * HALO, gw), bf16),
        ((ch + 2 * HALO, 2 * STATE), bf16),
        ((GROUPS, gh, tokens), bf16),
        ((ch, 2 * STATE), bf16),
        ((GROUPS, tokens, 2 * STATE), bf16),
        ((dp, ch, 2 * STATE), bf16),
        ((2, STATE, cw), f32),
        ((2, chunks, rows, STATE), bf16),
        ((2, chunks, rows, STATE), f32),
        ((2, chunks, rows, STATE), bf16),
        ((2, rows, STATE), bf16),
    ]
    dgate, dx, ddt, dh, tall = pl.pallas_call(
        functools.partial(mega_kernel, heads, cores),
        in_specs=[hbm] * 16,
        out_specs=[vmem] * 5,
        out_shape=[
            pltpu.VMEM((tokens, inner), bf16),
            pltpu.VMEM((tokens, inner), bf16),
            pltpu.VMEM((HEADS, tokens), bf16),
            pltpu.VMEM((tokens, width_in), bf16),
            pltpu.VMEM((2, GROUPS, chunks, rows, STATE), bf16),
        ],
        scratch_shapes=[pltpu.VMEM(shape, kind) for shape, kind in scratch]
        + [pltpu.SemaphoreType.DMA((send_slots,)), pltpu.SemaphoreType.DMA((arrival_slots,))]
        + [pltpu.SemaphoreType.DMA((16,))],
        compiler_params=pltpu.CompilerParams(
            collective_id=0, has_side_effects=True, vmem_limit_bytes=60 * 1024 * 1024
        ),
        name="mega",
    )(
        layer_activity.reshape(tokens, width_in),
        writer_matrix,
        reader_matrix,
        source_unfiltered.reshape(tokens, inner),
        switch_raw_signal.reshape(tokens, inner),
        saved_result.reshape(tokens, inner),
        final_adjoint.reshape(tokens, inner),
        delta_raw.reshape(tokens, HEADS).T,
        extra_logdrop.reshape(window, heads).T,
        source_filter_coefs,
        writer_filter_coefs,
        reader_filter_coefs,
        rescale_factor.reshape(1, inner),
        delta_offset.reshape(1, heads),
        fading_exponents.reshape(1, heads),
        direct_factor.reshape(1, heads),
    )
    d_gate, d_x, d_hidden, d_dt, d_w_b, d_w_c = pl.pallas_call(
        out_kernel,
        in_specs=[vmem] * 5,
        out_specs=[hbm] * 6,
        scratch_shapes=[pltpu.VMEM((2, cw, latent), f32), pltpu.SemaphoreType.DMA((6,))],
        out_shape=[
            jax.ShapeDtypeStruct((tokens, inner), bf16),
            jax.ShapeDtypeStruct((tokens, inner), bf16),
            jax.ShapeDtypeStruct((tokens, width_in), bf16),
            jax.ShapeDtypeStruct((HEADS, tokens), bf16),
            jax.ShapeDtypeStruct((cw, latent), f32),
            jax.ShapeDtypeStruct((cw, latent), f32),
        ],
        name="outputs",
    )(*[pltpu.with_memory_space_constraint(v, pltpu.VMEM) for v in (dgate, dx, dh, ddt, tall)])
    return (
        d_hidden.reshape(1, tokens, width_in),
        d_x.reshape(1, tokens, inner),
        d_gate.reshape(1, tokens, inner),
        d_dt.T.reshape(1, tokens, HEADS),
        d_w_b,
        d_w_c,
    )


def solution(mesh):
    in_specs = (
        P("dp", "sp", None),
        P("dp", None),
        P("dp", None),
        P("dp", "sp", None),
        P("dp", "sp", None),
        P("dp", "sp", None),
        P("dp", "sp", None),
        P("dp", "sp", None),
        P("dp", None, "sp"),
        P(None, "sp"),
        P(),
        P(),
        P("sp"),
        P("sp"),
        P("sp"),
        P(),
    )
    out_specs = (
        P("dp", "sp", None),
        P("dp", "sp", None),
        P("dp", "sp", None),
        P("dp", "sp", None),
        P("dp", None),
        P("dp", None),
    )
    return jax.shard_map(local, mesh=mesh, in_specs=in_specs, out_specs=out_specs, check_vma=False)
```
